256 devices in a mesh: rep: 2 (over z_hi), fs: 16 (over z_lo, y), tp: 8 (over x, core).
Axes of the slice: x: 4, y: 4, z: 8 (z_hi: 2, z_lo: 4; z = z_hi * 4 + z_lo), core: 2. Of those that a mesh axis runs over, the one named last changes fastest.
Arguments:
- stream: bfloat16 [32768, 2048], P(('rep', 'fs', 'tp')), may hold values from -6 to 6
- gain_before: float32 [2048], replicated, may hold values from 0.1 to 1.9
- gain_after: float32 [2048], replicated, may hold values from 0.1 to 1.9
- proj_gate: bfloat16 [2048, 3584], P('fs', 'tp'), may hold values from -0.125 to 0.125
- proj_lift: bfloat16 [2048, 3584], P('fs', 'tp'), may hold values from -0.125 to 0.125
- proj_down: bfloat16 [3584, 2048], P('tp', 'fs'), may hold values from -0.09375 to 0.09375
- mixer_gain: float32 [2048], replicated, may hold values from 0.1 to 1.9
- mixer_u: bfloat16 [2048, 2048], P('fs', 'tp'), may hold values from -0.125 to 0.125
- mixer_v: bfloat16 [2048, 2048], P('fs', 'tp'), may hold values from -1 to 1
- layer_gain: float32 [2048], P('tp'), may hold values from 0.1 to 1.9
- layer_shift: float32 [2048], P('tp'), may hold values from -3 to 3
- spatial: bfloat16 [16, 128, 128], P('tp'), may hold values from -0.5 to 0.5
- spatial_shift: float32 [16, 128], P('tp'), may hold values from 0.2 to 2
- mixer_down: bfloat16 [2048, 2048], P('tp', 'fs'), may hold values from -0.125 to 0.125
Outputs:
- result: bfloat16 [32768, 2048], P(('rep', 'fs', 'tp'))
The draws below stay inside these ranges and needn't reach their ends.
All inputs are finite; a program needn't handle non-finite values.
Results may differ from the reference program's by a relative error of at most 0.017.
Values may be sent and summed in bfloat16 or wider, within the bound.
A program may use at most 128 MiB of HBM per device.

```python
import jax
import jax.numpy as jnp
from jax import lax

D = 2048
FF = 3584
GROUPS = 16
GROUP_DIM = 128
SPAN = 128
TOK = 1024
A = 2048
TOKENS = 32768
N_TP = 8


def draw_mixer_v(key, part):
    first_key, second_key = jax.random.split(key)
    position = jnp.arange(A, dtype=jnp.float32) / (A - 1)
    rising = 4.0
    basis = jnp.clip(jax.random.normal(first_key, (D, A), jnp.float32), -4.0, 4.0)
    jitter = jnp.exp(jax.random.uniform(second_key, (A,), jnp.float32, -0.3, 0.3))
    column_scale = rising ** (position - 0.5) * jitter
    return jnp.clip(basis * column_scale * D ** (-0.5), -1.0, 1.0).astype(jnp.bfloat16)


def levels(own_key, dims, pieces, low, high):
    def one(dim, blocks):
        draws = jax.random.uniform(jax.random.fold_in(jax.random.fold_in(own_key, 6), dim), (blocks,), jnp.float32, low / len(pieces), high / len(pieces))
        return jnp.repeat(jnp.exp(draws), dims[dim] // blocks).reshape((-1,) + (1,) * (len(dims) - dim - 1))

    factor_of = one(*pieces[0])
    for cut in pieces[1:]:
        factor_of = factor_of * one(*cut)
    return factor_of


def noise(rng, extent, scale, reach, shards=(), kind=jnp.bfloat16):
    result = scale * jax.random.normal(rng, extent, jnp.float32)
    if shards:
        result = result * levels(rng, extent, shards, -0.22, 0.18)
    return jnp.clip(result, -reach, reach).astype(kind)


def setup_inputs(seed: int = 0) -> dict:
    keys = jax.random.split(jax.random.key(seed), 15)
    stream = noise(keys[0], (TOKENS, D), 1.0, 6.0, ((0, 256),))
    gain_before = jnp.clip(1.0 + 0.18 * jax.random.normal(keys[1], (D,), jnp.float32), 0.1, 1.9)
    gain_after = jnp.clip(1.0 + 0.18 * jax.random.normal(keys[2], (D,), jnp.float32), 0.1, 1.9)
    proj_gate = noise(keys[3], (D, FF), D ** -0.5, 0.125, ((0, 16), (1, 8)))
    proj_lift = noise(keys[4], (D, FF), D ** -0.5, 0.125, ((0, 16), (1, 8)))
    proj_down = noise(keys[5], (FF, D), FF ** -0.5, 0.09375, ((0, 8), (1, 16)))
    mixer_gain = jnp.clip(1.0 + 0.18 * jax.random.normal(keys[6], (D,), jnp.float32), 0.1, 1.9)
    mixer_u = noise(keys[7], (D, A), D ** -0.5, 0.125, ((0, 16), (1, 8)))
    mixer_v = draw_mixer_v(jax.random.fold_in(keys[14], 71), 0)
    layer_gain = jnp.clip(1.0 + 0.18 * jax.random.normal(keys[9], (A,), jnp.float32), 0.1, 1.9)
    layer_shift = noise(keys[10], (A,), 0.5, 3.0, ((0, 8),), jnp.float32)
    spatial = noise(keys[11], (GROUPS, SPAN, SPAN), SPAN ** -0.5, 0.5, ((0, 8),))
    spatial_shift = jnp.clip(0.2 + 1.8 * jax.random.uniform(keys[12], (GROUPS, SPAN), jnp.float32) ** levels(keys[12], (GROUPS, SPAN), ((0, 8),), -0.2, 0.2), 0.2, 2.0)
    mixer_down = noise(keys[13], (A, D), A ** -0.5, 0.125, ((0, 8), (1, 16)))
    return {"stream": stream, "gain_before": gain_before, "gain_after": gain_after, "proj_gate": proj_gate, "proj_lift": proj_lift, "proj_down": proj_down, "mixer_gain": mixer_gain, "mixer_u": mixer_u, "mixer_v": mixer_v, "layer_gain": layer_gain, "layer_shift": layer_shift, "spatial": spatial, "spatial_shift": spatial_shift, "mixer_down": mixer_down}


norm_epsilon = 1e-06
layer_epsilon = 1e-05

def norm_rows(row_block, scale_gain):
    widened = row_block.astype(jnp.float32)
    factor = lax.rsqrt(lax.optimization_barrier(jnp.mean(widened * widened, axis=1, keepdims=True)) + norm_epsilon)
    return (widened * factor * scale_gain).astype(jnp.bfloat16)

def blocked_sum(left_rows, right_rows):
    unit_count = left_rows.shape[1] // N_TP
    running = jnp.zeros((left_rows.shape[0], right_rows.shape[1]), jnp.float32)
    for member in range(N_TP):
        partial_value = jnp.dot(left_rows[:, member * unit_count:(member + 1) * unit_count], right_rows[member * unit_count:(member + 1) * unit_count], preferred_element_type=jnp.float32)
        running = running + lax.optimization_barrier(partial_value.astype(jnp.bfloat16)).astype(jnp.float32)
    return running

def half_step(row_block, scale_gain, proj_gate, proj_lift, proj_down):
    normed = norm_rows(row_block, scale_gain)
    gate_vals = jnp.dot(normed, proj_gate, preferred_element_type=jnp.float32)
    lift_vals = jnp.dot(normed, proj_lift, preferred_element_type=jnp.float32)
    hidden = (jax.nn.silu(gate_vals) * lift_vals).astype(jnp.bfloat16)
    delta = blocked_sum(hidden, proj_down)
    return (row_block.astype(jnp.float32) + 0.5 * delta).astype(jnp.bfloat16)

def token_mixer(row_block, mixer_gain, mixer_u, mixer_v, layer_gain, layer_shift, spatial, spatial_shift, mixer_down):
    normed = norm_rows(row_block, mixer_gain)
    u_vals = jnp.dot(normed, mixer_u, preferred_element_type=jnp.float32)
    v_vals = jnp.dot(normed, mixer_v, preferred_element_type=jnp.float32)
    lifted = jax.nn.gelu(v_vals)
    centre = lax.optimization_barrier(jnp.mean(lifted, axis=1, keepdims=True))
    spread = lax.optimization_barrier(jnp.mean(jnp.square(lifted - centre), axis=1, keepdims=True))
    normed_v = ((lifted - centre) * lax.rsqrt(spread + layer_epsilon) * layer_gain + layer_shift).astype(jnp.bfloat16)
    blocked = normed_v.reshape(TOK // SPAN, SPAN, GROUPS, GROUP_DIM).astype(jnp.float32)
    causal = jnp.tril(jnp.ones((SPAN, SPAN), dtype=bool))
    masked = jnp.where(causal[None], spatial.astype(jnp.float32), jnp.float32(0.0))
    mixed_v = jnp.einsum('gts,bsgd->btgd', masked, blocked) + spatial_shift.T[None, :, :, None]
    gated = (jax.nn.gelu(u_vals) * mixed_v.reshape(TOK, GROUPS * GROUP_DIM)).astype(jnp.bfloat16)
    delta = blocked_sum(gated, mixer_down)
    return (row_block.astype(jnp.float32) + delta).astype(jnp.bfloat16)

def reference(stream, gain_before, gain_after, proj_gate, proj_lift, proj_down, mixer_gain, mixer_u, mixer_v, layer_gain, layer_shift, spatial, spatial_shift, mixer_down):

    def one_sequence(row_block):
        first = half_step(row_block, gain_before, proj_gate, proj_lift, proj_down)
        second = token_mixer(first, mixer_gain, mixer_u, mixer_v, layer_gain, layer_shift, spatial, spatial_shift, mixer_down)
        return half_step(second, gain_after, proj_gate, proj_lift, proj_down)
    stacked = stream.reshape(stream.shape[0] // TOK, TOK, stream.shape[1])
    return lax.map(one_sequence, stacked).reshape(stream.shape)
```

```python
import jax
import jax.numpy as jnp
from jax import lax
from jax.experimental import pallas as pl
from jax.experimental.pallas import tpu as pltpu
from jax.sharding import PartitionSpec as P

MESH = pl.DeviceIdType.MESH
F32 = jnp.float32
BF16 = jnp.bfloat16
A = 2048
norm_epsilon = 1e-06
layer_epsilon = 1e-05
L, R = 0, 1
GL, DN, UV, MD = 0, 1, 2, 3
W_ROWS = (128, 448, 128, 256)
CH = 2
CROWS = 128 // CH
STEP = 16


def silu(v):
    return v / (1.0 + jnp.exp(-v))


def gelu(v):
    return 0.5 * v * (1.0 + jnp.tanh(0.7978845608028654 * (v + 0.044715 * (v * v * v))))


def dot(a, b):
    return jnp.dot(a, b, preferred_element_type=F32)


def widx(w, s, part, phase, i):
    return (((w * 2 + s) * 2 + part) * 2 + phase) * 4 + i


def kernel(
    stream, gain_b, gain_a, p_gate, p_lift, p_down, m_gain, m_u, m_v, l_gain, l_shift, spat, s_shift, m_down,
    out,
    wgl, wd, wuv, wmd, msp, sp2, prm,
    xs, po, ps, pc, pr, acc, hid, hid2, gu, lf, res, sto, sti, colm,
    w_send, w_recv, sw_send, sw_recv, ag_send, ag_recv, rs_send, rs_recv, st_send, st_recv,
):
    rep, fs, tp = lax.axis_index("rep"), lax.axis_index("fs"), lax.axis_index("tp")
    x, c = tp // 2, tp % 2
    zl, y = fs // 4, fs % 4
    z8 = rep * 4 + zl

    def dev(dx, dy, dz, dc):
        return (dz // 4, (dz % 4) * 4 + dy, dx * 2 + dc)

    sib = dev(x, y, z8, 1 - c)
    xo = (x + 1 + 2 * ((x + c) % 2)) % 4
    xt = (x + 1 + 2 * ((x + c + 1) % 2)) % 4
    partner = dev(xo, y, z8, c)
    y_plus, y_minus = dev(x, (y + 1) % 4, z8, c), dev(x, (y + 3) % 4, z8, c)
    z_plus, z_minus = dev(x, y, (z8 + 1) % 8, c), dev(x, y, (z8 + 7) % 8, c)
    swap_to = dev((x + 2) % 4, y, z8, c)
    weights = (wgl, wd, wuv, wmd)

    barrier = pltpu.get_barrier_semaphore()
    greeted = (
        sib, partner, dev(xo, y, z8, 1 - c), dev(xt, y, z8, 0), dev(xt, y, z8, 1),
        y_plus, y_minus, z_plus, z_minus, swap_to,
    )
    for other in greeted:
        pl.semaphore_signal(barrier, inc=1, device_id=other, device_id_type=MESH)

    sent = []

    def remote(src, dst, ssem, rsem, to):
        return pltpu.make_async_remote_copy(
            src_ref=src, dst_ref=dst, send_sem=ssem, recv_sem=rsem, device_id=to, device_id_type=MESH
        )

    def start(copy):
        copy.start()
        sent.append(copy)

    def region(w, s, part, phase, pos, sub):
        n = W_ROWS[w] // 2
        r0 = part * n
        if sub is not None:
            n //= 2
            r0 += sub * n
        rows = pl.ds(r0, n)
        ref = weights[w]
        if phase == 0:
            return ref.at[s, zl, pos, rows] if part == 0 else ref.at[s, pos, y, rows]
        return ref.at[s, pos, :, rows] if part == 0 else ref.at[s, :, pos, rows]

    def ring(part, phase):
        if part == phase:
            return y, y_plus, y_minus
        return zl, z_plus, z_minus

    def w_start(w, s, part, phase, i):
        me, plus, minus = ring(part, phase)
        pos = (me, me, (me + 3) % 4, (me + 1) % 4)[i]
        block = region(w, s, part, phase, pos, (None, None, 0, 1)[i])
        j = widx(w, s, part, phase, i)
        start(remote(block, block, w_send.at[j], w_recv.at[j], (plus, minus, plus, minus)[i]))

    def w_wait(w, s, part, phase, i):
        me, plus, minus = ring(part, phase)
        pos = ((me + 3) % 4, (me + 1) % 4, (me + 2) % 4, (me + 2) % 4)[i]
        block = region(w, s, part, phase, pos, (None, None, 0, 1)[i])
        j = widx(w, s, part, phase, i)
        remote(block, block, w_send.at[j], w_recv.at[j], plus).wait_recv()

    def p1(w, s):
        for part in (0, 1):
            for i in (0, 1):
                w_start(w, s, part, 0, i)

    def forward(w, s, phase):
        for part in (0, 1):
            for i in (0, 1):
                w_wait(w, s, part, phase, i)
                w_start(w, s, part, phase, i + 2)

    def p2(w, s):
        forward(w, s, 0)

    def p3(w, s):
        for part in (0, 1):
            w_wait(w, s, part, 0, 2)
            w_wait(w, s, part, 0, 3)
            for i in (0, 1):
                w_start(w, s, part, 1, i)

    def p4(w, s):
        forward(w, s, 1)

    def p5(w, s):
        for part in (0, 1):
            w_wait(w, s, part, 1, 2)
            w_wait(w, s, part, 1, 3)

    def swap(w):
        ref = weights[w]
        return remote(ref.at[0, zl, y], ref.at[1, zl, y], sw_send.at[w], sw_recv.at[w], swap_to)

    def ag_own(r, ch):
        rows = pl.ds(ch * CROWS, CROWS)
        j = r * 3 * CH + ch
        return (
            remote(xs.at[r, L, 0, rows], xs.at[r, R, 0, rows], ag_send.at[j], ag_recv.at[j], partner),
            remote(xs.at[r, L, 0, rows], xs.at[r, L, 1, rows], ag_send.at[j + CH], ag_recv.at[j + CH], sib),
        )

    def ag_fwd(r, ch):
        rows = pl.ds(ch * CROWS, CROWS)
        j = r * 3 * CH + 2 * CH + ch
        return remote(xs.at[r, R, 0, rows], xs.at[r, R, 1, rows], ag_send.at[j], ag_recv.at[j], sib)

    def ag_recv_partner(r, ch):
        rows = pl.ds(ch * CROWS, CROWS)
        j = r * 3 * CH + ch
        return remote(xs.at[r, R, 0, rows], xs.at[r, R, 0, rows], ag_send.at[j], ag_recv.at[j], partner)

    def ag_recv_sib(r, ch):
        rows = pl.ds(ch * CROWS, CROWS)
        j = r * 3 * CH + CH + ch
        return remote(xs.at[r, L, 1, rows], xs.at[r, L, 1, rows], ag_send.at[j], ag_recv.at[j], sib)

    def ag_recv_fwd(r, ch):
        rows = pl.ds(ch * CROWS, CROWS)
        j = r * 3 * CH + 2 * CH + ch
        return remote(xs.at[r, R, 1, rows], xs.at[r, R, 1, rows], ag_send.at[j], ag_recv.at[j], sib)

    def rs_d2d(r, b):
        j = r * (2 + CH) + b
        return remote(po.at[r, b], ps.at[r, b], rs_send.at[j], rs_recv.at[j], sib)

    def rs_ici(r, ch):
        rows = pl.ds(ch * CROWS, CROWS)
        j = r * (2 + CH) + 2 + ch
        return remote(pc.at[r, rows], pr.at[r, rows], rs_send.at[j], rs_recv.at[j], partner)

    def normed(rows, gain):
        factor = lax.rsqrt(jnp.mean(rows * rows, axis=1, keepdims=True) + norm_epsilon)
        return (rows * factor * gain[...]).astype(BF16)

    def ag_send_chunk(r, ch):
        for copy in ag_own(r, ch):
            start(copy)

    def ag_wait_left(r):
        for ch in range(CH):
            ag_recv_sib(r, ch).wait_recv()

    def ag_relay(r):
        for ch in range(CH):
            ag_recv_partner(r, ch).wait_recv()
            start(ag_fwd(r, ch))

    def ag_wait_right(r):
        for ch in range(CH):
            ag_recv_fwd(r, ch).wait_recv()

    wgl[0, zl, y] = jnp.concatenate(
        [
            piece
            for j in range(3)
            for piece in (p_gate[:, j * 128 : (j + 1) * 128], p_lift[:, j * 128 : (j + 1) * 128])
        ]
        + [p_gate[:, 384:448], p_lift[:, 384:448]],
        axis=1,
    )

    @pl.loop(0, 128 // STEP)
    def _(i):
        rows = pl.ds(i * STEP, STEP)
        old = stream[rows, :]
        res[rows, :] = old
        xs[0, L, 0, rows, :] = normed(old.astype(F32), gain_b)

    wd[0, zl, y] = p_down[...]
    wuv[0, zl, y] = jnp.concatenate([m_u[...], m_v[...]], axis=1)
    wmd[0, zl, y] = m_down[...]
    prm[0] = jnp.concatenate([l_gain[...], l_shift[...], s_shift[...], jnp.zeros((2, 128), F32)], axis=0)
    sp2[0] = spat[...]

    pl.semaphore_wait(barrier, len(greeted))

    p1(GL, 0)
    start(swap(GL))
    for ch in range(CH):
        ag_send_chunk(0, ch)
    p1(DN, 0)
    start(swap(DN))
    p1(UV, 0)
    start(swap(UV))
    p1(MD, 0)
    start(swap(MD))
    swap_prm = remote(prm.at[0], prm.at[1], sw_send.at[4], sw_recv.at[4], swap_to)
    swap_sp = remote(sp2.at[0], sp2.at[1], sw_send.at[5], sw_recv.at[5], swap_to)
    start(swap_prm)
    start(swap_sp)

    def batch_x(r, b):
        return xs[r, b].reshape(256, 2048)

    def up_slot(r, b, s):
        @pl.loop(0, 3)
        def _(j):
            cols = pl.ds(pl.multiple_of(j * 256, 256), 256)
            o = dot(batch_x(r, b), wgl[s, :, :, :, cols].reshape(2048, 256))
            to = pl.ds(pl.multiple_of(s * 384 + j * 128, 128), 128)
            hid[b, :, to] = (silu(o[:, :128]) * o[:, 128:]).astype(BF16)

    def up_tail(r, b):
        w = jnp.concatenate([wgl[s, :, :, :, 768:896].reshape(2048, 128) for s in (0, 1)], axis=1)
        o = dot(batch_x(r, b), w)
        t0, t1 = o[:, :128], o[:, 128:]
        low = lax.broadcasted_iota(jnp.int32, (256, 128), 1) < 64
        gate = jnp.where(low, t0, pltpu.roll(t1, 64, axis=1))
        lift = jnp.where(low, pltpu.roll(t0, 64, axis=1), t1)
        hid[b, :, 768:896] = (silu(gate) * lift).astype(BF16)

    def up(r, b):
        @pl.loop(0, 2)
        def _(s):
            up_slot(r, b, s)

        up_tail(r, b)

    def wd_cols(zz, yy):
        return jnp.concatenate(
            [wd[0, zz, yy, 0:384], wd[1, zz, yy, 0:384], wd[0, zz, yy, 384:448], wd[1, zz, yy, 384:448]], axis=0
        )

    def wmd_cols(zz, yy):
        return jnp.concatenate([wmd[0, zz, yy], wmd[1, zz, yy]], axis=0)

    def down(r, b, lhs, columns_of):
        @pl.loop(0, 8)
        def _(n):
            zz, yy = n // 2, (n % 2) * 2
            rhs = jnp.concatenate([columns_of(zz, yy), columns_of(zz, yy + 1)], axis=1)
            o = dot(lhs[b], rhs)
            cols = pl.ds(pl.multiple_of(n * 256, 256), 256)
            acc[b, :, cols] = o[:128]
            po[r, b, :, cols] = o[128:].astype(BF16)

        start(rs_d2d(r, b))

    def rs_right(r):
        rs_d2d(r, R).wait_recv()
        for ch in range(CH):

            @pl.loop(0, CROWS // STEP)
            def _(i):
                rows = pl.ds(ch * CROWS + i * STEP, STEP)
                pc[r, rows, :] = (acc[R, rows, :] + ps[r, R, rows, :].astype(F32)).astype(BF16)

            start(rs_ici(r, ch))

    def rs_left(r, coefficient, gain):
        rs_d2d(r, L).wait_recv()
        for ch in range(CH):
            rs_ici(r, ch).wait_recv()

            @pl.loop(0, CROWS // STEP)
            def _(i):
                rows = pl.ds(ch * CROWS + i * STEP, STEP)
                delta = acc[L, rows, :] + ps[r, L, rows, :].astype(F32) + pr[r, rows, :].astype(F32)
                new = (res[rows, :].astype(F32) + coefficient * delta).astype(BF16)
                if gain is None:
                    out[rows, :] = new
                else:
                    res[rows, :] = new
                    xs[r + 1, L, 0, rows, :] = normed(new.astype(F32), gain)

            if gain is not None:
                ag_send_chunk(r + 1, ch)

    def mixer_up(b):
        @pl.loop(0, 2)
        def _(s):
            to = pl.ds(pl.multiple_of(s * 256, 256), 256)
            gu[b, :, to] = gelu(dot(batch_x(1, b), wuv[s, :, :, :, 0:256].reshape(2048, 256)))
            lf[b, :, to] = gelu(dot(batch_x(1, b), wuv[s, :, :, :, 256:512].reshape(2048, 256)))

    lane = lax.broadcasted_iota(jnp.int32, (128, 128), 1)

    def stat_send():
        table = jnp.zeros((128, 128), F32)
        for q in (0, 1):
            for b in (0, 1):
                v = lf[b, q * 128 : (q + 1) * 128, :]
                mean = jnp.mean(v, axis=1, keepdims=True)
                dev2 = jnp.sum(jnp.square(v - mean), axis=1, keepdims=True)
                table = jnp.where(lane == q * 8 + b * 2, mean, table)
                table = jnp.where(lane == q * 8 + b * 2 + 1, dev2, table)
        flipped = table.T
        sto[0] = flipped[0:8]
        sto[1] = flipped[8:16]
        routes = (
            (0, 1, 0, sib),
            (1, 0, 0, sib),
            (0, 0, 1, partner),
            (0, 1, 2, dev(xo, y, z8, 1 - c)),
            (1, 0, 2, dev(xt, y, z8, 1 - c)),
            (1, 1, 1, dev(xt, y, z8, c)),
        )
        for q, dest, slot, to in routes:
            j = dest * 3 + slot
            start(remote(sto.at[q], sti.at[dest, slot], st_send.at[j], st_recv.at[j], to))

    def stat_combine():
        for dest in (0, 1):
            for slot in (0, 1, 2):
                j = dest * 3 + slot
                remote(sto.at[0], sti.at[dest, slot], st_send.at[j], st_recv.at[j], sib).wait_recv()
        rows = []
        for q in (0, 1):
            for b in (0, 1):
                parts = [(sto, q, None, b), (sti, q, 0, b), (sti, q, 1, 1 - b), (sti, q, 2, 1 - b)]
                means, devs = [], []
                for ref, qq, slot, bb in parts:
                    block = ref[qq] if slot is None else ref[qq, slot]
                    means.append(block[bb * 2 : bb * 2 + 1])
                    devs.append(block[bb * 2 + 1 : bb * 2 + 2])
                centre = (means[0] + means[1] + means[2] + means[3]) * 0.25
                spread = devs[0] + devs[1] + devs[2] + devs[3]
                for m in means:
                    spread = spread + 512.0 * jnp.square(m - centre)
                rows.append(centre)
                rows.append(lax.rsqrt(spread * (1.0 / A) + layer_epsilon))
        for s in (0, 1):
            for g in (0, 1):
                rows.append(prm[s, 4 + g : 5 + g])
        rows.append(jnp.zeros((116, 128), F32))
        colm[...] = jnp.concatenate(rows, axis=0).T

    def mixer_mid(b):
        for q in (0, 1):
            k = (q * 2 + b) * 2
            centre, factor = colm[:, k : k + 1], colm[:, k + 1 : k + 2]
            tok = pl.ds(q * 128, 128)
            for s in (0, 1):
                for g in (0, 1):
                    n = s * 2 + g
                    cols = pl.ds(n * 128, 128)
                    v = (lf[b, tok, cols] - centre) * factor * prm[s, g : g + 1] + prm[s, 2 + g : 3 + g]
                    mixed = dot(msp[n], v.astype(BF16)) + colm[:, 8 + n : 9 + n]
                    hid2[b, tok, cols] = (gu[b, tok, cols] * mixed).astype(BF16)

    p2(GL, 0)
    p3(GL, 0)
    swap(GL).wait_recv()
    p1(GL, 1)
    ag_relay(0)
    p2(GL, 1)
    p3(GL, 1)
    p2(DN, 0)
    swap(DN).wait_recv()
    p1(DN, 1)
    p4(GL, 0)
    p3(DN, 0)
    p2(DN, 1)
    p4(GL, 1)
    p3(DN, 1)
    ag_wait_left(0)
    ag_wait_right(0)
    p5(GL, 0)

    @pl.loop(0, 2)
    def _(b):
        up_slot(0, b, 0)

    p2(UV, 0)
    swap(UV).wait_recv()
    p1(UV, 1)
    p4(DN, 0)
    p3(UV, 0)
    p5(GL, 1)

    @pl.loop(0, 2)
    def _(b):
        up_slot(0, b, 1)
        up_tail(0, b)

    p2(UV, 1)
    p4(DN, 1)
    p3(UV, 1)
    p2(MD, 0)
    swap(MD).wait_recv()
    p1(MD, 1)
    p5(DN, 0)
    p5(DN, 1)
    down(0, R, hid, wd_cols)
    p4(UV, 0)
    p3(MD, 0)
    down(0, L, hid, wd_cols)
    p2(MD, 1)
    rs_right(0)
    p3(MD, 1)
    swap_prm.wait_recv()
    swap_sp.wait_recv()
    causal = lax.broadcasted_iota(jnp.int32, (128, 128), 0) >= lane
    for s in (0, 1):
        for g in (0, 1):
            msp[s * 2 + g] = jnp.where(causal, sp2[s, g].astype(F32), 0.0).astype(BF16)
    rs_left(0, 0.5, m_gain)
    p4(UV, 1)
    ag_relay(1)
    p5(UV, 0)
    p5(UV, 1)
    ag_wait_left(1)
    mixer_up(L)
    p4(MD, 0)
    ag_wait_right(1)
    mixer_up(R)
    stat_send()
    p4(MD, 1)
    stat_combine()
    mixer_mid(R)
    p5(MD, 0)
    p5(MD, 1)
    down(1, R, hid2, wmd_cols)
    mixer_mid(L)
    down(1, L, hid2, wmd_cols)
    rs_right(1)
    rs_left(1, 1.0, gain_a)
    ag_wait_left(2)
    up(2, L)
    ag_relay(2)
    ag_wait_right(2)
    up(2, R)
    down(2, R, hid, wd_cols)
    down(2, L, hid, wd_cols)
    rs_right(2)
    rs_left(2, 0.5, None)

    for copy in sent:
        copy.wait_send()


def layer(stream, gain_b, gain_a, p_gate, p_lift, p_down, m_gain, m_u, m_v, l_gain, l_shift, spat, s_shift, m_down):
    vmem = pl.BlockSpec(memory_space=pltpu.VMEM)
    dma = pltpu.SemaphoreType.DMA
    return pl.pallas_call(
        kernel,
        out_shape=jax.ShapeDtypeStruct((128, 2048), BF16),
        in_specs=[vmem] * 14,
        out_specs=vmem,
        scratch_shapes=[
            pltpu.VMEM((2, 4, 4, 128, 896), BF16),
            pltpu.VMEM((2, 4, 4, 448, 128), BF16),
            pltpu.VMEM((2, 4, 4, 128, 512), BF16),
            pltpu.VMEM((2, 4, 4, 256, 128), BF16),
            pltpu.VMEM((4, 128, 128), BF16),
            pltpu.VMEM((2, 2, 128, 128), BF16),
            pltpu.VMEM((2, 8, 128), F32),
            pltpu.VMEM((3, 2, 2, 128, 2048), BF16),
            pltpu.VMEM((3, 2, 128, 2048), BF16),
            pltpu.VMEM((3, 2, 128, 2048), BF16),
            pltpu.VMEM((3, 128, 2048), BF16),
            pltpu.VMEM((3, 128, 2048), BF16),
            pltpu.VMEM((2, 128, 2048), F32),
            pltpu.VMEM((2, 256, 896), BF16),
            pltpu.VMEM((2, 256, 512), BF16),
            pltpu.VMEM((2, 256, 512), F32),
            pltpu.VMEM((2, 256, 512), F32),
            pltpu.VMEM((128, 2048), BF16),
            pltpu.VMEM((2, 8, 128), F32),
            pltpu.VMEM((2, 3, 8, 128), F32),
            pltpu.VMEM((128, 128), F32),
            dma((128,)), dma((128,)),
            dma((6,)), dma((6,)),
            dma((9 * CH,)), dma((9 * CH,)),
            dma((3 * (2 + CH),)), dma((3 * (2 + CH),)),
            dma((6,)), dma((6,)),
        ],
        compiler_params=pltpu.CompilerParams(
            collective_id=0, has_side_effects=True, vmem_limit_bytes=58 * 1024 * 1024
        ),
    )(
        stream, gain_b.reshape(1, -1), gain_a.reshape(1, -1), p_gate, p_lift, p_down, m_gain.reshape(1, -1),
        m_u, m_v, l_gain.reshape(2, 128), l_shift.reshape(2, 128), spat, s_shift, m_down,
    )


def solution(mesh):
    placed = (
        P(("rep", "fs", "tp"), None),
        P(),
        P(),
        P("fs", "tp"),
        P("fs", "tp"),
        P("tp", "fs"),
        P(),
        P("fs", "tp"),
        P("fs", "tp"),
        P("tp"),
        P("tp"),
        P("tp", None, None),
        P("tp", None),
        P("tp", "fs"),
    )
    return jax.shard_map(
        layer, mesh=mesh, in_specs=placed, out_specs=P(("rep", "fs", "tp"), None), check_vma=False
    )
```

```python
import jax
import jax.numpy as jnp
from jax import lax
from jax.experimental import pallas as pl
from jax.experimental.pallas import tpu as pltpu
from jax.sharding import PartitionSpec as P

MESH = pl.DeviceIdType.MESH
F32 = jnp.float32
BF16 = jnp.bfloat16
A = 2048
norm_epsilon = 1e-06
layer_epsilon = 1e-05
L, R = 0, 1
GL, DN, UV, MD = 0, 1, 2, 3
W_ROWS = (128, 448, 128, 256)
CH = 2
CROWS = 128 // CH
STEP = 16


def silu(v):
    return v / (1.0 + jnp.exp(-v))


def gelu(v):
    return 0.5 * v * (1.0 + jnp.tanh(0.7978845608028654 * (v + 0.044715 * (v * v * v))))


def dot(a, b):
    return jnp.dot(a, b, preferred_element_type=F32)


def widx(w, s, part, phase, i):
    return (((w * 2 + s) * 2 + part) * 2 + phase) * 4 + i


def kernel(
    stream, gain_b, gain_a, p_gate, p_lift, p_down, m_gain, m_u, m_v, l_gain, l_shift, spat, s_shift, m_down,
    out,
    wgl, wd, wuv, wmd, msp, sp2, prm,
    xs, po, ps, pc, pr, acc, hid, hid2, gu, lf, res, sto, sti, colm,
    out_sem, w_send, w_recv, sw_send, sw_recv, ag_send, ag_recv, rs_send, rs_recv, st_send, st_recv,
):
    rep, fs, tp = lax.axis_index("rep"), lax.axis_index("fs"), lax.axis_index("tp")
    x, c = tp // 2, tp % 2
    zl, y = fs // 4, fs % 4
    z8 = rep * 4 + zl

    def dev(dx, dy, dz, dc):
        return (dz // 4, (dz % 4) * 4 + dy, dx * 2 + dc)

    sib = dev(x, y, z8, 1 - c)
    xo = (x + 1 + 2 * ((x + c) % 2)) % 4
    xt = (x + 1 + 2 * ((x + c + 1) % 2)) % 4
    partner = dev(xo, y, z8, c)
    y_plus, y_minus = dev(x, (y + 1) % 4, z8, c), dev(x, (y + 3) % 4, z8, c)
    z_plus, z_minus = dev(x, y, (z8 + 1) % 8, c), dev(x, y, (z8 + 7) % 8, c)
    swap_to = dev((x + 2) % 4, y, z8, c)
    weights = (wgl, wd, wuv, wmd)

    barrier = pltpu.get_barrier_semaphore()
    greeted = (
        sib, partner, dev(xo, y, z8, 1 - c), dev(xt, y, z8, 0), dev(xt, y, z8, 1),
        y_plus, y_minus, z_plus, z_minus, swap_to,
    )
    for other in greeted:
        pl.semaphore_signal(barrier, inc=1, device_id=other, device_id_type=MESH)

    sent = []

    def remote(src, dst, ssem, rsem, to):
        return pltpu.make_async_remote_copy(
            src_ref=src, dst_ref=dst, send_sem=ssem, recv_sem=rsem, device_id=to, device_id_type=MESH
        )

    def start(copy):
        copy.start()
        sent.append(copy)

    def region(w, s, part, phase, pos, sub):
        n = W_ROWS[w] // 2
        r0 = part * n
        if sub is not None:
            n //= 2
            r0 += sub * n
        rows = pl.ds(r0, n)
        ref = weights[w]
        if phase == 0:
            return ref.at[s, zl, pos, rows] if part == 0 else ref.at[s, pos, y, rows]
        return ref.at[s, pos, :, rows] if part == 0 else ref.at[s, :, pos, rows]

    def ring(part, phase):
        if part == phase:
            return y, y_plus, y_minus
        return zl, z_plus, z_minus

    def w_start(w, s, part, phase, i):
        me, plus, minus = ring(part, phase)
        pos = (me, me, (me + 3) % 4, (me + 1) % 4)[i]
        block = region(w, s, part, phase, pos, (None, None, 0, 1)[i])
        j = widx(w, s, part, phase, i)
        start(remote(block, block, w_send.at[j], w_recv.at[j], (plus, minus, plus, minus)[i]))

    def w_wait(w, s, part, phase, i):
        me, plus, minus = ring(part, phase)
        pos = ((me + 3) % 4, (me + 1) % 4, (me + 2) % 4, (me + 2) % 4)[i]
        block = region(w, s, part, phase, pos, (None, None, 0, 1)[i])
        j = widx(w, s, part, phase, i)
        remote(block, block, w_send.at[j], w_recv.at[j], plus).wait_recv()

    def p1(w, s):
        for part in (0, 1):
            for i in (0, 1):
                w_start(w, s, part, 0, i)

    def forward(w, s, phase):
        for part in (0, 1):
            for i in (0, 1):
                w_wait(w, s, part, phase, i)
                w_start(w, s, part, phase, i + 2)

    def p2(w, s):
        forward(w, s, 0)

    def p3(w, s):
        for part in (0, 1):
            w_wait(w, s, part, 0, 2)
            w_wait(w, s, part, 0, 3)
            for i in (0, 1):
                w_start(w, s, part, 1, i)

    def p4(w, s):
        forward(w, s, 1)

    def p5(w, s):
        for part in (0, 1):
            w_wait(w, s, part, 1, 2)
            w_wait(w, s, part, 1, 3)

    def swap(w):
        ref = weights[w]
        return remote(ref.at[0, zl, y], ref.at[1, zl, y], sw_send.at[w], sw_recv.at[w], swap_to)

    def ag_own(r, ch):
        rows = pl.ds(ch * CROWS, CROWS)
        j = r * 3 * CH + ch
        return (
            remote(xs.at[r, L, 0, rows], xs.at[r, R, 0, rows], ag_send.at[j], ag_recv.at[j], partner),
            remote(xs.at[r, L, 0, rows], xs.at[r, L, 1, rows], ag_send.at[j + CH], ag_recv.at[j + CH], sib),
        )

    def ag_fwd(r, ch):
        rows = pl.ds(ch * CROWS, CROWS)
        j = r * 3 * CH + 2 * CH + ch
        return remote(xs.at[r, R, 0, rows], xs.at[r, R, 1, rows], ag_send.at[j], ag_recv.at[j], sib)

    def ag_recv_partner(r, ch):
        rows = pl.ds(ch * CROWS, CROWS)
        j = r * 3 * CH + ch
        return remote(xs.at[r, R, 0, rows], xs.at[r, R, 0, rows], ag_send.at[j], ag_recv.at[j], partner)

    def ag_recv_sib(r, ch):
        rows = pl.ds(ch * CROWS, CROWS)
        j = r * 3 * CH + CH + ch
        return remote(xs.at[r, L, 1, rows], xs.at[r, L, 1, rows], ag_send.at[j], ag_recv.at[j], sib)

    def ag_recv_fwd(r, ch):
        rows = pl.ds(ch * CROWS, CROWS)
        j = r * 3 * CH + 2 * CH + ch
        return remote(xs.at[r, R, 1, rows], xs.at[r, R, 1, rows], ag_send.at[j], ag_recv.at[j], sib)

    def rs_d2d(r, b, half):
        j = r * 6 + b * 2 + half
        return remote(po.at[r, b, half], ps.at[r, b, half], rs_send.at[j], rs_recv.at[j], sib)

    def rs_ici(r, half):
        j = r * 6 + 4 + half
        return remote(pc.at[r, half], pr.at[r, half], rs_send.at[j], rs_recv.at[j], partner)

    def normed(rows, gain):
        factor = lax.rsqrt(jnp.mean(rows * rows, axis=1, keepdims=True) + norm_epsilon)
        return (rows * factor * gain[...]).astype(BF16)

    def ag_send_chunk(r, ch):
        for copy in ag_own(r, ch):
            start(copy)

    def ag_wait_left(r):
        for ch in range(CH):
            ag_recv_sib(r, ch).wait_recv()

    def ag_relay(r):
        for ch in range(CH):
            ag_recv_partner(r, ch).wait_recv()
            start(ag_fwd(r, ch))

    def ag_wait_right(r):
        for ch in range(CH):
            ag_recv_fwd(r, ch).wait_recv()

    wgl[0, zl, y] = jnp.concatenate(
        [
            piece
            for j in range(3)
            for piece in (p_gate[j * 128 : (j + 1) * 128], p_lift[j * 128 : (j + 1) * 128])
        ]
        + [p_gate[384:448], p_lift[384:448]],
        axis=0,
    ).T

    @pl.loop(0, 128 // STEP)
    def _(i):
        rows = pl.ds(i * STEP, STEP)
        old = stream[rows, :]
        res[rows, :] = old
        xs[0, L, 0, rows, :] = normed(old.astype(F32), gain_b)

    wd[0, zl, y] = p_down[...]
    wuv[0, zl, y] = jnp.concatenate([m_u[...], m_v[...]], axis=1)
    wmd[0, zl, y] = m_down[...]
    prm[0] = jnp.concatenate([l_gain[...], l_shift[...], s_shift[...], jnp.zeros((2, 128), F32)], axis=0)
    sp2[0] = spat[...]

    pl.semaphore_wait(barrier, len(greeted))

    swap_prm = remote(prm.at[0], prm.at[1], sw_send.at[4], sw_recv.at[4], swap_to)
    swap_sp = remote(sp2.at[0], sp2.at[1], sw_send.at[5], sw_recv.at[5], swap_to)
    p1(GL, 0)
    start(swap(GL))
    start(swap(DN))
    for ch in range(CH):
        ag_send_chunk(0, ch)
    start(swap(UV))
    start(swap(MD))
    start(swap_prm)
    start(swap_sp)

    def batch_x(r, b):
        return xs[r, b].reshape(256, 2048)

    def up_slot(r, b, s):
        @pl.loop(0, 3)
        def _(j):
            cols = pl.ds(pl.multiple_of(j * 256, 256), 256)
            o = dot(batch_x(r, b), wgl[s, :, :, :, cols].reshape(2048, 256))
            to = pl.ds(pl.multiple_of(s * 384 + j * 128, 128), 128)
            hid[b, :, to] = (silu(o[:, :128]) * o[:, 128:]).astype(BF16)

    def up_tail(r, b):
        w = jnp.concatenate([wgl[s, :, :, :, 768:896].reshape(2048, 128) for s in (0, 1)], axis=1)
        o = dot(batch_x(r, b), w)
        t0, t1 = o[:, :128], o[:, 128:]
        low = lax.broadcasted_iota(jnp.int32, (256, 128), 1) < 64
        gate = jnp.where(low, t0, pltpu.roll(t1, 64, axis=1))
        lift = jnp.where(low, pltpu.roll(t0, 64, axis=1), t1)
        hid[b, :, 768:896] = (silu(gate) * lift).astype(BF16)

    def up(r, b):
        @pl.loop(0, 2)
        def _(s):
            up_slot(r, b, s)

        up_tail(r, b)

    def wd_cols(zz, yy):
        return jnp.concatenate(
            [wd[0, zz, yy, 0:384], wd[1, zz, yy, 0:384], wd[0, zz, yy, 384:448], wd[1, zz, yy, 384:448]], axis=0
        )

    def wmd_cols(zz, yy):
        return jnp.concatenate([wmd[0, zz, yy], wmd[1, zz, yy]], axis=0)

    def down(r, b, half, lhs, columns_of):
        @pl.loop(0, 4, unroll=2)
        def _(n):
            zz, yy = half * 2 + n // 2, (n % 2) * 2
            rhs = jnp.concatenate([columns_of(zz, yy), columns_of(zz, yy + 1)], axis=1)
            o = dot(lhs[b], rhs)
            cols = pl.ds(pl.multiple_of(n * 256, 256), 256)
            acc[b, half, :, cols] = o[:128]
            po[r, b, half, :, cols] = o[128:].astype(BF16)

        start(rs_d2d(r, b, half))

    def rs_right(r, half):
        rs_d2d(r, R, half).wait_recv()

        @pl.loop(0, 128 // STEP)
        def _(i):
            rows = pl.ds(i * STEP, STEP)
            pc[r, half, rows, :] = (acc[R, half, rows, :] + ps[r, R, half, rows, :].astype(F32)).astype(BF16)

        start(rs_ici(r, half))

    def down_all(r, lhs, columns_of):
        down(r, R, 0, lhs, columns_of)
        down(r, R, 1, lhs, columns_of)
        rs_right(r, 0)
        down(r, L, 0, lhs, columns_of)
        rs_right(r, 1)
        down(r, L, 1, lhs, columns_of)

    def rs_left(r, coefficient, gain):
        for half in (0, 1):
            rs_d2d(r, L, half).wait_recv()
        for half in (0, 1):
            rs_ici(r, half).wait_recv()
        for ch in range(CH):

            @pl.loop(0, CROWS // STEP)
            def _(i):
                rows = pl.ds(ch * CROWS + i * STEP, STEP)
                delta = jnp.concatenate(
                    [
                        acc[L, half, rows, :] + ps[r, L, half, rows, :].astype(F32) + pr[r, half, rows, :].astype(F32)
                        for half in (0, 1)
                    ],
                    axis=1,
                )
                new = (res[rows, :].astype(F32) + coefficient * delta).astype(BF16)
                res[rows, :] = new
                if gain is not None:
                    xs[r + 1, L, 0, rows, :] = normed(new.astype(F32), gain)

            rows = pl.ds(ch * CROWS, CROWS)
            if gain is not None:
                ag_send_chunk(r + 1, ch)
            else:
                pltpu.make_async_copy(res.at[rows], out.at[rows], out_sem.at[ch]).start()

    def mixer_up(b):
        @pl.loop(0, 2)
        def _(s):
            to = pl.ds(pl.multiple_of(s * 256, 256), 256)
            gu[b, :, to] = gelu(dot(batch_x(1, b), wuv[s, :, :, :, 0:256].reshape(2048, 256)))
            lf[b, :, to] = gelu(dot(batch_x(1, b), wuv[s, :, :, :, 256:512].reshape(2048, 256)))

    lane = lax.broadcasted_iota(jnp.int32, (128, 128), 1)

    def stat_send():
        table = jnp.zeros((128, 128), F32)
        for q in (0, 1):
            for b in (0, 1):
                v = lf[b, q * 128 : (q + 1) * 128, :]
                mean = jnp.mean(v, axis=1, keepdims=True)
                dev2 = jnp.sum(jnp.square(v - mean), axis=1, keepdims=True)
                table = jnp.where(lane == q * 8 + b * 2, mean, table)
                table = jnp.where(lane == q * 8 + b * 2 + 1, dev2, table)
        flipped = table.T
        sto[0] = flipped[0:8]
        sto[1] = flipped[8:16]
        routes = (
            (0, 1, 0, sib),
            (1, 0, 0, sib),
            (0, 0, 1, partner),
            (0, 1, 2, dev(xo, y, z8, 1 - c)),
            (1, 0, 2, dev(xt, y, z8, 1 - c)),
            (1, 1, 1, dev(xt, y, z8, c)),
        )
        for q, dest, slot, to in routes:
            j = dest * 3 + slot
            start(remote(sto.at[q], sti.at[dest, slot], st_send.at[j], st_recv.at[j], to))

    def stat_combine():
        for dest in (0, 1):
            for slot in (0, 1, 2):
                j = dest * 3 + slot
                remote(sto.at[0], sti.at[dest, slot], st_send.at[j], st_recv.at[j], sib).wait_recv()
        rows = []
        for q in (0, 1):
            for b in (0, 1):
                parts = [(sto, q, None, b), (sti, q, 0, b), (sti, q, 1, 1 - b), (sti, q, 2, 1 - b)]
                means, devs = [], []
                for ref, qq, slot, bb in parts:
                    block = ref[qq] if slot is None else ref[qq, slot]
                    means.append(block[bb * 2 : bb * 2 + 1])
                    devs.append(block[bb * 2 + 1 : bb * 2 + 2])
                centre = (means[0] + means[1] + means[2] + means[3]) * 0.25
                spread = devs[0] + devs[1] + devs[2] + devs[3]
                for m in means:
                    spread = spread + 512.0 * jnp.square(m - centre)
                rows.append(centre)
                rows.append(lax.rsqrt(spread * (1.0 / A) + layer_epsilon))
        for s in (0, 1):
            for g in (0, 1):
                rows.append(prm[s, 4 + g : 5 + g])
        rows.append(jnp.zeros((116, 128), F32))
        colm[...] = jnp.concatenate(rows, axis=0).T

    def mixer_mid(b):
        for q in (0, 1):
            k = (q * 2 + b) * 2
            centre, factor = colm[:, k : k + 1], colm[:, k + 1 : k + 2]
            tok = pl.ds(q * 128, 128)
            for s in (0, 1):
                for g in (0, 1):
                    n = s * 2 + g
                    cols = pl.ds(n * 128, 128)
                    v = (lf[b, tok, cols] - centre) * factor * prm[s, g : g + 1] + prm[s, 2 + g : 3 + g]
                    mixed = dot(msp[n], v.astype(BF16)) + colm[:, 8 + n : 9 + n]
                    hid2[b, tok, cols] = (gu[b, tok, cols] * mixed).astype(BF16)

    p2(GL, 0)
    p1(DN, 0)
    swap(GL).wait_recv()
    p1(GL, 1)
    p3(GL, 0)
    p2(DN, 0)
    p2(GL, 1)
    swap(DN).wait_recv()
    p1(DN, 1)
    p1(UV, 0)
    p4(GL, 0)
    p3(GL, 1)
    p2(DN, 1)
    p2(UV, 0)
    swap(UV).wait_recv()
    p1(UV, 1)
    p3(DN, 0)
    ag_relay(0)
    p4(GL, 1)
    p3(DN, 1)
    ag_wait_left(0)
    ag_wait_right(0)
    p5(GL, 0)

    @pl.loop(0, 2)
    def _(b):
        up_slot(0, b, 0)

    p4(DN, 0)
    p2(UV, 1)
    p1(MD, 0)
    p5(GL, 1)

    @pl.loop(0, 2)
    def _(b):
        up_slot(0, b, 1)
        up_tail(0, b)

    p4(DN, 1)
    p3(UV, 0)
    p2(MD, 0)
    swap(MD).wait_recv()
    p1(MD, 1)
    p3(UV, 1)
    swap_prm.wait_recv()
    swap_sp.wait_recv()
    causal = lax.broadcasted_iota(jnp.int32, (128, 128), 0) >= lane
    for s in (0, 1):
        for g in (0, 1):
            msp[s * 2 + g] = jnp.where(causal, sp2[s, g].astype(F32), 0.0).astype(BF16)
    p5(DN, 0)
    p5(DN, 1)
    down_all(0, hid, wd_cols)
    p4(UV, 0)
    p3(MD, 0)
    p2(MD, 1)
    rs_left(0, 0.5, m_gain)
    p4(UV, 1)
    p3(MD, 1)
    ag_relay(1)
    p5(UV, 0)
    p5(UV, 1)
    ag_wait_left(1)
    mixer_up(L)
    p4(MD, 0)
    ag_wait_right(1)
    mixer_up(R)
    stat_send()
    p4(MD, 1)
    stat_combine()
    mixer_mid(R)
    mixer_mid(L)
    p5(MD, 0)
    p5(MD, 1)
    down_all(1, hid2, wmd_cols)
    rs_left(1, 1.0, gain_a)
    ag_wait_left(2)
    up(2, L)
    ag_relay(2)
    ag_wait_right(2)
    up(2, R)
    down_all(2, hid, wd_cols)
    rs_left(2, 0.5, None)

    for ch in range(CH):
        rows = pl.ds(ch * CROWS, CROWS)
        pltpu.make_async_copy(res.at[rows], out.at[rows], out_sem.at[ch]).wait()
    for copy in sent:
        copy.wait_send()


def layer(stream, gain_b, gain_a, p_gate, p_lift, p_down, m_gain, m_u, m_v, l_gain, l_shift, spat, s_shift, m_down):
    vmem = pl.BlockSpec(memory_space=pltpu.VMEM)
    dma = pltpu.SemaphoreType.DMA
    return pl.pallas_call(
        kernel,
        out_shape=jax.ShapeDtypeStruct((128, 2048), BF16),
        in_specs=[vmem] * 14,
        out_specs=pl.BlockSpec(memory_space=pl.ANY),
        scratch_shapes=[
            pltpu.VMEM((2, 4, 4, 128, 896), BF16),
            pltpu.VMEM((2, 4, 4, 448, 128), BF16),
            pltpu.VMEM((2, 4, 4, 128, 512), BF16),
            pltpu.VMEM((2, 4, 4, 256, 128), BF16),
            pltpu.VMEM((4, 128, 128), BF16),
            pltpu.VMEM((2, 2, 128, 128), BF16),
            pltpu.VMEM((2, 8, 128), F32),
            pltpu.VMEM((3, 2, 2, 128, 2048), BF16),
            pltpu.VMEM((3, 2, 2, 128, 1024), BF16),
            pltpu.VMEM((3, 2, 2, 128, 1024), BF16),
            pltpu.VMEM((3, 2, 128, 1024), BF16),
            pltpu.VMEM((3, 2, 128, 1024), BF16),
            pltpu.VMEM((2, 2, 128, 1024), F32),
            pltpu.VMEM((2, 256, 896), BF16),
            pltpu.VMEM((2, 256, 512), BF16),
            pltpu.VMEM((2, 256, 512), F32),
            pltpu.VMEM((2, 256, 512), F32),
            pltpu.VMEM((128, 2048), BF16),
            pltpu.VMEM((2, 8, 128), F32),
            pltpu.VMEM((2, 3, 8, 128), F32),
            pltpu.VMEM((128, 128), F32),
            dma((CH,)),
            dma((128,)), dma((128,)),
            dma((6,)), dma((6,)),
            dma((9 * CH,)), dma((9 * CH,)),
            dma((18,)), dma((18,)),
            dma((6,)), dma((6,)),
        ],
        compiler_params=pltpu.CompilerParams(
            collective_id=0, has_side_effects=True, vmem_limit_bytes=58 * 1024 * 1024
        ),
    )(
        stream, gain_b.reshape(1, -1), gain_a.reshape(1, -1), p_gate.T, p_lift.T, p_down, m_gain.reshape(1, -1),
        m_u, m_v, l_gain.reshape(2, 128), l_shift.reshape(2, 128), spat, s_shift, m_down,
    )


def solution(mesh):
    placed = (
        P(("rep", "fs", "tp"), None),
        P(),
        P(),
        P("fs", "tp"),
        P("fs", "tp"),
        P("tp", "fs"),
        P(),
        P("fs", "tp"),
        P("fs", "tp"),
        P("tp"),
        P("tp"),
        P("tp", None, None),
        P("tp", None),
        P("tp", "fs"),
    )
    return jax.shard_map(
        layer, mesh=mesh, in_specs=placed, out_specs=P(("rep", "fs", "tp"), None), check_vma=False
    )
```

```python
import jax
import jax.numpy as jnp
from jax import lax
from jax.experimental import pallas as pl
from jax.experimental.pallas import tpu as pltpu
from jax.sharding import PartitionSpec as P

MESH = pl.DeviceIdType.MESH
F32 = jnp.float32
BF16 = jnp.bfloat16
A = 2048
norm_epsilon = 1e-06
layer_epsilon = 1e-05
L, R = 0, 1
GL, DN, UV, MD = 0, 1, 2, 3
W_ROWS = (128, 448, 128, 256)
CH = 2
CROWS = 128 // CH
STEP = 16


def silu(v):
    return v / (1.0 + jnp.exp(-v))


def gelu(v):
    return 0.5 * v * (1.0 + jnp.tanh(0.7978845608028654 * (v + 0.044715 * (v * v * v))))


def dot(a, b):
    return jnp.dot(a, b, preferred_element_type=F32)


def recv_index(w, s, part, phase, i):
    return ((w * 3 + s * 2 + phase - s) * 2 + part) * 3 + min(i, 2)


def kernel(
    stream, gain_b, gain_a, p_gate, p_lift, p_down, m_gain, m_u, m_v, l_gain, l_shift, spat, s_shift, m_down,
    out,
    wgl, wd, wuv, wmd, rgl, rd, ruv, rmd, msp, sp2, prm,
    xs, po, ps, pc, pr, acc, hid, hid2, gu, lf, res, sto, sti, colm,
    w_send, w_recv, x_recv, sw_send, sw_recv, ag_send, ag_recv, rs_send, rs_recv, st_send, st_recv,
):
    rep, fs, tp = lax.axis_index("rep"), lax.axis_index("fs"), lax.axis_index("tp")
    x, c = tp // 2, tp % 2
    zl, y = fs // 4, fs % 4
    z8 = rep * 4 + zl

    def dev(dx, dy, dz, dc):
        return (dz // 4, (dz % 4) * 4 + dy, dx * 2 + dc)

    sib = dev(x, y, z8, 1 - c)
    xo = (x + 1 + 2 * ((x + c) % 2)) % 4
    xt = (x + 1 + 2 * ((x + c + 1) % 2)) % 4
    partner = dev(xo, y, z8, c)
    y_plus, y_minus = dev(x, (y + 1) % 4, z8, c), dev(x, (y + 3) % 4, z8, c)
    z_plus, z_minus = dev(x, y, (z8 + 1) % 8, c), dev(x, y, (z8 + 7) % 8, c)
    swap_to = dev((x + 2) % 4, y, z8, c)
    weights = (wgl, wd, wuv, wmd)
    relays = (rgl, rd, ruv, rmd)
    x_dirs = (dev((x + 1) % 4, y, z8, c), dev((x + 3) % 4, y, z8, c))

    barrier = pltpu.get_barrier_semaphore()
    greeted = (
        sib, partner, dev(xo, y, z8, 1 - c), dev(xt, y, z8, 0), dev(xt, y, z8, 1),
        y_plus, y_minus, z_plus, z_minus, swap_to,
    )
    for other in greeted:
        pl.semaphore_signal(barrier, inc=1, device_id=other, device_id_type=MESH)

    def remote(src, dst, ssem, rsem, to):
        return pltpu.make_async_remote_copy(
            src_ref=src, dst_ref=dst, send_sem=ssem, recv_sem=rsem, device_id=to, device_id_type=MESH
        )

    def start(copy):
        copy.start()

    def region(w, s, part, phase, pos, sub):
        n = W_ROWS[w] // 2
        r0 = part * n
        if sub is not None:
            n //= 2
            r0 += sub * n
        rows = pl.ds(r0, n)
        ref = weights[w]
        if phase == 0:
            return ref.at[s, zl, pos, rows] if part == 0 else ref.at[s, pos, y, rows]
        return ref.at[s, pos, :, rows] if part == 0 else ref.at[s, :, pos, rows]

    def ring(part, phase):
        if part == phase:
            return y, y_plus, y_minus
        return zl, z_plus, z_minus

    def w_start(w, s, part, phase, i):
        me, plus, minus = ring(part, phase)
        pos = (me, me, (me + 3) % 4, (me + 1) % 4)[i]
        block = region(w, s, part, phase, pos, (None, None, 0, 1)[i])
        j = recv_index(w, s, part, phase, i)
        start(remote(block, block, w_send.at[w * 4 + s + phase], w_recv.at[j], (plus, minus, plus, minus)[i]))

    def w_wait(w, s, part, phase, i):
        me, plus, minus = ring(part, phase)
        pos = ((me + 3) % 4, (me + 1) % 4, (me + 2) % 4)[i]
        block = region(w, s, part, phase, pos, None)
        j = recv_index(w, s, part, phase, i)
        remote(block, block, w_send.at[w * 4 + s + phase], w_recv.at[j], plus).wait_recv()

    def p1(w):
        for part in (0, 1):
            for i in (0, 1):
                w_start(w, 0, part, 0, i)

    def forward(w, s, phase):
        for part in (0, 1):
            for i in (0, 1):
                w_wait(w, s, part, phase, i)
                w_start(w, s, part, phase, i + 2)

    def p2(w):
        forward(w, 0, 0)

    def x_copy(w, part, relayed):
        me = ring(part, 1)[0]
        block = region(w, 0, part, 1, me, None)
        if relayed:
            src, dst = relays[w].at[part], region(w, 1, part, 1, me, None)
        else:
            src, dst = block, relays[w].at[part]
        return remote(src, dst, w_send.at[w * 4 + 3], x_recv.at[w * 4 + relayed * 2 + part], x_dirs[part])

    def px(w):
        for part in (0, 1):
            w_wait(w, 0, part, 0, 2)
            start(x_copy(w, part, 0))

    def xr(w):
        for part in (0, 1):
            x_copy(w, part, 0).wait_recv()
            start(x_copy(w, part, 1))

    def p3(w, s):
        for part in (0, 1):
            if s == 1:
                x_copy(w, part, 1).wait_recv()
            for i in (0, 1):
                w_start(w, s, part, 1, i)

    def p4(w, s):
        forward(w, s, 1)

    def p5(w, s):
        for part in (0, 1):
            w_wait(w, s, part, 1, 2)

    def wait_sent():
        def drained(ref, sem):
            remote(ref, ref, sem, x_recv.at[0], sib).wait_send()

        for w in range(4):
            ref = weights[w]
            drained(ref.at[0, 0, 0:3], w_send.at[w * 4])
            drained(ref.at[0, 0:3], w_send.at[w * 4 + 1])
            drained(ref.at[1, 0:3], w_send.at[w * 4 + 2])
            drained(ref.at[0, 0:2], w_send.at[w * 4 + 3])
        for r in range(3):
            drained(xs.at[r, 0], ag_send.at[r * 2])
            drained(xs.at[r, 0, 0], ag_send.at[r * 2 + 1])
            drained(po.at[r], rs_send.at[r * 2])
            drained(pc.at[r], rs_send.at[r * 2 + 1])
        drained(sti, st_send.at[0])
        swap_prm.wait_send()
        swap_sp.wait_send()

    def ag_ici(r, ch):
        rows = pl.ds(ch * CROWS, CROWS)
        return remote(
            xs.at[r, L, 0, rows], xs.at[r, R, 0, rows], ag_send.at[r * 2], ag_recv.at[r * (CH + 2) + ch], partner
        )

    def ag_d2d(r, rows):
        return remote(
            xs.at[r, L, 0, rows], xs.at[r, L, 1, rows], ag_send.at[r * 2], ag_recv.at[r * (CH + 2) + CH], sib
        )

    def ag_fwd(r, rows):
        return remote(
            xs.at[r, R, 0, rows], xs.at[r, R, 1, rows], ag_send.at[r * 2 + 1], ag_recv.at[r * (CH + 2) + CH + 1], sib
        )

    def rs_d2d(r, b, half):
        return remote(
            po.at[r, b, half], ps.at[r, b, half], rs_send.at[r * 2], rs_recv.at[r * 4 + (half if b == R else 2)], sib
        )

    def rs_ici(r, half):
        return remote(pc.at[r, half], pr.at[r, half], rs_send.at[r * 2 + 1], rs_recv.at[r * 4 + 3], partner)

    def normed(rows, gain):
        factor = lax.rsqrt(jnp.mean(rows * rows, axis=1, keepdims=True) + norm_epsilon)
        return (rows * factor * gain[...]).astype(BF16)

    def ag_send_chunk(r, ch):
        start(ag_ici(r, ch))
        start(ag_d2d(r, pl.ds(ch * CROWS, CROWS)))

    def ag_wait_left(r):
        ag_d2d(r, pl.ds(0, 128)).wait_recv()

    def ag_relay(r):
        for ch in range(CH):
            ag_ici(r, ch).wait_recv()
            start(ag_fwd(r, pl.ds(ch * CROWS, CROWS)))

    def ag_wait_right(r):
        ag_fwd(r, pl.ds(0, 128)).wait_recv()

    wgl[0, zl, y] = jnp.concatenate(
        [
            piece
            for j in range(3)
            for piece in (p_gate[j * 128 : (j + 1) * 128], p_lift[j * 128 : (j + 1) * 128])
        ]
        + [p_gate[384:448], p_lift[384:448]],
        axis=0,
    ).T

    @pl.loop(0, 128 // STEP)
    def _(i):
        rows = pl.ds(i * STEP, STEP)
        old = stream[rows, :]
        res[rows, :] = old
        xs[0, L, 0, rows, :] = normed(old.astype(F32), gain_b)

    wd[0, zl, y] = p_down[...]
    wuv[0, zl, y] = jnp.concatenate([m_u[...], m_v[...]], axis=1)
    wmd[0, zl, y] = m_down[...]
    prm[0] = jnp.concatenate([l_gain[...], l_shift[...], s_shift[...], jnp.zeros((2, 128), F32)], axis=0)
    sp2[0] = spat[...]

    pl.semaphore_wait(barrier, len(greeted))

    swap_prm = remote(prm.at[0], prm.at[1], sw_send.at[0], sw_recv.at[0], swap_to)
    swap_sp = remote(sp2.at[0], sp2.at[1], sw_send.at[1], sw_recv.at[1], swap_to)
    p1(GL)
    start(swap_prm)
    start(swap_sp)
    for ch in range(CH):
        ag_send_chunk(0, ch)

    def batch_x(r, b):
        return xs[r, b].reshape(256, 2048)

    def up_slot(r, b, s):
        @pl.loop(0, 3)
        def _(j):
            cols = pl.ds(pl.multiple_of(j * 256, 256), 256)
            o = dot(batch_x(r, b), wgl[s, :, :, :, cols].reshape(2048, 256))
            to = pl.ds(pl.multiple_of(s * 384 + j * 128, 128), 128)
            hid[b, :, to] = (silu(o[:, :128]) * o[:, 128:]).astype(BF16)

    def up_tail(r, b):
        w = jnp.concatenate([wgl[s, :, :, :, 768:896].reshape(2048, 128) for s in (0, 1)], axis=1)
        o = dot(batch_x(r, b), w)
        t0, t1 = o[:, :128], o[:, 128:]
        low = lax.broadcasted_iota(jnp.int32, (256, 128), 1) < 64
        gate = jnp.where(low, t0, pltpu.roll(t1, 64, axis=1))
        lift = jnp.where(low, pltpu.roll(t0, 64, axis=1), t1)
        hid[b, :, 768:896] = (silu(gate) * lift).astype(BF16)

    def up(r, b):
        @pl.loop(0, 2)
        def _(s):
            up_slot(r, b, s)

        up_tail(r, b)

    def wd_cols(zz, yy):
        return jnp.concatenate(
            [wd[0, zz, yy, 0:384], wd[1, zz, yy, 0:384], wd[0, zz, yy, 384:448], wd[1, zz, yy, 384:448]], axis=0
        )

    def wmd_cols(zz, yy):
        return jnp.concatenate([wmd[0, zz, yy], wmd[1, zz, yy]], axis=0)

    def down(r, b, half, lhs, columns_of):
        @pl.loop(0, 4, unroll=2)
        def _(n):
            zz, yy = half * 2 + n // 2, (n % 2) * 2
            rhs = jnp.concatenate([columns_of(zz, yy), columns_of(zz, yy + 1)], axis=1)
            o = dot(lhs[b], rhs)
            cols = pl.ds(pl.multiple_of(n * 256, 256), 256)
            acc[b, half, :, cols] = o[:128]
            po[r, b, half, :, cols] = o[128:].astype(BF16)

        start(rs_d2d(r, b, half))

    def rs_right(r, half):
        rs_d2d(r, R, half).wait_recv()

        @pl.loop(0, 128 // STEP)
        def _(i):
            rows = pl.ds(i * STEP, STEP)
            pc[r, half, rows, :] = (acc[R, half, rows, :] + ps[r, R, half, rows, :].astype(F32)).astype(BF16)

        start(rs_ici(r, half))

    def down_all(r, lhs, columns_of):
        down(r, R, 0, lhs, columns_of)
        down(r, R, 1, lhs, columns_of)
        rs_right(r, 0)
        down(r, L, 0, lhs, columns_of)
        rs_right(r, 1)
        down(r, L, 1, lhs, columns_of)

    def rs_left(r, coefficient, gain):
        remote(po.at[r, L], ps.at[r, L], rs_send.at[r * 2], rs_recv.at[r * 4 + 2], sib).wait_recv()
        remote(pc.at[r], pr.at[r], rs_send.at[r * 2 + 1], rs_recv.at[r * 4 + 3], partner).wait_recv()
        for ch in range(CH):

            @pl.loop(0, CROWS // STEP)
            def _(i):
                rows = pl.ds(ch * CROWS + i * STEP, STEP)
                delta = jnp.concatenate(
                    [
                        acc[L, half, rows, :] + ps[r, L, half, rows, :].astype(F32) + pr[r, half, rows, :].astype(F32)
                        for half in (0, 1)
                    ],
                    axis=1,
                )
                new = (res[rows, :].astype(F32) + coefficient * delta).astype(BF16)
                if gain is None:
                    out[rows, :] = new
                else:
                    res[rows, :] = new
                    xs[r + 1, L, 0, rows, :] = normed(new.astype(F32), gain)

            rows = pl.ds(ch * CROWS, CROWS)
            if gain is not None:
                ag_send_chunk(r + 1, ch)

    def mixer_up(b):
        @pl.loop(0, 2)
        def _(s):
            to = pl.ds(pl.multiple_of(s * 256, 256), 256)
            gu[b, :, to] = gelu(dot(batch_x(1, b), wuv[s, :, :, :, 0:256].reshape(2048, 256)))
            lf[b, :, to] = gelu(dot(batch_x(1, b), wuv[s, :, :, :, 256:512].reshape(2048, 256)))

    lane = lax.broadcasted_iota(jnp.int32, (128, 128), 1)

    def stat_send():
        table = jnp.zeros((128, 128), F32)
        for q in (0, 1):
            for b in (0, 1):
                v = lf[b, q * 128 : (q + 1) * 128, :]
                mean = jnp.mean(v, axis=1, keepdims=True)
                dev2 = jnp.sum(jnp.square(v - mean), axis=1, keepdims=True)
                table = jnp.where(lane == q * 8 + b * 2, mean, table)
                table = jnp.where(lane == q * 8 + b * 2 + 1, dev2, table)
        flipped = table.T
        sto[0] = flipped[0:8]
        sto[1] = flipped[8:16]
        routes = (
            (0, 1, 0, sib),
            (1, 0, 0, sib),
            (0, 0, 1, partner),
            (0, 1, 2, dev(xo, y, z8, 1 - c)),
            (1, 0, 2, dev(xt, y, z8, 1 - c)),
            (1, 1, 1, dev(xt, y, z8, c)),
        )
        for q, dest, slot, to in routes:
            start(remote(sto.at[q], sti.at[dest, slot], st_send.at[0], st_recv.at[0], to))

    def stat_combine():
        remote(sti, sti, st_send.at[0], st_recv.at[0], sib).wait_recv()
        rows = []
        for q in (0, 1):
            for b in (0, 1):
                parts = [(sto, q, None, b), (sti, q, 0, b), (sti, q, 1, 1 - b), (sti, q, 2, 1 - b)]
                means, devs = [], []
                for ref, qq, slot, bb in parts:
                    block = ref[qq] if slot is None else ref[qq, slot]
                    means.append(block[bb * 2 : bb * 2 + 1])
                    devs.append(block[bb * 2 + 1 : bb * 2 + 2])
                centre = (means[0] + means[1] + means[2] + means[3]) * 0.25
                spread = devs[0] + devs[1] + devs[2] + devs[3]
                for m in means:
                    spread = spread + 512.0 * jnp.square(m - centre)
                rows.append(centre)
                rows.append(lax.rsqrt(spread * (1.0 / A) + layer_epsilon))
        for s in (0, 1):
            for g in (0, 1):
                rows.append(prm[s, 4 + g : 5 + g])
        rows.append(jnp.zeros((116, 128), F32))
        colm[...] = jnp.concatenate(rows, axis=0).T

    def mixer_mid(b):
        for q in (0, 1):
            k = (q * 2 + b) * 2
            centre, factor = colm[:, k : k + 1], colm[:, k + 1 : k + 2]
            tok = pl.ds(q * 128, 128)
            for s in (0, 1):
                for g in (0, 1):
                    n = s * 2 + g
                    cols = pl.ds(n * 128, 128)
                    v = (lf[b, tok, cols] - centre) * factor * prm[s, g : g + 1] + prm[s, 2 + g : 3 + g]
                    mixed = dot(msp[n], v.astype(BF16)) + colm[:, 8 + n : 9 + n]
                    hid2[b, tok, cols] = (gu[b, tok, cols] * mixed).astype(BF16)

    p2(GL)
    p1(DN)
    px(GL)
    p3(GL, 0)
    p2(DN)
    p1(UV)
    p4(GL, 0)
    xr(GL)
    px(DN)
    p3(DN, 0)
    p2(UV)
    p1(MD)
    ag_relay(0)
    ag_wait_left(0)
    ag_wait_right(0)
    p5(GL, 0)

    @pl.loop(0, 2)
    def _(b):
        up_slot(0, b, 0)

    p4(DN, 0)
    p3(GL, 1)
    xr(DN)
    px(UV)
    p2(MD)
    p4(GL, 1)
    p3(DN, 1)
    px(MD)
    xr(UV)
    p5(GL, 1)

    @pl.loop(0, 2)
    def _(b):
        up_slot(0, b, 1)
        up_tail(0, b)

    p4(DN, 1)
    p3(UV, 0)
    xr(MD)
    p3(UV, 1)
    swap_prm.wait_recv()
    swap_sp.wait_recv()
    causal = lax.broadcasted_iota(jnp.int32, (128, 128), 0) >= lane
    for s in (0, 1):
        for g in (0, 1):
            msp[s * 2 + g] = jnp.where(causal, sp2[s, g].astype(F32), 0.0).astype(BF16)
    p5(DN, 0)
    p5(DN, 1)
    down_all(0, hid, wd_cols)
    p4(UV, 0)
    p3(MD, 0)
    rs_left(0, 0.5, m_gain)
    p4(UV, 1)
    p3(MD, 1)
    ag_relay(1)
    p5(UV, 0)
    p5(UV, 1)
    ag_wait_left(1)
    mixer_up(L)
    p4(MD, 0)
    ag_wait_right(1)
    mixer_up(R)
    stat_send()
    p4(MD, 1)
    stat_combine()
    mixer_mid(R)
    mixer_mid(L)
    p5(MD, 0)
    p5(MD, 1)
    down_all(1, hid2, wmd_cols)
    rs_left(1, 1.0, gain_a)
    ag_wait_left(2)
    up(2, L)
    ag_relay(2)
    ag_wait_right(2)
    up(2, R)
    down_all(2, hid, wd_cols)
    rs_left(2, 0.5, None)

    wait_sent()


def layer(stream, gain_b, gain_a, p_gate, p_lift, p_down, m_gain, m_u, m_v, l_gain, l_shift, spat, s_shift, m_down):
    vmem = pl.BlockSpec(memory_space=pltpu.VMEM)
    dma = pltpu.SemaphoreType.DMA
    return pl.pallas_call(
        kernel,
        out_shape=pltpu.VMEM((128, 2048), BF16),
        in_specs=[vmem] * 14,
        out_specs=vmem,
        scratch_shapes=[
            pltpu.VMEM((2, 4, 4, 128, 896), BF16),
            pltpu.VMEM((2, 4, 4, 448, 128), BF16),
            pltpu.VMEM((2, 4, 4, 128, 512), BF16),
            pltpu.VMEM((2, 4, 4, 256, 128), BF16),
            pltpu.VMEM((2, 4, 64, 896), BF16),
            pltpu.VMEM((2, 4, 224, 128), BF16),
            pltpu.VMEM((2, 4, 64, 512), BF16),
            pltpu.VMEM((2, 4, 128, 128), BF16),
            pltpu.VMEM((4, 128, 128), BF16),
            pltpu.VMEM((2, 2, 128, 128), BF16),
            pltpu.VMEM((2, 8, 128), F32),
            pltpu.VMEM((3, 2, 2, 128, 2048), BF16),
            pltpu.VMEM((3, 2, 2, 128, 1024), BF16),
            pltpu.VMEM((3, 2, 2, 128, 1024), BF16),
            pltpu.VMEM((3, 2, 128, 1024), BF16),
            pltpu.VMEM((3, 2, 128, 1024), BF16),
            pltpu.VMEM((2, 2, 128, 1024), F32),
            pltpu.VMEM((2, 256, 896), BF16),
            pltpu.VMEM((2, 256, 512), BF16),
            pltpu.VMEM((2, 256, 512), F32),
            pltpu.VMEM((2, 256, 512), F32),
            pltpu.VMEM((128, 2048), BF16),
            pltpu.VMEM((2, 8, 128), F32),
            pltpu.VMEM((2, 3, 8, 128), F32),
            pltpu.VMEM((128, 128), F32),
            dma((16,)), dma((72,)), dma((16,)),
            dma((2,)), dma((2,)),
            dma((6,)), dma((3 * (CH + 2),)),
            dma((6,)), dma((12,)),
            dma((1,)), dma((1,)),
        ],
        compiler_params=pltpu.CompilerParams(
            collective_id=0, has_side_effects=True, vmem_limit_bytes=58 * 1024 * 1024
        ),
    )(
        stream, gain_b.reshape(1, -1), gain_a.reshape(1, -1), p_gate.T, p_lift.T, p_down, m_gain.reshape(1, -1),
        m_u, m_v, l_gain.reshape(2, 128), l_shift.reshape(2, 128), spat, s_shift, m_down,
    )


def solution(mesh):
    placed = (
        P(("rep", "fs", "tp"), None),
        P(),
        P(),
        P("fs", "tp"),
        P("fs", "tp"),
        P("tp", "fs"),
        P(),
        P("fs", "tp"),
        P("fs", "tp"),
        P("tp"),
        P("tp"),
        P("tp", None, None),
        P("tp", None),
        P("tp", "fs"),
    )
    return jax.shard_map(
        layer, mesh=mesh, in_specs=placed, out_specs=P(("rep", "fs", "tp"), None), check_vma=False
    )
```

```python
import jax
import jax.numpy as jnp
from jax import lax
from jax.experimental import pallas as pl
from jax.experimental.pallas import tpu as pltpu
from jax.sharding import PartitionSpec as P

MESH = pl.DeviceIdType.MESH
F32 = jnp.float32
BF16 = jnp.bfloat16
A = 2048
norm_epsilon = 1e-06
layer_epsilon = 1e-05
L, R = 0, 1
GL, DN, UV, MD = 0, 1, 2, 3
W_ROWS = (128, 448, 128, 256)
CH = 2
CROWS = 128 // CH
STEP = 16


def silu(v):
    return v / (1.0 + jnp.exp(-v))


def gelu(v):
    return 0.5 * v * (1.0 + jnp.tanh(0.7978845608028654 * (v + 0.044715 * (v * v * v))))


def dot(a, b):
    return jnp.dot(a, b, preferred_element_type=F32)


def recv_index(w, s, part, phase, i):
    return ((w * 3 + s * 2 + phase - s) * 2 + part) * 3 + min(i, 2)


def kernel(
    stream, h_gain_b, h_gain_a, p_gate, p_lift, p_down, h_gain_m, m_u, m_v, l_gain, l_shift, spat, s_shift, m_down,
    out,
    wgl, wd, wuv, wmd, rgl, rd, ruv, rmd, gate_lift, gain_b, gain_a, m_gain, small, msp, sp2, prm,
    xs, po, ps, pc, pr, acc, hid, hid2, gu, lf, res, sto, sti, colm,
    in_sem, w_send, w_recv, x_recv, sw_send, sw_recv, ag_send, ag_recv, rs_send, rs_recv, st_send, st_recv,
):
    rep, fs, tp = lax.axis_index("rep"), lax.axis_index("fs"), lax.axis_index("tp")
    x, c = tp // 2, tp % 2
    zl, y = fs // 4, fs % 4
    z8 = rep * 4 + zl

    def dev(dx, dy, dz, dc):
        return (dz // 4, (dz % 4) * 4 + dy, dx * 2 + dc)

    sib = dev(x, y, z8, 1 - c)
    xo = (x + 1 + 2 * ((x + c) % 2)) % 4
    xt = (x + 1 + 2 * ((x + c + 1) % 2)) % 4
    partner = dev(xo, y, z8, c)
    y_plus, y_minus = dev(x, (y + 1) % 4, z8, c), dev(x, (y + 3) % 4, z8, c)
    z_plus, z_minus = dev(x, y, (z8 + 1) % 8, c), dev(x, y, (z8 + 7) % 8, c)
    swap_to = dev((x + 2) % 4, y, z8, c)
    weights = (wgl, wd, wuv, wmd)
    relays = (rgl, rd, ruv, rmd)
    x_dirs = (dev((x + 1) % 4, y, z8, c), dev((x + 3) % 4, y, z8, c))

    barrier = pltpu.get_barrier_semaphore()
    greeted = (
        sib, partner, dev(xo, y, z8, 1 - c), dev(xt, y, z8, 0), dev(xt, y, z8, 1),
        y_plus, y_minus, z_plus, z_minus, swap_to,
    )
    for other in greeted:
        pl.semaphore_signal(barrier, inc=1, device_id=other, device_id_type=MESH)

    def remote(src, dst, ssem, rsem, to):
        return pltpu.make_async_remote_copy(
            src_ref=src, dst_ref=dst, send_sem=ssem, recv_sem=rsem, device_id=to, device_id_type=MESH
        )

    def start(copy):
        copy.start()

    loads = [
        pltpu.make_async_copy(src, dst, in_sem.at[i])
        for i, (src, dst) in enumerate(
            (
                (p_down, wd.at[0, zl, y]),
                (p_gate, gate_lift.at[0]),
                (p_lift, gate_lift.at[1]),
                (stream, res),
                (h_gain_b, gain_b),
                (m_u, wuv.at[0, zl, y, :, pl.ds(0, 256)]),
                (m_v, wuv.at[0, zl, y, :, pl.ds(256, 256)]),
                (m_down, wmd.at[0, zl, y]),
                (l_gain, small.at[0]),
                (l_shift, small.at[1]),
                (s_shift, small.at[2]),
                (spat, sp2.at[0]),
                (h_gain_m, m_gain),
                (h_gain_a, gain_a),
            )
        )
    ]
    for load in loads:
        load.start()

    def region(w, s, part, phase, pos, sub):
        n = W_ROWS[w] // 2
        r0 = part * n
        if sub is not None:
            n //= 2
            r0 += sub * n
        rows = pl.ds(r0, n)
        ref = weights[w]
        if phase == 0:
            return ref.at[s, zl, pos, rows] if part == 0 else ref.at[s, pos, y, rows]
        return ref.at[s, pos, :, rows] if part == 0 else ref.at[s, :, pos, rows]

    def ring(part, phase):
        if part == phase:
            return y, y_plus, y_minus
        return zl, z_plus, z_minus

    def w_start(w, s, part, phase, i):
        me, plus, minus = ring(part, phase)
        pos = (me, me, (me + 3) % 4, (me + 1) % 4)[i]
        block = region(w, s, part, phase, pos, (None, None, 0, 1)[i])
        j = recv_index(w, s, part, phase, i)
        start(remote(block, block, w_send.at[w * 4 + s + phase], w_recv.at[j], (plus, minus, plus, minus)[i]))

    def w_wait(w, s, part, phase, i):
        me, plus, minus = ring(part, phase)
        pos = ((me + 3) % 4, (me + 1) % 4, (me + 2) % 4)[i]
        block = region(w, s, part, phase, pos, None)
        j = recv_index(w, s, part, phase, i)
        remote(block, block, w_send.at[w * 4 + s + phase], w_recv.at[j], plus).wait_recv()

    def p1(w):
        for part in (0, 1):
            for i in (0, 1):
                w_start(w, 0, part, 0, i)

    def forward(w, s, phase):
        for part in (0, 1):
            for i in (0, 1):
                w_wait(w, s, part, phase, i)
                w_start(w, s, part, phase, i + 2)

    def p2(w):
        forward(w, 0, 0)

    def x_copy(w, part, relayed):
        me = ring(part, 1)[0]
        block = region(w, 0, part, 1, me, None)
        if relayed:
            src, dst = relays[w].at[part], region(w, 1, part, 1, me, None)
        else:
            src, dst = block, relays[w].at[part]
        return remote(src, dst, w_send.at[w * 4 + 3], x_recv.at[w * 4 + relayed * 2 + part], x_dirs[part])

    def ready(w):
        for part in (0, 1):
            w_wait(w, 0, part, 0, 2)

    def x1(w):
        for part in (0, 1):
            start(x_copy(w, part, 0))

    def xr(w):
        for part in (0, 1):
            x_copy(w, part, 0).wait_recv()
            start(x_copy(w, part, 1))

    def p3(w, s):
        for part in (0, 1):
            if s == 1:
                x_copy(w, part, 1).wait_recv()
            for i in (0, 1):
                w_start(w, s, part, 1, i)

    def p4(w, s):
        forward(w, s, 1)

    def p5(w, s):
        for part in (0, 1):
            w_wait(w, s, part, 1, 2)

    def wait_sent():
        def drained(ref, sem):
            remote(ref, ref, sem, x_recv.at[0], sib).wait_send()

        for w in range(4):
            ref = weights[w]
            drained(ref.at[0, 0, 0:3], w_send.at[w * 4])
            drained(ref.at[0, 0:3], w_send.at[w * 4 + 1])
            drained(ref.at[1, 0:3], w_send.at[w * 4 + 2])
            drained(ref.at[0, 0:2], w_send.at[w * 4 + 3])
        for r in range(3):
            drained(xs.at[r, 0], ag_send.at[r * 2])
            drained(xs.at[r, 0, 0], ag_send.at[r * 2 + 1])
            drained(po.at[r], rs_send.at[r * 2])
            drained(pc.at[r], rs_send.at[r * 2 + 1])
        drained(sti, st_send.at[0])
        swap_prm.wait_send()
        swap_sp.wait_send()

    def ag_ici(r, ch):
        rows = pl.ds(ch * CROWS, CROWS)
        return remote(
            xs.at[r, L, 0, rows], xs.at[r, R, 0, rows], ag_send.at[r * 2], ag_recv.at[r * (CH + 2) + ch], partner
        )

    def ag_d2d(r, rows):
        return remote(
            xs.at[r, L, 0, rows], xs.at[r, L, 1, rows], ag_send.at[r * 2], ag_recv.at[r * (CH + 2) + CH], sib
        )

    def ag_fwd(r, rows):
        return remote(
            xs.at[r, R, 0, rows], xs.at[r, R, 1, rows], ag_send.at[r * 2 + 1], ag_recv.at[r * (CH + 2) + CH + 1], sib
        )

    def rs_d2d(r, b, half):
        return remote(
            po.at[r, b, half], ps.at[r, b, half], rs_send.at[r * 2], rs_recv.at[r * 4 + (half if b == R else 2)], sib
        )

    def rs_ici(r, half):
        return remote(pc.at[r, half], pr.at[r, half], rs_send.at[r * 2 + 1], rs_recv.at[r * 4 + 3], partner)

    def normed(rows, gain):
        factor = lax.rsqrt(jnp.mean(rows * rows, axis=1, keepdims=True) + norm_epsilon)
        return (rows * factor * gain[...]).astype(BF16)

    def ag_send_chunk(r, ch):
        start(ag_ici(r, ch))
        start(ag_d2d(r, pl.ds(ch * CROWS, CROWS)))

    def ag_wait_left(r):
        ag_d2d(r, pl.ds(0, 128)).wait_recv()

    def ag_relay(r, chunks=range(CH)):
        for ch in chunks:
            ag_ici(r, ch).wait_recv()
            start(ag_fwd(r, pl.ds(ch * CROWS, CROWS)))

    def ag_wait_right(r):
        ag_fwd(r, pl.ds(0, 128)).wait_recv()

    loads[0].wait()
    pl.semaphore_wait(barrier, len(greeted))
    p1(DN)
    loads[1].wait()
    loads[2].wait()
    wgl[0, zl, y] = jnp.concatenate(
        [gate_lift[half, j * 128 : (j + 1) * 128] for j in range(3) for half in (0, 1)]
        + [gate_lift[half, 384:448] for half in (0, 1)],
        axis=0,
    ).T
    p1(GL)
    for load in loads[3:]:
        load.wait()

    @pl.loop(0, 128 // STEP)
    def _(i):
        rows = pl.ds(i * STEP, STEP)
        xs[0, L, 0, rows, :] = normed(res[rows, :].astype(F32), gain_b)

    prm[0] = jnp.concatenate([small[0], small[1], small[2], jnp.zeros((2, 128), F32)], axis=0)
    swap_prm = remote(prm.at[0], prm.at[1], sw_send.at[0], sw_recv.at[0], swap_to)
    swap_sp = remote(sp2.at[0], sp2.at[1], sw_send.at[1], sw_recv.at[1], swap_to)
    for ch in range(CH):
        ag_send_chunk(0, ch)
    start(swap_prm)
    start(swap_sp)

    def batch_x(r, b):
        return xs[r, b].reshape(256, 2048)

    def up_slot(r, b, s):
        o = dot(batch_x(r, b), wgl[s, :, :, :, 0:768].reshape(2048, 768))
        for j in range(3):
            to = pl.ds(pl.multiple_of(s * 384 + j * 128, 128), 128)
            hid[b, :, to] = (silu(o[:, j * 256 : j * 256 + 128]) * o[:, j * 256 + 128 : j * 256 + 256]).astype(BF16)

    def up_tail(r, b):
        w = jnp.concatenate([wgl[s, :, :, :, 768:896].reshape(2048, 128) for s in (0, 1)], axis=1)
        o = dot(batch_x(r, b), w)
        t0, t1 = o[:, :128], o[:, 128:]
        low = lax.broadcasted_iota(jnp.int32, (256, 128), 1) < 64
        gate = jnp.where(low, t0, pltpu.roll(t1, 64, axis=1))
        lift = jnp.where(low, pltpu.roll(t0, 64, axis=1), t1)
        hid[b, :, 768:896] = (silu(gate) * lift).astype(BF16)

    def up(r, b):
        @pl.loop(0, 2)
        def _(s):
            up_slot(r, b, s)

        up_tail(r, b)

    def wd_cols(zz, yy):
        return jnp.concatenate(
            [wd[0, zz, yy, 0:384], wd[1, zz, yy, 0:384], wd[0, zz, yy, 384:448], wd[1, zz, yy, 384:448]], axis=0
        )

    def wmd_cols(zz, yy):
        return jnp.concatenate([wmd[0, zz, yy], wmd[1, zz, yy]], axis=0)

    def down(r, b, half, lhs, columns_of):
        rhs = jnp.concatenate([columns_of(half * 2 + n // 4, n % 4) for n in range(8)], axis=1)
        o = dot(lhs[b], rhs)
        acc[b, half] = o[:128]
        po[r, b, half] = o[128:].astype(BF16)
        start(rs_d2d(r, b, half))

    def rs_right(r, half):
        rs_d2d(r, R, half).wait_recv()

        @pl.loop(0, 128 // STEP)
        def _(i):
            rows = pl.ds(i * STEP, STEP)
            pc[r, half, rows, :] = (acc[R, half, rows, :] + ps[r, R, half, rows, :].astype(F32)).astype(BF16)

        start(rs_ici(r, half))

    def down_all(r, lhs, columns_of, between=None):
        down(r, R, 0, lhs, columns_of)
        down(r, R, 1, lhs, columns_of)
        rs_right(r, 0)
        if between is not None:
            between()
            rs_right(r, 1)
        down(r, L, 0, lhs, columns_of)
        if between is None:
            rs_right(r, 1)
        down(r, L, 1, lhs, columns_of)

    def rs_left(r, coefficient, gain):
        remote(po.at[r, L], ps.at[r, L], rs_send.at[r * 2], rs_recv.at[r * 4 + 2], sib).wait_recv()
        remote(pc.at[r], pr.at[r], rs_send.at[r * 2 + 1], rs_recv.at[r * 4 + 3], partner).wait_recv()
        for ch in range(CH):

            @pl.loop(0, CROWS // STEP)
            def _(i):
                rows = pl.ds(ch * CROWS + i * STEP, STEP)
                delta = jnp.concatenate(
                    [
                        acc[L, half, rows, :] + ps[r, L, half, rows, :].astype(F32) + pr[r, half, rows, :].astype(F32)
                        for half in (0, 1)
                    ],
                    axis=1,
                )
                new = (res[rows, :].astype(F32) + coefficient * delta).astype(BF16)
                if gain is None:
                    out[rows, :] = new
                else:
                    res[rows, :] = new
                    xs[r + 1, L, 0, rows, :] = normed(new.astype(F32), gain)

            rows = pl.ds(ch * CROWS, CROWS)
            if gain is not None:
                ag_send_chunk(r + 1, ch)

    def mixer_up(b):
        @pl.loop(0, 2)
        def _(s):
            to = pl.ds(pl.multiple_of(s * 256, 256), 256)
            o = dot(batch_x(1, b), wuv[s].reshape(2048, 512))
            gu[b, :, to] = gelu(o[:, :256])
            lf[b, :, to] = gelu(o[:, 256:])

    lane = lax.broadcasted_iota(jnp.int32, (128, 128), 1)

    def stat_send():
        table = jnp.zeros((128, 128), F32)
        for q in (0, 1):
            for b in (0, 1):
                v = lf[b, q * 128 : (q + 1) * 128, :]
                mean = jnp.mean(v, axis=1, keepdims=True)
                dev2 = jnp.sum(jnp.square(v - mean), axis=1, keepdims=True)
                table = jnp.where(lane == q * 8 + b * 2, mean, table)
                table = jnp.where(lane == q * 8 + b * 2 + 1, dev2, table)
        flipped = table.T
        sto[0] = flipped[0:8]
        sto[1] = flipped[8:16]
        routes = (
            (0, 1, 0, sib),
            (1, 0, 0, sib),
            (0, 0, 1, partner),
            (0, 1, 2, dev(xo, y, z8, 1 - c)),
            (1, 0, 2, dev(xt, y, z8, 1 - c)),
            (1, 1, 1, dev(xt, y, z8, c)),
        )
        for q, dest, slot, to in routes:
            start(remote(sto.at[q], sti.at[dest, slot], st_send.at[0], st_recv.at[0], to))

    def stat_combine():
        remote(sti, sti, st_send.at[0], st_recv.at[0], sib).wait_recv()
        rows = []
        for q in (0, 1):
            for b in (0, 1):
                parts = [(sto, q, None, b), (sti, q, 0, b), (sti, q, 1, 1 - b), (sti, q, 2, 1 - b)]
                means, devs = [], []
                for ref, qq, slot, bb in parts:
                    block = ref[qq] if slot is None else ref[qq, slot]
                    means.append(block[bb * 2 : bb * 2 + 1])
                    devs.append(block[bb * 2 + 1 : bb * 2 + 2])
                centre = (means[0] + means[1] + means[2] + means[3]) * 0.25
                spread = devs[0] + devs[1] + devs[2] + devs[3]
                for m in means:
                    spread = spread + 512.0 * jnp.square(m - centre)
                rows.append(centre)
                rows.append(lax.rsqrt(spread * (1.0 / A) + layer_epsilon))
        for s in (0, 1):
            for g in (0, 1):
                rows.append(prm[s, 4 + g : 5 + g])
        rows.append(jnp.zeros((116, 128), F32))
        colm[...] = jnp.concatenate(rows, axis=0).T

    def mixer_mid(b):
        for q in (0, 1):
            k = (q * 2 + b) * 2
            centre, factor = colm[:, k : k + 1], colm[:, k + 1 : k + 2]
            tok = pl.ds(q * 128, 128)
            for s in (0, 1):
                for g in (0, 1):
                    n = s * 2 + g
                    cols = pl.ds(n * 128, 128)
                    v = (lf[b, tok, cols] - centre) * factor * prm[s, g : g + 1] + prm[s, 2 + g : 3 + g]
                    mixed = dot(msp[n], v.astype(BF16)) + colm[:, 8 + n : 9 + n]
                    hid2[b, tok, cols] = (gu[b, tok, cols] * mixed).astype(BF16)

    p2(DN)
    p2(GL)
    p1(UV)
    ready(DN)
    p3(DN, 0)
    ready(GL)
    x1(GL)
    p3(GL, 0)
    p2(UV)
    p1(MD)
    p4(DN, 0)
    xr(GL)
    x1(DN)
    p4(GL, 0)
    ready(UV)
    p2(MD)
    ag_relay(0)
    ag_wait_left(0)
    ag_wait_right(0)
    p3(GL, 1)
    p5(GL, 0)

    @pl.loop(0, 2)
    def _(b):
        up_slot(0, b, 0)

    xr(DN)
    x1(UV)
    ready(MD)
    p4(GL, 1)
    p3(DN, 1)
    xr(UV)
    x1(MD)
    p5(GL, 1)
    up_slot(0, L, 1)
    up_tail(0, L)
    p4(DN, 1)
    p3(UV, 0)
    up_slot(0, R, 1)
    up_tail(0, R)
    xr(MD)
    p5(DN, 0)
    p5(DN, 1)
    p3(UV, 1)
    down_all(0, hid, wd_cols)
    p4(UV, 0)
    p3(MD, 0)
    swap_prm.wait_recv()
    swap_sp.wait_recv()
    causal = lax.broadcasted_iota(jnp.int32, (128, 128), 0) >= lane
    for s in (0, 1):
        for g in (0, 1):
            msp[s * 2 + g] = jnp.where(causal, sp2[s, g].astype(F32), 0.0).astype(BF16)
    rs_left(0, 0.5, m_gain)
    p4(UV, 1)
    p3(MD, 1)
    p4(MD, 0)
    ag_relay(1, (0,))
    p5(UV, 0)
    p5(UV, 1)
    ag_wait_left(1)
    mixer_up(L)
    ag_relay(1, (1,))
    p4(MD, 1)
    ag_wait_right(1)
    mixer_up(R)
    stat_send()
    p5(MD, 0)
    p5(MD, 1)
    stat_combine()
    mixer_mid(R)
    down_all(1, hid2, wmd_cols, lambda: mixer_mid(L))
    rs_left(1, 1.0, gain_a)
    ag_wait_left(2)
    up(2, L)
    ag_relay(2)
    ag_wait_right(2)
    up(2, R)
    down_all(2, hid, wd_cols)
    rs_left(2, 0.5, None)
    wait_sent()


def layer(stream, gain_b, gain_a, p_gate, p_lift, p_down, m_gain, m_u, m_v, l_gain, l_shift, spat, s_shift, m_down):
    dma = pltpu.SemaphoreType.DMA
    return pl.pallas_call(
        kernel,
        out_shape=pltpu.VMEM((128, 2048), BF16),
        in_specs=[pl.BlockSpec(memory_space=pl.ANY)] * 14,
        out_specs=pl.BlockSpec(memory_space=pltpu.VMEM),
        scratch_shapes=[
            pltpu.VMEM((2, 4, 4, 128, 896), BF16),
            pltpu.VMEM((2, 4, 4, 448, 128), BF16),
            pltpu.VMEM((2, 4, 4, 128, 512), BF16),
            pltpu.VMEM((2, 4, 4, 256, 128), BF16),
            pltpu.VMEM((2, 4, 64, 896), BF16),
            pltpu.VMEM((2, 4, 224, 128), BF16),
            pltpu.VMEM((2, 4, 64, 512), BF16),
            pltpu.VMEM((2, 4, 128, 128), BF16),
            pltpu.VMEM((2, 448, 128), BF16),
            pltpu.VMEM((1, 2048), F32),
            pltpu.VMEM((1, 2048), F32),
            pltpu.VMEM((1, 2048), F32),
            pltpu.VMEM((3, 2, 128), F32),
            pltpu.VMEM((4, 128, 128), BF16),
            pltpu.VMEM((2, 2, 128, 128), BF16),
            pltpu.VMEM((2, 8, 128), F32),
            pltpu.VMEM((3, 2, 2, 128, 2048), BF16),
            pltpu.VMEM((3, 2, 2, 128, 1024), BF16),
            pltpu.VMEM((3, 2, 2, 128, 1024), BF16),
            pltpu.VMEM((3, 2, 128, 1024), BF16),
            pltpu.VMEM((3, 2, 128, 1024), BF16),
            pltpu.VMEM((2, 2, 128, 1024), F32),
            pltpu.VMEM((2, 256, 896), BF16),
            pltpu.VMEM((2, 256, 512), BF16),
            pltpu.VMEM((2, 256, 512), F32),
            pltpu.VMEM((2, 256, 512), F32),
            pltpu.VMEM((128, 2048), BF16),
            pltpu.VMEM((2, 8, 128), F32),
            pltpu.VMEM((2, 3, 8, 128), F32),
            pltpu.VMEM((128, 128), F32),
            dma((14,)),
            dma((16,)), dma((72,)), dma((16,)),
            dma((2,)), dma((2,)),
            dma((6,)), dma((3 * (CH + 2),)),
            dma((6,)), dma((12,)),
            dma((1,)), dma((1,)),
        ],
        compiler_params=pltpu.CompilerParams(
            collective_id=0, has_side_effects=True, vmem_limit_bytes=58 * 1024 * 1024
        ),
    )(
        stream, gain_b.reshape(1, -1), gain_a.reshape(1, -1), p_gate.T, p_lift.T, p_down, m_gain.reshape(1, -1),
        m_u, m_v, l_gain.reshape(2, 128), l_shift.reshape(2, 128), spat, s_shift, m_down,
    )


def solution(mesh):
    placed = (
        P(("rep", "fs", "tp"), None),
        P(),
        P(),
        P("fs", "tp"),
        P("fs", "tp"),
        P("tp", "fs"),
        P(),
        P("fs", "tp"),
        P("fs", "tp"),
        P("tp"),
        P("tp"),
        P("tp", None, None),
        P("tp", None),
        P("tp", "fs"),
    )
    return jax.shard_map(
        layer, mesh=mesh, in_specs=placed, out_specs=P(("rep", "fs", "tp"), None), check_vma=False
    )
```

```python
import jax
import jax.numpy as jnp
from jax import lax
from jax.experimental import pallas as pl
from jax.experimental.pallas import tpu as pltpu
from jax.sharding import PartitionSpec as P

MESH = pl.DeviceIdType.MESH
F32 = jnp.float32
BF16 = jnp.bfloat16
A = 2048
norm_epsilon = 1e-06
layer_epsilon = 1e-05
L, R = 0, 1
GL, DN, UV, MD = 0, 1, 2, 3
W_ROWS = (128, 448, 128, 256)
CH = 2
CROWS = 128 // CH
STEP = 16


def silu(v):
    return v / (1.0 + jnp.exp(-v))


def gelu(v):
    return 0.5 * v * (1.0 + jnp.tanh(0.7978845608028654 * (v + 0.044715 * (v * v * v))))


def dot(a, b):
    return jnp.dot(a, b, preferred_element_type=F32)


def recv_index(w, s, part, phase, i):
    return ((w * 3 + s * 2 + phase - s) * 2 + part) * 3 + min(i, 2)


def kernel(
    stream, h_gain_b, h_gain_a, p_gate, p_lift, p_down, h_gain_m, m_u, m_v, l_gain, l_shift, spat, s_shift, m_down,
    out,
    wgl, wd, wuv, wmd, rgl, rd, ruv, rmd, gate_lift, gain_b, gain_a, m_gain, small, msp, sp2, prm,
    xs, po, ps, pc, pr, acc, hid, hid2, gu, lf, res, sto, sti, colm,
    in_sem, w_send, w_recv, x_recv, sw_send, sw_recv, ag_send, ag_recv, rs_send, rs_recv, st_send, st_recv,
):
    rep, fs, tp = lax.axis_index("rep"), lax.axis_index("fs"), lax.axis_index("tp")
    x, c = tp // 2, tp % 2
    zl, y = fs // 4, fs % 4
    z8 = rep * 4 + zl

    def dev(dx, dy, dz, dc):
        return (dz // 4, (dz % 4) * 4 + dy, dx * 2 + dc)

    sib = dev(x, y, z8, 1 - c)
    xo = (x + 1 + 2 * ((x + c) % 2)) % 4
    xt = (x + 1 + 2 * ((x + c + 1) % 2)) % 4
    partner = dev(xo, y, z8, c)
    y_plus, y_minus = dev(x, (y + 1) % 4, z8, c), dev(x, (y + 3) % 4, z8, c)
    z_plus, z_minus = dev(x, y, (z8 + 1) % 8, c), dev(x, y, (z8 + 7) % 8, c)
    swap_to = dev((x + 2) % 4, y, z8, c)
    weights = (wgl, wd, wuv, wmd)
    relays = (rgl, rd, ruv, rmd)
    x_dirs = (dev((x + 1) % 4, y, z8, c), dev((x + 3) % 4, y, z8, c))

    barrier = pltpu.get_barrier_semaphore()
    greeted = (
        sib, partner, dev(xo, y, z8, 1 - c), dev(xt, y, z8, 0), dev(xt, y, z8, 1),
        y_plus, y_minus, z_plus, z_minus, swap_to,
    )
    for other in greeted:
        pl.semaphore_signal(barrier, inc=1, device_id=other, device_id_type=MESH)

    def remote(src, dst, ssem, rsem, to):
        return pltpu.make_async_remote_copy(
            src_ref=src, dst_ref=dst, send_sem=ssem, recv_sem=rsem, device_id=to, device_id_type=MESH
        )

    def start(copy):
        copy.start()

    loads = [
        pltpu.make_async_copy(src, dst, in_sem.at[i])
        for i, (src, dst) in enumerate(
            (
                (p_down, wd.at[0, zl, y]),
                (p_gate, gate_lift.at[0]),
                (p_lift, gate_lift.at[1]),
                (stream.at[pl.ds(0, CROWS)], res.at[0]),
                (stream.at[pl.ds(CROWS, CROWS)], res.at[1]),
                (h_gain_b, gain_b),
                (m_u, wuv.at[0, zl, y, :, pl.ds(0, 256)]),
                (m_v, wuv.at[0, zl, y, :, pl.ds(256, 256)]),
                (m_down, wmd.at[0, zl, y]),
                (l_gain, small.at[0]),
                (l_shift, small.at[1]),
                (s_shift, small.at[2]),
                (spat, sp2.at[0]),
                (h_gain_m, m_gain),
                (h_gain_a, gain_a),
            )
        )
    ]
    for load in loads:
        load.start()

    def region(w, s, part, phase, pos, sub):
        n = W_ROWS[w] // 2
        r0 = part * n
        if sub is not None:
            n //= 2
            r0 += sub * n
        rows = pl.ds(r0, n)
        ref = weights[w]
        if phase == 0:
            return ref.at[s, zl, pos, rows] if part == 0 else ref.at[s, pos, y, rows]
        return ref.at[s, pos, :, rows] if part == 0 else ref.at[s, :, pos, rows]

    def ring(part, phase):
        if part == phase:
            return y, y_plus, y_minus
        return zl, z_plus, z_minus

    def w_start(w, s, part, phase, i):
        me, plus, minus = ring(part, phase)
        pos = (me, me, (me + 3) % 4, (me + 1) % 4)[i]
        block = region(w, s, part, phase, pos, (None, None, 0, 1)[i])
        j = recv_index(w, s, part, phase, i)
        start(remote(block, block, w_send.at[w * 4 + s + phase], w_recv.at[j], (plus, minus, plus, minus)[i]))

    def w_wait(w, s, part, phase, i):
        me, plus, minus = ring(part, phase)
        pos = ((me + 3) % 4, (me + 1) % 4, (me + 2) % 4)[i]
        block = region(w, s, part, phase, pos, None)
        j = recv_index(w, s, part, phase, i)
        remote(block, block, w_send.at[w * 4 + s + phase], w_recv.at[j], plus).wait_recv()

    def p1(w):
        for part in (0, 1):
            for i in (0, 1):
                w_start(w, 0, part, 0, i)

    def forward(w, s, phase):
        for part in (0, 1):
            for i in (0, 1):
                w_wait(w, s, part, phase, i)
                w_start(w, s, part, phase, i + 2)

    def p2(w):
        forward(w, 0, 0)

    def x_copy(w, part, relayed):
        me = ring(part, 1)[0]
        block = region(w, 0, part, 1, me, None)
        if relayed:
            src, dst = relays[w].at[part], region(w, 1, part, 1, me, None)
        else:
            src, dst = block, relays[w].at[part]
        return remote(src, dst, w_send.at[w * 4 + 3], x_recv.at[w * 4 + relayed * 2 + part], x_dirs[part])

    def ready(w):
        for part in (0, 1):
            w_wait(w, 0, part, 0, 2)

    def x1(w):
        for part in (0, 1):
            start(x_copy(w, part, 0))

    def xr(w):
        for part in (0, 1):
            x_copy(w, part, 0).wait_recv()
            start(x_copy(w, part, 1))

    def p3(w, s):
        for part in (0, 1):
            if s == 1:
                x_copy(w, part, 1).wait_recv()
            for i in (0, 1):
                w_start(w, s, part, 1, i)

    def p4(w, s):
        forward(w, s, 1)

    def p5(w, s):
        for part in (0, 1):
            w_wait(w, s, part, 1, 2)

    def wait_sent():
        def drained(ref, sem):
            remote(ref, ref, sem, x_recv.at[0], sib).wait_send()

        for w in range(4):
            ref = weights[w]
            drained(ref.at[0, 0, 0:3], w_send.at[w * 4])
            drained(ref.at[0, 0:3], w_send.at[w * 4 + 1])
            drained(ref.at[1, 0:3], w_send.at[w * 4 + 2])
            drained(ref.at[0, 0:2], w_send.at[w * 4 + 3])
        for r in range(3):
            drained(xs.at[r, 0], ag_send.at[r * 2])
            drained(xs.at[r, 0, :, 0], ag_send.at[r * 2 + 1])
            drained(po.at[r], rs_send.at[r * 2])
            drained(pc.at[r], rs_send.at[r * 2 + 1])
        drained(sti, st_send.at[0])
        swap_prm.wait_send()
        swap_sp.wait_send()

    def ag_ici(r, ch):
        return remote(
            xs.at[r, L, ch, 0], xs.at[r, R, ch, 0], ag_send.at[r * 2], ag_recv.at[r * (2 * CH + 1) + ch], partner
        )

    def ag_d2d(r, ch):
        chunk = pl.ds(0, CH) if ch is None else ch
        return remote(
            xs.at[r, L, chunk, 0], xs.at[r, L, chunk, 1], ag_send.at[r * 2], ag_recv.at[r * (2 * CH + 1) + 2 * CH], sib
        )

    def ag_fwd(r, ch):
        return remote(
            xs.at[r, R, ch, 0], xs.at[r, R, ch, 1], ag_send.at[r * 2 + 1], ag_recv.at[r * (2 * CH + 1) + CH + ch], sib
        )

    def rs_d2d_right(r, ch):
        return remote(po.at[r, R, ch], ps.at[r, R, ch], rs_send.at[r * 2], rs_recv.at[r * (2 * CH + 1) + ch], sib)

    def rs_d2d_left(r):
        return remote(po.at[r, L], ps.at[r, L], rs_send.at[r * 2], rs_recv.at[r * (2 * CH + 1) + 2 * CH], sib)

    def rs_ici(r, ch):
        return remote(pc.at[r, ch], pr.at[r, ch], rs_send.at[r * 2 + 1], rs_recv.at[r * (2 * CH + 1) + CH + ch], partner)

    def normed(rows, gain):
        factor = lax.rsqrt(jnp.mean(rows * rows, axis=1, keepdims=True) + norm_epsilon)
        return (rows * factor * gain[...]).astype(BF16)

    def ag_send_chunk(r, ch):
        start(ag_ici(r, ch))
        start(ag_d2d(r, ch))

    def ag_wait_left(r):
        ag_d2d(r, None).wait_recv()

    def ag_relay(r, ch):
        ag_ici(r, ch).wait_recv()
        start(ag_fwd(r, ch))

    def ag_wait_right(r, ch):
        ag_fwd(r, ch).wait_recv()

    loads[0].wait()
    pl.semaphore_wait(barrier, len(greeted))
    p1(DN)
    loads[1].wait()
    loads[2].wait()
    wgl[0, zl, y] = jnp.concatenate(
        [gate_lift[half, j * 128 : (j + 1) * 128] for j in range(3) for half in (0, 1)]
        + [gate_lift[half, 384:448] for half in (0, 1)],
        axis=0,
    ).T
    p1(GL)
    for load in loads[3:]:
        load.wait()

    for ch in range(CH):

        @pl.loop(0, CROWS // STEP)
        def _(i):
            rows = pl.ds(i * STEP, STEP)
            xs[0, L, ch, 0, rows, :] = normed(res[ch, rows, :].astype(F32), gain_b)

    prm[0] = jnp.concatenate([small[0], small[1], small[2], jnp.zeros((2, 128), F32)], axis=0)
    swap_prm = remote(prm.at[0], prm.at[1], sw_send.at[0], sw_recv.at[0], swap_to)
    swap_sp = remote(sp2.at[0], sp2.at[1], sw_send.at[1], sw_recv.at[1], swap_to)
    for ch in range(CH):
        ag_send_chunk(0, ch)
    start(swap_prm)
    start(swap_sp)

    def pick(ref, b, ch):
        return ref[b].reshape(256, ref.shape[-1]) if ch is None else ref[b, ch]

    def put(ref, b, ch, cols, value):
        if ch is None:
            for k in range(CH):
                ref[b, k, :, cols] = value[k * 128 : (k + 1) * 128]
        else:
            ref[b, ch, :, cols] = value

    def batch_x(r, b, ch):
        return xs[r, b].reshape(256, 2048) if ch is None else xs[r, b, ch].reshape(128, 2048)

    def up_slot(r, b, s, ch=None):
        o = dot(batch_x(r, b, ch), wgl[s, :, :, :, 0:768].reshape(2048, 768))
        for j in range(3):
            to = pl.ds(pl.multiple_of(s * 384 + j * 128, 128), 128)
            h = silu(o[:, j * 256 : j * 256 + 128]) * o[:, j * 256 + 128 : j * 256 + 256]
            put(hid, b, ch, to, h.astype(BF16))

    def up_tail(r, b, ch=None):
        w = jnp.concatenate([wgl[s, :, :, :, 768:896].reshape(2048, 128) for s in (0, 1)], axis=1)
        o = dot(batch_x(r, b, ch), w)
        t0, t1 = o[:, :128], o[:, 128:]
        low = lax.broadcasted_iota(jnp.int32, t0.shape, 1) < 64
        gate = jnp.where(low, t0, pltpu.roll(t1, 64, axis=1))
        lift = jnp.where(low, pltpu.roll(t0, 64, axis=1), t1)
        put(hid, b, ch, pl.ds(768, 128), (silu(gate) * lift).astype(BF16))

    def up(r, b, ch=None):
        @pl.loop(0, 2)
        def _(s):
            up_slot(r, b, s, ch)

        up_tail(r, b, ch)

    def wd_cols(zz, yy):
        return jnp.concatenate(
            [wd[0, zz, yy, 0:384], wd[1, zz, yy, 0:384], wd[0, zz, yy, 384:448], wd[1, zz, yy, 384:448]], axis=0
        )

    def wmd_cols(zz, yy):
        return jnp.concatenate([wmd[0, zz, yy], wmd[1, zz, yy]], axis=0)

    def down(r, b, ch, half, lhs, columns_of):
        rhs = jnp.concatenate([columns_of(half * 2 + n // 4, n % 4) for n in range(8)], axis=1)
        o = dot(pick(lhs, b, ch), rhs)
        cols = pl.ds(half * 1024, 1024)
        for i, k in enumerate(range(CH) if ch is None else (ch,)):
            acc[b, k, :, cols] = o[i * 128 : i * 128 + 64]
            po[r, b, k, :, cols] = o[i * 128 + 64 : i * 128 + 128].astype(BF16)

    def down_right(r, ch, lhs, columns_of):
        for half in (0, 1):
            down(r, R, ch, half, lhs, columns_of)
        start(rs_d2d_right(r, ch))

    def rs_right(r, ch):
        rs_d2d_right(r, ch).wait_recv()

        @pl.loop(0, CROWS // STEP)
        def _(i):
            rows = pl.ds(i * STEP, STEP)
            pc[r, ch, rows, :] = (acc[R, ch, rows, :] + ps[r, R, ch, rows, :].astype(F32)).astype(BF16)

        start(rs_ici(r, ch))

    def down_rest(r, lhs, columns_of, first):
        first()
        down(r, L, None, 0, lhs, columns_of)
        rs_right(r, 1)
        down(r, L, None, 1, lhs, columns_of)
        start(rs_d2d_left(r))

    def rs_left(r, coefficient, gain):
        rs_d2d_left(r).wait_recv()
        for ch in range(CH):
            rs_ici(r, ch).wait_recv()

            @pl.loop(0, CROWS // STEP)
            def _(i):
                rows = pl.ds(i * STEP, STEP)
                delta = acc[L, ch, rows, :] + ps[r, L, ch, rows, :].astype(F32) + pr[r, ch, rows, :].astype(F32)
                new = (res[ch, rows, :].astype(F32) + coefficient * delta).astype(BF16)
                if gain is None:
                    out[pl.ds(ch * CROWS + i * STEP, STEP), :] = new
                else:
                    res[ch, rows, :] = new
                    xs[r + 1, L, ch, 0, rows, :] = normed(new.astype(F32), gain)

            if gain is not None:
                ag_send_chunk(r + 1, ch)

    def mixer_up(b, ch=None):
        @pl.loop(0, 2)
        def _(s):
            to = pl.ds(pl.multiple_of(s * 256, 256), 256)
            o = dot(batch_x(1, b, ch), wuv[s].reshape(2048, 512))
            put(gu, b, ch, to, gelu(o[:, :256]))
            put(lf, b, ch, to, gelu(o[:, 256:]))

    def tokens(ref, b, q, cols):
        return jnp.concatenate([ref[b, k, q * 64 : q * 64 + 64, cols] for k in range(CH)], axis=0)

    lane = lax.broadcasted_iota(jnp.int32, (128, 128), 1)

    def stat_send():
        table = jnp.zeros((128, 128), F32)
        for q in (0, 1):
            for b in (0, 1):
                v = tokens(lf, b, q, slice(None))
                mean = jnp.mean(v, axis=1, keepdims=True)
                dev2 = jnp.sum(jnp.square(v - mean), axis=1, keepdims=True)
                table = jnp.where(lane == q * 8 + b * 2, mean, table)
                table = jnp.where(lane == q * 8 + b * 2 + 1, dev2, table)
        flipped = table.T
        sto[0] = flipped[0:8]
        sto[1] = flipped[8:16]
        routes = (
            (0, 1, 0, sib),
            (1, 0, 0, sib),
            (0, 0, 1, partner),
            (0, 1, 2, dev(xo, y, z8, 1 - c)),
            (1, 0, 2, dev(xt, y, z8, 1 - c)),
            (1, 1, 1, dev(xt, y, z8, c)),
        )
        for q, dest, slot, to in routes:
            start(remote(sto.at[q], sti.at[dest, slot], st_send.at[0], st_recv.at[0], to))

    def stat_combine():
        remote(sti, sti, st_send.at[0], st_recv.at[0], sib).wait_recv()
        rows = []
        for q in (0, 1):
            for b in (0, 1):
                parts = [(sto, q, None, b), (sti, q, 0, b), (sti, q, 1, 1 - b), (sti, q, 2, 1 - b)]
                means, devs = [], []
                for ref, qq, slot, bb in parts:
                    block = ref[qq] if slot is None else ref[qq, slot]
                    means.append(block[bb * 2 : bb * 2 + 1])
                    devs.append(block[bb * 2 + 1 : bb * 2 + 2])
                centre = (means[0] + means[1] + means[2] + means[3]) * 0.25
                spread = devs[0] + devs[1] + devs[2] + devs[3]
                for m in means:
                    spread = spread + 512.0 * jnp.square(m - centre)
                rows.append(centre)
                rows.append(lax.rsqrt(spread * (1.0 / A) + layer_epsilon))
        for s in (0, 1):
            for g in (0, 1):
                rows.append(prm[s, 4 + g : 5 + g])
        rows.append(jnp.zeros((116, 128), F32))
        colm[...] = jnp.concatenate(rows, axis=0).T

    def mixer_mid(b):
        for q in (0, 1):
            k = (q * 2 + b) * 2
            centre, factor = colm[:, k : k + 1], colm[:, k + 1 : k + 2]
            for s in (0, 1):
                for g in (0, 1):
                    n = s * 2 + g
                    cols = pl.ds(n * 128, 128)
                    v = (tokens(lf, b, q, cols) - centre) * factor * prm[s, g : g + 1] + prm[s, 2 + g : 3 + g]
                    mixed = dot(msp[n], v.astype(BF16)) + colm[:, 8 + n : 9 + n]
                    gated = (tokens(gu, b, q, cols) * mixed).astype(BF16)
                    for k in range(CH):
                        hid2[b, k, q * 64 : q * 64 + 64, cols] = gated[k * 64 : k * 64 + 64]

    p2(DN)
    p2(GL)
    p1(UV)
    ready(DN)
    p3(DN, 0)
    ready(GL)
    x1(GL)
    p3(GL, 0)
    p2(UV)
    p1(MD)
    p4(DN, 0)
    xr(GL)
    x1(DN)
    p4(GL, 0)
    ready(UV)
    p2(MD)
    ag_relay(0, 0)
    ag_relay(0, 1)
    ag_wait_left(0)
    ag_wait_right(0, 0)
    ag_wait_right(0, 1)
    p3(GL, 1)
    p5(GL, 0)

    @pl.loop(0, 2)
    def _(b):
        up_slot(0, b, 0)

    xr(DN)
    x1(UV)
    ready(MD)
    p4(GL, 1)
    p3(DN, 1)
    xr(UV)
    x1(MD)
    p5(GL, 1)
    up_slot(0, L, 1)
    up_tail(0, L)
    p4(DN, 1)
    p3(UV, 0)
    up_slot(0, R, 1)
    up_tail(0, R)
    xr(MD)
    p5(DN, 0)
    p5(DN, 1)
    p3(UV, 1)
    down_right(0, 0, hid, wd_cols)
    down_right(0, 1, hid, wd_cols)
    down_rest(0, hid, wd_cols, lambda: rs_right(0, 0))
    p4(UV, 0)
    p3(MD, 0)
    swap_prm.wait_recv()
    swap_sp.wait_recv()
    causal = lax.broadcasted_iota(jnp.int32, (128, 128), 0) >= lane
    for s in (0, 1):
        for g in (0, 1):
            msp[s * 2 + g] = jnp.where(causal, sp2[s, g].astype(F32), 0.0).astype(BF16)
    rs_left(0, 0.5, m_gain)
    p4(UV, 1)
    p3(MD, 1)
    p4(MD, 0)
    ag_relay(1, 0)
    p5(UV, 0)
    p5(UV, 1)
    ag_wait_left(1)
    mixer_up(L)
    ag_wait_right(1, 0)
    ag_relay(1, 1)
    p4(MD, 1)
    mixer_up(R, 0)
    ag_wait_right(1, 1)
    mixer_up(R, 1)
    stat_send()
    p5(MD, 0)
    p5(MD, 1)
    stat_combine()
    mixer_mid(R)
    down_right(1, 0, hid2, wmd_cols)
    down_right(1, 1, hid2, wmd_cols)
    mixer_mid(L)
    down_rest(1, hid2, wmd_cols, lambda: rs_right(1, 0))
    rs_left(1, 1.0, gain_a)
    ag_wait_left(2)
    up(2, L)
    ag_relay(2, 0)
    ag_wait_right(2, 0)
    up(2, R, 0)
    ag_relay(2, 1)
    down_right(2, 0, hid, wd_cols)
    ag_wait_right(2, 1)
    up(2, R, 1)
    rs_right(2, 0)
    down_right(2, 1, hid, wd_cols)
    down_rest(2, hid, wd_cols, lambda: None)
    rs_left(2, 0.5, None)
    wait_sent()


def layer(stream, gain_b, gain_a, p_gate, p_lift, p_down, m_gain, m_u, m_v, l_gain, l_shift, spat, s_shift, m_down):
    dma = pltpu.SemaphoreType.DMA
    return pl.pallas_call(
        kernel,
        out_shape=pltpu.VMEM((128, 2048), BF16),
        in_specs=[pl.BlockSpec(memory_space=pl.ANY)] * 14,
        out_specs=pl.BlockSpec(memory_space=pltpu.VMEM),
        scratch_shapes=[
            pltpu.VMEM((2, 4, 4, 128, 896), BF16),
            pltpu.VMEM((2, 4, 4, 448, 128), BF16),
            pltpu.VMEM((2, 4, 4, 128, 512), BF16),
            pltpu.VMEM((2, 4, 4, 256, 128), BF16),
            pltpu.VMEM((2, 4, 64, 896), BF16),
            pltpu.VMEM((2, 4, 224, 128), BF16),
            pltpu.VMEM((2, 4, 64, 512), BF16),
            pltpu.VMEM((2, 4, 128, 128), BF16),
            pltpu.VMEM((2, 448, 128), BF16),
            pltpu.VMEM((1, 2048), F32),
            pltpu.VMEM((1, 2048), F32),
            pltpu.VMEM((1, 2048), F32),
            pltpu.VMEM((3, 2, 128), F32),
            pltpu.VMEM((4, 128, 128), BF16),
            pltpu.VMEM((2, 2, 128, 128), BF16),
            pltpu.VMEM((2, 8, 128), F32),
            pltpu.VMEM((3, 2, CH, 2, CROWS, 2048), BF16),
            pltpu.VMEM((3, 2, CH, CROWS, 2048), BF16),
            pltpu.VMEM((3, 2, CH, CROWS, 2048), BF16),
            pltpu.VMEM((3, CH, CROWS, 2048), BF16),
            pltpu.VMEM((3, CH, CROWS, 2048), BF16),
            pltpu.VMEM((2, CH, CROWS, 2048), F32),
            pltpu.VMEM((2, CH, 128, 896), BF16),
            pltpu.VMEM((2, CH, 128, 512), BF16),
            pltpu.VMEM((2, CH, 128, 512), F32),
            pltpu.VMEM((2, CH, 128, 512), F32),
            pltpu.VMEM((CH, CROWS, 2048), BF16),
            pltpu.VMEM((2, 8, 128), F32),
            pltpu.VMEM((2, 3, 8, 128), F32),
            pltpu.VMEM((128, 128), F32),
            dma((15,)),
            dma((16,)), dma((72,)), dma((16,)),
            dma((2,)), dma((2,)),
            dma((6,)), dma((3 * (2 * CH + 1),)),
            dma((6,)), dma((3 * (2 * CH + 1),)),
            dma((1,)), dma((1,)),
        ],
        compiler_params=pltpu.CompilerParams(
            collective_id=0, has_side_effects=True, vmem_limit_bytes=58 * 1024 * 1024
        ),
    )(
        stream, gain_b.reshape(1, -1), gain_a.reshape(1, -1), p_gate.T, p_lift.T, p_down, m_gain.reshape(1, -1),
        m_u, m_v, l_gain.reshape(2, 128), l_shift.reshape(2, 128), spat, s_shift, m_down,
    )


def solution(mesh):
    placed = (
        P(("rep", "fs", "tp"), None),
        P(),
        P(),
        P("fs", "tp"),
        P("fs", "tp"),
        P("tp", "fs"),
        P(),
        P("fs", "tp"),
        P("fs", "tp"),
        P("tp"),
        P("tp"),
        P("tp", None, None),
        P("tp", None),
        P("tp", "fs"),
    )
    return jax.shard_map(
        layer, mesh=mesh, in_specs=placed, out_specs=P(("rep", "fs", "tp"), None), check_vma=False
    )
```

```python
import jax
import jax.numpy as jnp
from jax import lax
from jax.experimental import pallas as pl
from jax.experimental.pallas import tpu as pltpu
from jax.sharding import PartitionSpec as P

MESH = pl.DeviceIdType.MESH
F32 = jnp.float32
BF16 = jnp.bfloat16
A = 2048
norm_epsilon = 1e-06
layer_epsilon = 1e-05
L, R = 0, 1
GL, DN, UV, MD = 0, 1, 2, 3
W_ROWS = (128, 448, 128, 256)
CH = 2
CROWS = 128 // CH
STEP = 16


def silu(v):
    return v / (1.0 + jnp.exp(-v))


def gelu(v):
    return 0.5 * v * (1.0 + jnp.tanh(0.7978845608028654 * (v + 0.044715 * (v * v * v))))


def dot(a, b):
    return jnp.dot(a, b, preferred_element_type=F32)


def recv_index(w, s, part, phase, i):
    return ((w * 3 + s * 2 + phase - s) * 2 + part) * 3 + min(i, 2)


def kernel(
    stream, h_gain_b, h_gain_a, p_gate, p_lift, p_down, h_gain_m, m_u, m_v, l_gain, l_shift, spat, s_shift, m_down,
    out,
    wgl, wd, wuv, wmd, rgl, rd, ruv, rmd, gate_lift, gain_b, gain_a, m_gain, small, msp, sp2, prm,
    xs, po, ps, pc, pr, acc, hid, hid2, gu, lf, res, sto, sti, colm,
    in_sem, w_send, w_recv, x_recv, sw_send, sw_recv, ag_send, ag_recv, rs_send, rs_recv, st_send, st_recv,
):
    rep, fs, tp = lax.axis_index("rep"), lax.axis_index("fs"), lax.axis_index("tp")
    x, c = tp // 2, tp % 2
    zl, y = fs // 4, fs % 4
    z8 = rep * 4 + zl

    def dev(dx, dy, dz, dc):
        return (dz // 4, (dz % 4) * 4 + dy, dx * 2 + dc)

    sib = dev(x, y, z8, 1 - c)
    xo = (x + 1 + 2 * ((x + c) % 2)) % 4
    xt = (x + 1 + 2 * ((x + c + 1) % 2)) % 4
    partner = dev(xo, y, z8, c)
    y_plus, y_minus = dev(x, (y + 1) % 4, z8, c), dev(x, (y + 3) % 4, z8, c)
    z_plus, z_minus = dev(x, y, (z8 + 1) % 8, c), dev(x, y, (z8 + 7) % 8, c)
    swap_to = dev((x + 2) % 4, y, z8, c)
    weights = (wgl, wd, wuv, wmd)
    relays = (rgl, rd, ruv, rmd)
    x_dirs = (dev((x + 1) % 4, y, z8, c), dev((x + 3) % 4, y, z8, c))

    barrier = pltpu.get_barrier_semaphore()
    greeted = (
        sib, partner, dev(xo, y, z8, 1 - c), dev(xt, y, z8, 0), dev(xt, y, z8, 1),
        y_plus, y_minus, z_plus, z_minus, swap_to,
    )
    for other in greeted:
        pl.semaphore_signal(barrier, inc=1, device_id=other, device_id_type=MESH)

    def remote(src, dst, ssem, rsem, to):
        return pltpu.make_async_remote_copy(
            src_ref=src, dst_ref=dst, send_sem=ssem, recv_sem=rsem, device_id=to, device_id_type=MESH
        )

    def start(copy):
        copy.start()

    loads = [
        pltpu.make_async_copy(src, dst, in_sem.at[i])
        for i, (src, dst) in enumerate(
            (
                (p_down, wd.at[0, zl, y]),
                (p_gate, gate_lift.at[0]),
                (p_lift, gate_lift.at[1]),
                (stream.at[pl.ds(0, CROWS)], res.at[0]),
                (stream.at[pl.ds(CROWS, CROWS)], res.at[1]),
                (h_gain_b, gain_b),
                (m_u, wuv.at[0, zl, y, :, pl.ds(0, 256)]),
                (m_v, wuv.at[0, zl, y, :, pl.ds(256, 256)]),
                (m_down, wmd.at[0, zl, y]),
                (l_gain, small.at[0]),
                (l_shift, small.at[1]),
                (s_shift, small.at[2]),
                (spat, sp2.at[0]),
                (h_gain_m, m_gain),
                (h_gain_a, gain_a),
            )
        )
    ]
    for load in loads:
        load.start()

    def region(w, s, part, phase, pos, sub):
        n = W_ROWS[w] // 2
        r0 = part * n
        if sub is not None:
            n //= 2
            r0 += sub * n
        rows = pl.ds(r0, n)
        ref = weights[w]
        if phase == 0:
            return ref.at[s, zl, pos, rows] if part == 0 else ref.at[s, pos, y, rows]
        return ref.at[s, pos, :, rows] if part == 0 else ref.at[s, :, pos, rows]

    def ring(part, phase):
        if part == phase:
            return y, y_plus, y_minus
        return zl, z_plus, z_minus

    def w_start(w, s, part, phase, i):
        me, plus, minus = ring(part, phase)
        pos = (me, me, (me + 3) % 4, (me + 1) % 4)[i]
        block = region(w, s, part, phase, pos, (None, None, 0, 1)[i])
        j = recv_index(w, s, part, phase, i)
        start(remote(block, block, w_send.at[w * 4 + s + phase], w_recv.at[j], (plus, minus, plus, minus)[i]))

    def w_wait(w, s, part, phase, i):
        me, plus, minus = ring(part, phase)
        pos = ((me + 3) % 4, (me + 1) % 4, (me + 2) % 4)[i]
        block = region(w, s, part, phase, pos, None)
        j = recv_index(w, s, part, phase, i)
        remote(block, block, w_send.at[w * 4 + s + phase], w_recv.at[j], plus).wait_recv()

    def p1(w):
        for part in (0, 1):
            for i in (0, 1):
                w_start(w, 0, part, 0, i)

    def forward(w, s, phase):
        for part in (0, 1):
            for i in (0, 1):
                w_wait(w, s, part, phase, i)
                w_start(w, s, part, phase, i + 2)

    def p2(w):
        forward(w, 0, 0)

    def x_copy(w, part, relayed):
        me = ring(part, 1)[0]
        block = region(w, 0, part, 1, me, None)
        if relayed:
            src, dst = relays[w].at[part], region(w, 1, part, 1, me, None)
        else:
            src, dst = block, relays[w].at[part]
        return remote(src, dst, w_send.at[w * 4 + 3], x_recv.at[w * 4 + relayed * 2 + part], x_dirs[part])

    def ready(w):
        for part in (0, 1):
            w_wait(w, 0, part, 0, 2)

    def x1(w):
        for part in (0, 1):
            start(x_copy(w, part, 0))

    def xr(w):
        for part in (0, 1):
            x_copy(w, part, 0).wait_recv()
            start(x_copy(w, part, 1))

    def p3(w, s):
        for part in (0, 1):
            if s == 1:
                x_copy(w, part, 1).wait_recv()
            for i in (0, 1):
                w_start(w, s, part, 1, i)

    def p4(w, s):
        forward(w, s, 1)

    def p5(w, s):
        for part in (0, 1):
            w_wait(w, s, part, 1, 2)

    def wait_sent():
        def drained(ref, sem):
            remote(ref, ref, sem, x_recv.at[0], sib).wait_send()

        for w in range(4):
            ref = weights[w]
            drained(ref.at[0, 0, 0:3], w_send.at[w * 4])
            drained(ref.at[0, 0:3], w_send.at[w * 4 + 1])
            drained(ref.at[1, 0:3], w_send.at[w * 4 + 2])
            drained(ref.at[0, 0:2], w_send.at[w * 4 + 3])
        for r in range(3):
            drained(xs.at[r, 0], ag_send.at[r * 2])
            drained(xs.at[r, 0, :, 0], ag_send.at[r * 2 + 1])
            drained(po.at[r], rs_send.at[r * 2])
            drained(pc.at[r], rs_send.at[r * 2 + 1])
        drained(sti, st_send.at[0])
        swap_prm.wait_send()
        swap_sp.wait_send()

    def ag_ici(r, ch):
        return remote(
            xs.at[r, L, ch, 0], xs.at[r, R, ch, 0], ag_send.at[r * 2], ag_recv.at[r * (2 * CH + 1) + ch], partner
        )

    def ag_d2d(r, ch):
        chunk = pl.ds(0, CH) if ch is None else ch
        return remote(
            xs.at[r, L, chunk, 0], xs.at[r, L, chunk, 1], ag_send.at[r * 2], ag_recv.at[r * (2 * CH + 1) + 2 * CH], sib
        )

    def ag_fwd(r, ch):
        return remote(
            xs.at[r, R, ch, 0], xs.at[r, R, ch, 1], ag_send.at[r * 2 + 1], ag_recv.at[r * (2 * CH + 1) + CH + ch], sib
        )

    def rs_d2d_right(r, ch):
        return remote(po.at[r, R, ch], ps.at[r, R, ch], rs_send.at[r * 2], rs_recv.at[r * (2 * CH + 1) + ch], sib)

    def rs_d2d_left(r):
        return remote(po.at[r, L], ps.at[r, L], rs_send.at[r * 2], rs_recv.at[r * (2 * CH + 1) + 2 * CH], sib)

    def rs_ici(r, ch):
        return remote(pc.at[r, ch], pr.at[r, ch], rs_send.at[r * 2 + 1], rs_recv.at[r * (2 * CH + 1) + CH + ch], partner)

    def normed(rows, gain):
        factor = lax.rsqrt(jnp.mean(rows * rows, axis=1, keepdims=True) + norm_epsilon)
        return (rows * factor * gain[...]).astype(BF16)

    def ag_send_chunk(r, ch):
        start(ag_ici(r, ch))
        start(ag_d2d(r, ch))

    def ag_wait_left(r):
        ag_d2d(r, None).wait_recv()

    def ag_relay(r, ch):
        ag_ici(r, ch).wait_recv()
        start(ag_fwd(r, ch))

    def ag_wait_right(r, ch):
        ag_fwd(r, ch).wait_recv()

    loads[0].wait()
    pl.semaphore_wait(barrier, len(greeted))
    p1(DN)
    loads[1].wait()
    loads[2].wait()
    wgl[0, zl, y] = jnp.concatenate(
        [gate_lift[half, j * 128 : (j + 1) * 128] for j in range(3) for half in (0, 1)]
        + [gate_lift[half, 384:448] for half in (0, 1)],
        axis=0,
    ).T
    p1(GL)
    for load in loads[3:]:
        load.wait()

    for ch in range(CH):

        @pl.loop(0, CROWS // STEP)
        def _(i):
            rows = pl.ds(i * STEP, STEP)
            xs[0, L, ch, 0, rows, :] = normed(res[ch, rows, :].astype(F32), gain_b)

    prm[0] = jnp.concatenate([small[0], small[1], small[2], jnp.zeros((2, 128), F32)], axis=0)
    swap_prm = remote(prm.at[0], prm.at[1], sw_send.at[0], sw_recv.at[0], swap_to)
    swap_sp = remote(sp2.at[0], sp2.at[1], sw_send.at[1], sw_recv.at[1], swap_to)
    for ch in range(CH):
        ag_send_chunk(0, ch)
    start(swap_prm)
    start(swap_sp)

    def pick(ref, b, ch):
        return ref[b].reshape(256, ref.shape[-1]) if ch is None else ref[b, ch]

    def put(ref, b, ch, cols, value):
        if ch is None:
            for k in range(CH):
                ref[b, k, :, cols] = value[k * 128 : (k + 1) * 128]
        else:
            ref[b, ch, :, cols] = value

    def batch_x(r, b, ch):
        return xs[r, b].reshape(256, 2048) if ch is None else xs[r, b, ch].reshape(128, 2048)

    def up_slot(r, b, s, ch=None):
        o = dot(batch_x(r, b, ch), wgl[s, :, :, :, 0:768].reshape(2048, 768))
        for j in range(3):
            to = pl.ds(pl.multiple_of(s * 384 + j * 128, 128), 128)
            h = silu(o[:, j * 256 : j * 256 + 128]) * o[:, j * 256 + 128 : j * 256 + 256]
            put(hid, b, ch, to, h.astype(BF16))

    def up_tail(r, b, ch=None):
        w = jnp.concatenate([wgl[s, :, :, :, 768:896].reshape(2048, 128) for s in (0, 1)], axis=1)
        o = dot(batch_x(r, b, ch), w)
        t0, t1 = o[:, :128], o[:, 128:]
        low = lax.broadcasted_iota(jnp.int32, t0.shape, 1) < 64
        gate = jnp.where(low, t0, pltpu.roll(t1, 64, axis=1))
        lift = jnp.where(low, pltpu.roll(t0, 64, axis=1), t1)
        put(hid, b, ch, pl.ds(768, 128), (silu(gate) * lift).astype(BF16))

    def up(r, b, ch=None):
        for s in (0, 1):
            up_slot(r, b, s, ch)
        up_tail(r, b, ch)

    def wd_cols(zz, yy):
        return jnp.concatenate(
            [wd[0, zz, yy, 0:384], wd[1, zz, yy, 0:384], wd[0, zz, yy, 384:448], wd[1, zz, yy, 384:448]], axis=0
        )

    def wmd_cols(zz, yy):
        return jnp.concatenate([wmd[0, zz, yy], wmd[1, zz, yy]], axis=0)

    def down(r, b, ch, half, lhs, columns_of):
        rhs = jnp.concatenate([columns_of(half * 2 + n // 4, n % 4) for n in range(8)], axis=1)
        o = dot(pick(lhs, b, ch), rhs)
        cols = pl.ds(half * 1024, 1024)
        for i, k in enumerate(range(CH) if ch is None else (ch,)):
            acc[b, k, :, cols] = o[i * 128 : i * 128 + 64]
            po[r, b, k, :, cols] = o[i * 128 + 64 : i * 128 + 128].astype(BF16)

    def down_right(r, ch, lhs, columns_of):
        for half in (0, 1):
            down(r, R, ch, half, lhs, columns_of)
        start(rs_d2d_right(r, ch))

    def rs_right(r, ch):
        rs_d2d_right(r, ch).wait_recv()

        @pl.loop(0, CROWS // STEP)
        def _(i):
            rows = pl.ds(i * STEP, STEP)
            pc[r, ch, rows, :] = (acc[R, ch, rows, :] + ps[r, R, ch, rows, :].astype(F32)).astype(BF16)

        start(rs_ici(r, ch))

    def down_rest(r, lhs, columns_of, first):
        first()
        down(r, L, None, 0, lhs, columns_of)
        rs_right(r, 1)
        down(r, L, None, 1, lhs, columns_of)
        start(rs_d2d_left(r))

    def rs_left(r, coefficient, gain, between=None):
        rs_d2d_left(r).wait_recv()
        for ch in range(CH):
            rs_ici(r, ch).wait_recv()

            @pl.loop(0, CROWS // STEP)
            def _(i):
                rows = pl.ds(i * STEP, STEP)
                delta = acc[L, ch, rows, :] + ps[r, L, ch, rows, :].astype(F32) + pr[r, ch, rows, :].astype(F32)
                new = (res[ch, rows, :].astype(F32) + coefficient * delta).astype(BF16)
                if gain is None:
                    out[pl.ds(ch * CROWS + i * STEP, STEP), :] = new
                else:
                    res[ch, rows, :] = new
                    xs[r + 1, L, ch, 0, rows, :] = normed(new.astype(F32), gain)

            if gain is not None:
                ag_send_chunk(r + 1, ch)
            if between is not None and ch == 0:
                between()

    def mixer_up(b, ch=None):
        for s in (0, 1):
            to = pl.ds(s * 256, 256)
            o = dot(batch_x(1, b, ch), wuv[s].reshape(2048, 512))
            put(gu, b, ch, to, gelu(o[:, :256]))
            put(lf, b, ch, to, gelu(o[:, 256:]))

    def tokens(ref, b, q, cols):
        return jnp.concatenate([ref[b, k, q * 64 : q * 64 + 64, cols] for k in range(CH)], axis=0)

    lane = lax.broadcasted_iota(jnp.int32, (128, 128), 1)

    def stat_send():
        table = jnp.zeros((128, 128), F32)
        for q in (0, 1):
            for b in (0, 1):
                v = tokens(lf, b, q, slice(None))
                mean = jnp.mean(v, axis=1, keepdims=True)
                dev2 = jnp.sum(jnp.square(v - mean), axis=1, keepdims=True)
                table = jnp.where(lane == q * 8 + b * 2, mean, table)
                table = jnp.where(lane == q * 8 + b * 2 + 1, dev2, table)
        flipped = table.T
        sto[0] = flipped[0:8]
        sto[1] = flipped[8:16]
        routes = (
            (0, 1, 0, sib),
            (1, 0, 0, sib),
            (0, 0, 1, partner),
            (0, 1, 2, dev(xo, y, z8, 1 - c)),
            (1, 0, 2, dev(xt, y, z8, 1 - c)),
            (1, 1, 1, dev(xt, y, z8, c)),
        )
        for q, dest, slot, to in routes:
            start(remote(sto.at[q], sti.at[dest, slot], st_send.at[0], st_recv.at[0], to))

    def stat_combine():
        remote(sti, sti, st_send.at[0], st_recv.at[0], sib).wait_recv()
        rows = []
        for q in (0, 1):
            for b in (0, 1):
                parts = [(sto, q, None, b), (sti, q, 0, b), (sti, q, 1, 1 - b), (sti, q, 2, 1 - b)]
                means, devs = [], []
                for ref, qq, slot, bb in parts:
                    block = ref[qq] if slot is None else ref[qq, slot]
                    means.append(block[bb * 2 : bb * 2 + 1])
                    devs.append(block[bb * 2 + 1 : bb * 2 + 2])
                centre = (means[0] + means[1] + means[2] + means[3]) * 0.25
                spread = devs[0] + devs[1] + devs[2] + devs[3]
                for m in means:
                    spread = spread + 512.0 * jnp.square(m - centre)
                rows.append(centre)
                rows.append(lax.rsqrt(spread * (1.0 / A) + layer_epsilon))
        for s in (0, 1):
            for g in (0, 1):
                rows.append(prm[s, 4 + g : 5 + g])
        rows.append(jnp.zeros((116, 128), F32))
        colm[...] = jnp.concatenate(rows, axis=0).T

    def mixer_mid(b):
        for q in (0, 1):
            k = (q * 2 + b) * 2
            centre, factor = colm[:, k : k + 1], colm[:, k + 1 : k + 2]
            for s in (0, 1):
                for g in (0, 1):
                    n = s * 2 + g
                    cols = pl.ds(n * 128, 128)
                    v = (tokens(lf, b, q, cols) - centre) * factor * prm[s, g : g + 1] + prm[s, 2 + g : 3 + g]
                    mixed = dot(msp[n], v.astype(BF16)) + colm[:, 8 + n : 9 + n]
                    gated = (tokens(gu, b, q, cols) * mixed).astype(BF16)
                    for k in range(CH):
                        hid2[b, k, q * 64 : q * 64 + 64, cols] = gated[k * 64 : k * 64 + 64]

    p2(DN)
    p1(UV)
    p2(GL)
    p1(MD)
    ready(DN)
    p3(DN, 0)
    ready(GL)
    x1(GL)
    p3(GL, 0)
    p2(UV)
    p4(DN, 0)
    xr(GL)
    x1(DN)
    p4(GL, 0)
    ready(UV)
    p2(MD)
    ag_relay(0, 0)
    ag_relay(0, 1)
    ag_wait_left(0)
    ag_wait_right(0, 0)
    ag_wait_right(0, 1)
    p3(GL, 1)
    p5(GL, 0)

    @pl.loop(0, 2)
    def _(b):
        up_slot(0, b, 0)

    xr(DN)
    x1(UV)
    ready(MD)
    p4(GL, 1)
    p3(DN, 1)
    xr(UV)
    x1(MD)
    p5(GL, 1)
    up_slot(0, L, 1)
    up_tail(0, L)
    p4(DN, 1)
    p3(UV, 0)
    up_slot(0, R, 1)
    up_tail(0, R)
    xr(MD)
    p5(DN, 0)
    p5(DN, 1)
    p3(UV, 1)
    down_right(0, 0, hid, wd_cols)
    down_right(0, 1, hid, wd_cols)
    down_rest(0, hid, wd_cols, lambda: rs_right(0, 0))
    p4(UV, 0)
    p3(MD, 0)
    swap_prm.wait_recv()
    swap_sp.wait_recv()
    causal = lax.broadcasted_iota(jnp.int32, (128, 128), 0) >= lane
    for s in (0, 1):
        for g in (0, 1):
            msp[s * 2 + g] = jnp.where(causal, sp2[s, g].astype(F32), 0.0).astype(BF16)

    def weights_between():
        p4(UV, 1)
        p3(MD, 1)

    rs_left(0, 0.5, m_gain, weights_between)
    p4(MD, 0)
    ag_relay(1, 0)
    p5(UV, 0)
    p5(UV, 1)
    ag_relay(1, 1)
    ag_wait_left(1)
    mixer_up(L)
    ag_wait_right(1, 0)
    p4(MD, 1)
    mixer_up(R, 0)
    ag_wait_right(1, 1)
    mixer_up(R, 1)
    stat_send()
    p5(MD, 0)
    p5(MD, 1)
    stat_combine()
    mixer_mid(R)
    down_right(1, 0, hid2, wmd_cols)
    down_right(1, 1, hid2, wmd_cols)
    mixer_mid(L)
    down_rest(1, hid2, wmd_cols, lambda: rs_right(1, 0))
    rs_left(1, 1.0, gain_a)
    ag_wait_left(2)
    up_slot(2, L, 0)
    ag_relay(2, 0)
    up_slot(2, L, 1)
    up_tail(2, L)
    ag_wait_right(2, 0)
    up_slot(2, R, 0, 0)
    ag_relay(2, 1)
    up_slot(2, R, 1, 0)
    up_tail(2, R, 0)
    down_right(2, 0, hid, wd_cols)
    ag_wait_right(2, 1)
    up(2, R, 1)
    rs_right(2, 0)
    down_right(2, 1, hid, wd_cols)
    down_rest(2, hid, wd_cols, lambda: None)
    rs_left(2, 0.5, None)
    wait_sent()


def layer(stream, gain_b, gain_a, p_gate, p_lift, p_down, m_gain, m_u, m_v, l_gain, l_shift, spat, s_shift, m_down):
    dma = pltpu.SemaphoreType.DMA
    return pl.pallas_call(
        kernel,
        out_shape=pltpu.VMEM((128, 2048), BF16),
        in_specs=[pl.BlockSpec(memory_space=pl.ANY)] * 14,
        out_specs=pl.BlockSpec(memory_space=pltpu.VMEM),
        scratch_shapes=[
            pltpu.VMEM((2, 4, 4, 128, 896), BF16),
            pltpu.VMEM((2, 4, 4, 448, 128), BF16),
            pltpu.VMEM((2, 4, 4, 128, 512), BF16),
            pltpu.VMEM((2, 4, 4, 256, 128), BF16),
            pltpu.VMEM((2, 4, 64, 896), BF16),
            pltpu.VMEM((2, 4, 224, 128), BF16),
            pltpu.VMEM((2, 4, 64, 512), BF16),
            pltpu.VMEM((2, 4, 128, 128), BF16),
            pltpu.VMEM((2, 448, 128), BF16),
            pltpu.VMEM((1, 2048), F32),
            pltpu.VMEM((1, 2048), F32),
            pltpu.VMEM((1, 2048), F32),
            pltpu.VMEM((3, 2, 128), F32),
            pltpu.VMEM((4, 128, 128), BF16),
            pltpu.VMEM((2, 2, 128, 128), BF16),
            pltpu.VMEM((2, 8, 128), F32),
            pltpu.VMEM((3, 2, CH, 2, CROWS, 2048), BF16),
            pltpu.VMEM((3, 2, CH, CROWS, 2048), BF16),
            pltpu.VMEM((3, 2, CH, CROWS, 2048), BF16),
            pltpu.VMEM((3, CH, CROWS, 2048), BF16),
            pltpu.VMEM((3, CH, CROWS, 2048), BF16),
            pltpu.VMEM((2, CH, CROWS, 2048), F32),
            pltpu.VMEM((2, CH, 128, 896), BF16),
            pltpu.VMEM((2, CH, 128, 512), BF16),
            pltpu.VMEM((2, CH, 128, 512), F32),
            pltpu.VMEM((2, CH, 128, 512), F32),
            pltpu.VMEM((CH, CROWS, 2048), BF16),
            pltpu.VMEM((2, 8, 128), F32),
            pltpu.VMEM((2, 3, 8, 128), F32),
            pltpu.VMEM((128, 128), F32),
            dma((15,)),
            dma((16,)), dma((72,)), dma((16,)),
            dma((2,)), dma((2,)),
            dma((6,)), dma((3 * (2 * CH + 1),)),
            dma((6,)), dma((3 * (2 * CH + 1),)),
            dma((1,)), dma((1,)),
        ],
        compiler_params=pltpu.CompilerParams(
            collective_id=0, has_side_effects=True, vmem_limit_bytes=58 * 1024 * 1024
        ),
    )(
        stream, gain_b.reshape(1, -1), gain_a.reshape(1, -1), p_gate.T, p_lift.T, p_down, m_gain.reshape(1, -1),
        m_u, m_v, l_gain.reshape(2, 128), l_shift.reshape(2, 128), spat, s_shift, m_down,
    )


def solution(mesh):
    placed = (
        P(("rep", "fs", "tp"), None),
        P(),
        P(),
        P("fs", "tp"),
        P("fs", "tp"),
        P("tp", "fs"),
        P(),
        P("fs", "tp"),
        P("fs", "tp"),
        P("tp"),
        P("tp"),
        P("tp", None, None),
        P("tp", None),
        P("tp", "fs"),
    )
    return jax.shard_map(
        layer, mesh=mesh, in_specs=placed, out_specs=P(("rep", "fs", "tp"), None), check_vma=False
    )
```

```python
import jax
import jax.numpy as jnp
from jax import lax
from jax.experimental import pallas as pl
from jax.experimental.pallas import tpu as pltpu
from jax.sharding import PartitionSpec as P

MESH = pl.DeviceIdType.MESH
F32 = jnp.float32
BF16 = jnp.bfloat16
A = 2048
norm_epsilon = 1e-06
layer_epsilon = 1e-05
L, R = 0, 1
GL, DN, UV, MD = 0, 1, 2, 3
W_ROWS = (128, 448, 128, 256)
CH = 2
CROWS = 128 // CH
STEP = 16


def silu(v):
    return v / (1.0 + jnp.exp(-v))


def gelu(v):
    return 0.5 * v * (1.0 + jnp.tanh(0.7978845608028654 * (v + 0.044715 * (v * v * v))))


def dot(a, b):
    return jnp.dot(a, b, preferred_element_type=F32)


def recv_index(w, s, part, phase, i):
    return ((w * 3 + s * 2 + phase - s) * 2 + part) * 3 + min(i, 2)


def kernel(
    stream, h_gain_b, h_gain_a, p_gate, p_lift, p_down, h_gain_m, m_u, m_v, l_gain, l_shift, spat, s_shift, m_down,
    out,
    wgl, wd, wuv, wmd, rgl, rd, ruv, rmd, gate_lift, gain_b, gain_a, m_gain, small, msp, sp2, prm,
    xs, po, ps, pc, pr, acc, hid, hid2, gu, lf, res, sto, sti, colm,
    in_sem, w_send, w_recv, x_recv, sw_send, sw_recv, ag_send, ag_recv, rs_send, rs_recv, st_send, st_recv,
):
    rep, fs, tp = lax.axis_index("rep"), lax.axis_index("fs"), lax.axis_index("tp")
    x, c = tp // 2, tp % 2
    zl, y = fs // 4, fs % 4
    z8 = rep * 4 + zl

    def dev(dx, dy, dz, dc):
        return (dz // 4, (dz % 4) * 4 + dy, dx * 2 + dc)

    sib = dev(x, y, z8, 1 - c)
    xo = (x + 1 + 2 * ((x + c) % 2)) % 4
    xt = (x + 1 + 2 * ((x + c + 1) % 2)) % 4
    partner = dev(xo, y, z8, c)
    y_plus, y_minus = dev(x, (y + 1) % 4, z8, c), dev(x, (y + 3) % 4, z8, c)
    z_plus, z_minus = dev(x, y, (z8 + 1) % 8, c), dev(x, y, (z8 + 7) % 8, c)
    swap_to = dev((x + 2) % 4, y, z8, c)
    weights = (wgl, wd, wuv, wmd)
    relays = (rgl, rd, ruv, rmd)
    x_dirs = (dev((x + 1) % 4, y, z8, c), dev((x + 3) % 4, y, z8, c))

    barrier = pltpu.get_barrier_semaphore()
    greeted = (
        sib, partner, dev(xo, y, z8, 1 - c), dev(xt, y, z8, 0), dev(xt, y, z8, 1),
        y_plus, y_minus, z_plus, z_minus, swap_to,
    )
    for other in greeted:
        pl.semaphore_signal(barrier, inc=1, device_id=other, device_id_type=MESH)

    def remote(src, dst, ssem, rsem, to):
        return pltpu.make_async_remote_copy(
            src_ref=src, dst_ref=dst, send_sem=ssem, recv_sem=rsem, device_id=to, device_id_type=MESH
        )

    def start(copy):
        copy.start()

    loads = [
        pltpu.make_async_copy(src, dst, in_sem.at[i])
        for i, (src, dst) in enumerate(
            (
                (p_down, wd.at[0, zl, y]),
                (p_gate, gate_lift.at[0]),
                (p_lift, gate_lift.at[1]),
                (stream.at[pl.ds(0, CROWS)], res.at[0]),
                (stream.at[pl.ds(CROWS, CROWS)], res.at[1]),
                (h_gain_b, gain_b),
                (m_u, wuv.at[0, zl, y, :, pl.ds(0, 256)]),
                (m_v, wuv.at[0, zl, y, :, pl.ds(256, 256)]),
                (m_down, wmd.at[0, zl, y]),
                (l_gain, small.at[0]),
                (l_shift, small.at[1]),
                (s_shift, small.at[2]),
                (spat, sp2.at[0]),
                (h_gain_m, m_gain),
                (h_gain_a, gain_a),
            )
        )
    ]
    for load in loads:
        load.start()

    def region(w, s, part, phase, pos, sub):
        n = W_ROWS[w] // 2
        r0 = part * n
        if sub is not None:
            n //= 2
            r0 += sub * n
        rows = pl.ds(r0, n)
        ref = weights[w]
        if phase == 0:
            return ref.at[s, zl, pos, rows] if part == 0 else ref.at[s, pos, y, rows]
        return ref.at[s, pos, :, rows] if part == 0 else ref.at[s, :, pos, rows]

    def ring(part, phase):
        if part == phase:
            return y, y_plus, y_minus
        return zl, z_plus, z_minus

    def w_start(w, s, part, phase, i):
        me, plus, minus = ring(part, phase)
        pos = (me, me, (me + 3) % 4, (me + 1) % 4)[i]
        block = region(w, s, part, phase, pos, (None, None, 0, 1)[i])
        j = recv_index(w, s, part, phase, i)
        start(remote(block, block, w_send.at[w * 4 + s + phase], w_recv.at[j], (plus, minus, plus, minus)[i]))

    def w_wait(w, s, part, phase, i):
        me, plus, minus = ring(part, phase)
        pos = ((me + 3) % 4, (me + 1) % 4, (me + 2) % 4)[i]
        block = region(w, s, part, phase, pos, None)
        j = recv_index(w, s, part, phase, i)
        remote(block, block, w_send.at[w * 4 + s + phase], w_recv.at[j], plus).wait_recv()

    def p1(w):
        for part in (0, 1):
            for i in (0, 1):
                w_start(w, 0, part, 0, i)

    def forward(w, s, phase):
        for part in (0, 1):
            for i in (0, 1):
                w_wait(w, s, part, phase, i)
                w_start(w, s, part, phase, i + 2)

    def p2(w):
        forward(w, 0, 0)

    def x_copy(w, part, relayed):
        me = ring(part, 1)[0]
        block = region(w, 0, part, 1, me, None)
        if relayed:
            src, dst = relays[w].at[part], region(w, 1, part, 1, me, None)
        else:
            src, dst = block, relays[w].at[part]
        return remote(src, dst, w_send.at[w * 4 + 3], x_recv.at[w * 4 + relayed * 2 + part], x_dirs[part])

    def ready(w):
        for part in (0, 1):
            w_wait(w, 0, part, 0, 2)

    def x1(w):
        for part in (0, 1):
            start(x_copy(w, part, 0))

    def xr(w):
        for part in (0, 1):
            x_copy(w, part, 0).wait_recv()
            start(x_copy(w, part, 1))

    def p3(w, s):
        for part in (0, 1):
            if s == 1:
                x_copy(w, part, 1).wait_recv()
            for i in (0, 1):
                w_start(w, s, part, 1, i)

    def p4(w, s):
        forward(w, s, 1)

    def p5(w, s):
        for part in (0, 1):
            w_wait(w, s, part, 1, 2)

    def wait_sent():
        def drained(ref, sem):
            remote(ref, ref, sem, x_recv.at[0], sib).wait_send()

        for w in range(4):
            ref = weights[w]
            drained(ref.at[0, 0, 0:3], w_send.at[w * 4])
            drained(ref.at[0, 0:3], w_send.at[w * 4 + 1])
            drained(ref.at[1, 0:3], w_send.at[w * 4 + 2])
            drained(ref.at[0, 0:2], w_send.at[w * 4 + 3])
        for r in range(3):
            drained(xs.at[r, 0], ag_send.at[r * 2])
            drained(xs.at[r, 0, :, 0], ag_send.at[r * 2 + 1])
            drained(po.at[r], rs_send.at[r * 2])
            drained(pc.at[r], rs_send.at[r * 2 + 1])
        drained(sti, st_send.at[0])
        swap_prm.wait_send()
        swap_sp.wait_send()

    def ag_ici(r, ch):
        return remote(
            xs.at[r, L, ch, 0], xs.at[r, R, ch, 0], ag_send.at[r * 2], ag_recv.at[r * (2 * CH + 1) + ch], partner
        )

    def ag_d2d(r, ch):
        chunk = pl.ds(0, CH) if ch is None else ch
        return remote(
            xs.at[r, L, chunk, 0], xs.at[r, L, chunk, 1], ag_send.at[r * 2], ag_recv.at[r * (2 * CH + 1) + 2 * CH], sib
        )

    def ag_fwd(r, ch):
        return remote(
            xs.at[r, R, ch, 0], xs.at[r, R, ch, 1], ag_send.at[r * 2 + 1], ag_recv.at[r * (2 * CH + 1) + CH + ch], sib
        )

    def rs_d2d_right(r, ch):
        return remote(po.at[r, R, ch], ps.at[r, R, ch], rs_send.at[r * 2], rs_recv.at[r * (2 * CH + 1) + ch], sib)

    def rs_d2d_left(r):
        return remote(po.at[r, L], ps.at[r, L], rs_send.at[r * 2], rs_recv.at[r * (2 * CH + 1) + 2 * CH], sib)

    def rs_ici(r, ch):
        return remote(pc.at[r, ch], pr.at[r, ch], rs_send.at[r * 2 + 1], rs_recv.at[r * (2 * CH + 1) + CH + ch], partner)

    def normed(rows, gain):
        factor = lax.rsqrt(jnp.mean(rows * rows, axis=1, keepdims=True) + norm_epsilon)
        return (rows * factor * gain[...]).astype(BF16)

    def ag_send_chunk(r, ch):
        start(ag_ici(r, ch))
        start(ag_d2d(r, ch))

    def ag_wait_left(r):
        ag_d2d(r, None).wait_recv()

    def ag_relay(r, ch):
        ag_ici(r, ch).wait_recv()
        start(ag_fwd(r, ch))

    def ag_wait_right(r, ch):
        ag_fwd(r, ch).wait_recv()

    loads[0].wait()
    pl.semaphore_wait(barrier, len(greeted))
    p1(DN)
    loads[1].wait()
    loads[2].wait()
    wgl[0, zl, y] = jnp.concatenate(
        [gate_lift[half, j * 128 : (j + 1) * 128] for j in range(3) for half in (0, 1)]
        + [gate_lift[half, 384:448] for half in (0, 1)],
        axis=0,
    ).T
    p1(GL)
    for load in loads[3:]:
        load.wait()

    for ch in range(CH):

        @pl.loop(0, CROWS // STEP)
        def _(i):
            rows = pl.ds(i * STEP, STEP)
            xs[0, L, ch, 0, rows, :] = normed(res[ch, rows, :].astype(F32), gain_b)

    prm[0] = jnp.concatenate([small[0], small[1], small[2], jnp.zeros((2, 128), F32)], axis=0)
    swap_prm = remote(prm.at[0], prm.at[1], sw_send.at[0], sw_recv.at[0], swap_to)
    swap_sp = remote(sp2.at[0], sp2.at[1], sw_send.at[1], sw_recv.at[1], swap_to)
    for ch in range(CH):
        ag_send_chunk(0, ch)
    start(swap_prm)
    start(swap_sp)

    def pick(ref, b, ch):
        return ref[b].reshape(256, ref.shape[-1]) if ch is None else ref[b, ch]

    def put(ref, b, ch, cols, value):
        if ch is None:
            for k in range(CH):
                ref[b, k, :, cols] = value[k * 128 : (k + 1) * 128]
        else:
            ref[b, ch, :, cols] = value

    def batch_x(r, b, ch):
        return xs[r, b].reshape(256, 2048) if ch is None else xs[r, b, ch].reshape(128, 2048)

    def up_slot(r, b, s, ch=None):
        o = dot(batch_x(r, b, ch), wgl[s, :, :, :, 0:768].reshape(2048, 768))
        for j in range(3):
            to = pl.ds(pl.multiple_of(s * 384 + j * 128, 128), 128)
            h = silu(o[:, j * 256 : j * 256 + 128]) * o[:, j * 256 + 128 : j * 256 + 256]
            put(hid, b, ch, to, h.astype(BF16))

    def up_tail(r, b, ch=None):
        w = jnp.concatenate([wgl[s, :, :, :, 768:896].reshape(2048, 128) for s in (0, 1)], axis=1)
        o = dot(batch_x(r, b, ch), w)
        t0, t1 = o[:, :128], o[:, 128:]
        low = lax.broadcasted_iota(jnp.int32, t0.shape, 1) < 64
        gate = jnp.where(low, t0, pltpu.roll(t1, 64, axis=1))
        lift = jnp.where(low, pltpu.roll(t0, 64, axis=1), t1)
        put(hid, b, ch, pl.ds(768, 128), (silu(gate) * lift).astype(BF16))

    def up(r, b, ch=None):
        for s in (0, 1):
            up_slot(r, b, s, ch)
        up_tail(r, b, ch)

    def wd_cols(zz, yy):
        return jnp.concatenate(
            [wd[0, zz, yy, 0:384], wd[1, zz, yy, 0:384], wd[0, zz, yy, 384:448], wd[1, zz, yy, 384:448]], axis=0
        )

    def wmd_cols(zz, yy):
        return jnp.concatenate([wmd[0, zz, yy], wmd[1, zz, yy]], axis=0)

    def down(r, b, ch, half, lhs, columns_of):
        rhs = jnp.concatenate([columns_of(half * 2 + n // 4, n % 4) for n in range(8)], axis=1)
        o = dot(pick(lhs, b, ch), rhs)
        cols = pl.ds(half * 1024, 1024)
        for i, k in enumerate(range(CH) if ch is None else (ch,)):
            acc[b, k, :, cols] = o[i * 128 : i * 128 + 64]
            po[r, b, k, :, cols] = o[i * 128 + 64 : i * 128 + 128].astype(BF16)

    def down_right(r, ch, lhs, columns_of):
        for half in (0, 1):
            down(r, R, ch, half, lhs, columns_of)
        start(rs_d2d_right(r, ch))

    def rs_right(r, ch):
        rs_d2d_right(r, ch).wait_recv()

        @pl.loop(0, CROWS // STEP)
        def _(i):
            rows = pl.ds(i * STEP, STEP)
            pc[r, ch, rows, :] = (acc[R, ch, rows, :] + ps[r, R, ch, rows, :].astype(F32)).astype(BF16)

        start(rs_ici(r, ch))

    def down_rest(r, lhs, columns_of, first):
        first()
        down(r, L, None, 0, lhs, columns_of)
        rs_right(r, 1)
        down(r, L, None, 1, lhs, columns_of)
        start(rs_d2d_left(r))

    def rs_left(r, coefficient, gain, between=None):
        rs_d2d_left(r).wait_recv()
        for ch in range(CH):
            rs_ici(r, ch).wait_recv()

            @pl.loop(0, CROWS // STEP)
            def _(i):
                rows = pl.ds(i * STEP, STEP)
                delta = acc[L, ch, rows, :] + ps[r, L, ch, rows, :].astype(F32) + pr[r, ch, rows, :].astype(F32)
                new = (res[ch, rows, :].astype(F32) + coefficient * delta).astype(BF16)
                if gain is None:
                    out[pl.ds(ch * CROWS + i * STEP, STEP), :] = new
                else:
                    res[ch, rows, :] = new
                    xs[r + 1, L, ch, 0, rows, :] = normed(new.astype(F32), gain)

            if gain is not None:
                ag_send_chunk(r + 1, ch)
            if between is not None and ch == 0:
                between()

    def mixer_up(b, ch=None):
        for s in (0, 1):
            to = pl.ds(s * 256, 256)
            o = dot(batch_x(1, b, ch), wuv[s].reshape(2048, 512))
            put(gu, b, ch, to, gelu(o[:, :256]))
            put(lf, b, ch, to, gelu(o[:, 256:]))

    def tokens(ref, b, q, cols):
        return jnp.concatenate([ref[b, k, q * 64 : q * 64 + 64, cols] for k in range(CH)], axis=0)

    lane = lax.broadcasted_iota(jnp.int32, (128, 128), 1)

    def stat_send():
        table = jnp.zeros((128, 128), F32)
        for q in (0, 1):
            for b in (0, 1):
                v = tokens(lf, b, q, slice(None))
                mean = jnp.mean(v, axis=1, keepdims=True)
                dev2 = jnp.sum(jnp.square(v - mean), axis=1, keepdims=True)
                table = jnp.where(lane == q * 8 + b * 2, mean, table)
                table = jnp.where(lane == q * 8 + b * 2 + 1, dev2, table)
        flipped = table.T
        sto[0] = flipped[0:8]
        sto[1] = flipped[8:16]
        routes = (
            (0, 1, 0, sib),
            (1, 0, 0, sib),
            (0, 0, 1, partner),
            (0, 1, 2, dev(xo, y, z8, 1 - c)),
            (1, 0, 2, dev(xt, y, z8, 1 - c)),
            (1, 1, 1, dev(xt, y, z8, c)),
        )
        for q, dest, slot, to in routes:
            start(remote(sto.at[q], sti.at[dest, slot], st_send.at[0], st_recv.at[0], to))

    def stat_combine():
        remote(sti, sti, st_send.at[0], st_recv.at[0], sib).wait_recv()
        rows = []
        for q in (0, 1):
            for b in (0, 1):
                parts = [(sto, q, None, b), (sti, q, 0, b), (sti, q, 1, 1 - b), (sti, q, 2, 1 - b)]
                means, devs = [], []
                for ref, qq, slot, bb in parts:
                    block = ref[qq] if slot is None else ref[qq, slot]
                    means.append(block[bb * 2 : bb * 2 + 1])
                    devs.append(block[bb * 2 + 1 : bb * 2 + 2])
                centre = (means[0] + means[1] + means[2] + means[3]) * 0.25
                spread = devs[0] + devs[1] + devs[2] + devs[3]
                for m in means:
                    spread = spread + 512.0 * jnp.square(m - centre)
                rows.append(centre)
                rows.append(lax.rsqrt(spread * (1.0 / A) + layer_epsilon))
        for s in (0, 1):
            for g in (0, 1):
                rows.append(prm[s, 4 + g : 5 + g])
        rows.append(jnp.zeros((116, 128), F32))
        colm[...] = jnp.concatenate(rows, axis=0).T

    def mixer_mid(b):
        for q in (0, 1):
            k = (q * 2 + b) * 2
            centre, factor = colm[:, k : k + 1], colm[:, k + 1 : k + 2]
            for s in (0, 1):
                for g in (0, 1):
                    n = s * 2 + g
                    cols = pl.ds(n * 128, 128)
                    v = (tokens(lf, b, q, cols) - centre) * factor * prm[s, g : g + 1] + prm[s, 2 + g : 3 + g]
                    mixed = dot(msp[n], v.astype(BF16)) + colm[:, 8 + n : 9 + n]
                    gated = (tokens(gu, b, q, cols) * mixed).astype(BF16)
                    for k in range(CH):
                        hid2[b, k, q * 64 : q * 64 + 64, cols] = gated[k * 64 : k * 64 + 64]

    p2(DN)
    p1(UV)
    p2(GL)
    p1(MD)
    ready(DN)
    p3(DN, 0)
    ready(GL)
    x1(GL)
    p3(GL, 0)
    p2(UV)
    p4(DN, 0)
    xr(GL)
    x1(DN)
    p4(GL, 0)
    ready(UV)
    p2(MD)
    ag_relay(0, 0)
    ag_relay(0, 1)
    ag_wait_left(0)
    ag_wait_right(0, 0)
    ag_wait_right(0, 1)
    p3(GL, 1)
    p5(GL, 0)

    @pl.loop(0, 2)
    def _(b):
        up_slot(0, b, 0)

    xr(DN)
    x1(UV)
    ready(MD)
    p4(GL, 1)
    p3(DN, 1)
    xr(UV)
    x1(MD)
    p5(GL, 1)
    up_slot(0, L, 1)
    up_tail(0, L)
    p4(DN, 1)
    p3(UV, 0)
    up_slot(0, R, 1)
    up_tail(0, R)
    xr(MD)
    p5(DN, 0)
    p5(DN, 1)
    p3(UV, 1)
    down_right(0, 0, hid, wd_cols)
    down_right(0, 1, hid, wd_cols)
    down_rest(0, hid, wd_cols, lambda: rs_right(0, 0))
    p4(UV, 0)
    swap_prm.wait_recv()
    swap_sp.wait_recv()
    causal = lax.broadcasted_iota(jnp.int32, (128, 128), 0) >= lane
    for s in (0, 1):
        for g in (0, 1):
            msp[s * 2 + g] = jnp.where(causal, sp2[s, g].astype(F32), 0.0).astype(BF16)

    def weights_between():
        p4(UV, 1)
        p3(MD, 0)
        p3(MD, 1)

    rs_left(0, 0.5, m_gain, weights_between)
    p4(MD, 0)
    ag_relay(1, 0)
    p5(UV, 0)
    p5(UV, 1)
    ag_relay(1, 1)
    ag_wait_left(1)
    mixer_up(L)
    ag_wait_right(1, 0)
    mixer_up(R, 0)
    p4(MD, 1)
    ag_wait_right(1, 1)
    mixer_up(R, 1)
    stat_send()
    p5(MD, 0)
    p5(MD, 1)
    stat_combine()
    mixer_mid(R)
    down_right(1, 0, hid2, wmd_cols)
    down_right(1, 1, hid2, wmd_cols)
    mixer_mid(L)
    down_rest(1, hid2, wmd_cols, lambda: rs_right(1, 0))
    rs_left(1, 1.0, gain_a)
    ag_wait_left(2)
    up_slot(2, L, 0)
    ag_relay(2, 0)
    up_slot(2, L, 1)
    up_tail(2, L)
    ag_wait_right(2, 0)
    up_slot(2, R, 0, 0)
    ag_relay(2, 1)
    up_slot(2, R, 1, 0)
    up_tail(2, R, 0)
    down_right(2, 0, hid, wd_cols)
    ag_wait_right(2, 1)
    up(2, R, 1)
    rs_right(2, 0)
    down_right(2, 1, hid, wd_cols)
    down_rest(2, hid, wd_cols, lambda: None)
    rs_left(2, 0.5, None)
    wait_sent()


def layer(stream, gain_b, gain_a, p_gate, p_lift, p_down, m_gain, m_u, m_v, l_gain, l_shift, spat, s_shift, m_down):
    dma = pltpu.SemaphoreType.DMA
    return pl.pallas_call(
        kernel,
        out_shape=pltpu.VMEM((128, 2048), BF16),
        in_specs=[pl.BlockSpec(memory_space=pl.ANY)] * 14,
        out_specs=pl.BlockSpec(memory_space=pltpu.VMEM),
        scratch_shapes=[
            pltpu.VMEM((2, 4, 4, 128, 896), BF16),
            pltpu.VMEM((2, 4, 4, 448, 128), BF16),
            pltpu.VMEM((2, 4, 4, 128, 512), BF16),
            pltpu.VMEM((2, 4, 4, 256, 128), BF16),
            pltpu.VMEM((2, 4, 64, 896), BF16),
            pltpu.VMEM((2, 4, 224, 128), BF16),
            pltpu.VMEM((2, 4, 64, 512), BF16),
            pltpu.VMEM((2, 4, 128, 128), BF16),
            pltpu.VMEM((2, 448, 128), BF16),
            pltpu.VMEM((1, 2048), F32),
            pltpu.VMEM((1, 2048), F32),
            pltpu.VMEM((1, 2048), F32),
            pltpu.VMEM((3, 2, 128), F32),
            pltpu.VMEM((4, 128, 128), BF16),
            pltpu.VMEM((2, 2, 128, 128), BF16),
            pltpu.VMEM((2, 8, 128), F32),
            pltpu.VMEM((3, 2, CH, 2, CROWS, 2048), BF16),
            pltpu.VMEM((3, 2, CH, CROWS, 2048), BF16),
            pltpu.VMEM((3, 2, CH, CROWS, 2048), BF16),
            pltpu.VMEM((3, CH, CROWS, 2048), BF16),
            pltpu.VMEM((3, CH, CROWS, 2048), BF16),
            pltpu.VMEM((2, CH, CROWS, 2048), F32),
            pltpu.VMEM((2, CH, 128, 896), BF16),
            pltpu.VMEM((2, CH, 128, 512), BF16),
            pltpu.VMEM((2, CH, 128, 512), F32),
            pltpu.VMEM((2, CH, 128, 512), F32),
            pltpu.VMEM((CH, CROWS, 2048), BF16),
            pltpu.VMEM((2, 8, 128), F32),
            pltpu.VMEM((2, 3, 8, 128), F32),
            pltpu.VMEM((128, 128), F32),
            dma((15,)),
            dma((16,)), dma((72,)), dma((16,)),
            dma((2,)), dma((2,)),
            dma((6,)), dma((3 * (2 * CH + 1),)),
            dma((6,)), dma((3 * (2 * CH + 1),)),
            dma((1,)), dma((1,)),
        ],
        compiler_params=pltpu.CompilerParams(
            collective_id=0, has_side_effects=True, vmem_limit_bytes=58 * 1024 * 1024
        ),
    )(
        stream, gain_b.reshape(1, -1), gain_a.reshape(1, -1), p_gate.T, p_lift.T, p_down, m_gain.reshape(1, -1),
        m_u, m_v, l_gain.reshape(2, 128), l_shift.reshape(2, 128), spat, s_shift, m_down,
    )


def solution(mesh):
    placed = (
        P(("rep", "fs", "tp"), None),
        P(),
        P(),
        P("fs", "tp"),
        P("fs", "tp"),
        P("tp", "fs"),
        P(),
        P("fs", "tp"),
        P("fs", "tp"),
        P("tp"),
        P("tp"),
        P("tp", None, None),
        P("tp", None),
        P("tp", "fs"),
    )
    return jax.shard_map(
        layer, mesh=mesh, in_specs=placed, out_specs=P(("rep", "fs", "tp"), None), check_vma=False
    )
```

```python
import jax
import jax.numpy as jnp
from jax import lax
from jax.experimental import pallas as pl
from jax.experimental.pallas import tpu as pltpu
from jax.sharding import PartitionSpec as P

MESH = pl.DeviceIdType.MESH
F32 = jnp.float32
BF16 = jnp.bfloat16
A = 2048
norm_epsilon = 1e-06
layer_epsilon = 1e-05
L, R = 0, 1
GL, DN, UV, MD = 0, 1, 2, 3
W_ROWS = (128, 448, 128, 256)
CH = 2
CROWS = 128 // CH
STEP = 16


def silu(v):
    return v / (1.0 + jnp.exp(-v))


def gelu(v):
    return 0.5 * v * (1.0 + jnp.tanh(0.7978845608028654 * (v + 0.044715 * (v * v * v))))


def dot(a, b):
    return jnp.dot(a, b, preferred_element_type=F32)


def recv_index(w, s, part, phase, i):
    return ((w * 3 + s * 2 + phase - s) * 2 + part) * 3 + min(i, 2)


def kernel(
    stream, h_gain_b, h_gain_a, p_gate, p_lift, p_down, h_gain_m, m_u, m_v, l_gain, l_shift, spat, s_shift, m_down,
    out,
    wgl, wd, wuv, wmd, rgl, rd, ruv, rmd, gate_lift, gain_b, gain_a, m_gain, small, msp, sp2, prm,
    xs, po, ps, pc, pr, acc, hid, hid2, gu, lf, res, sto, sti, colm,
    in_sem, w_send, w_recv, x_recv, sw_send, sw_recv, ag_send, ag_recv, rs_send, rs_recv, st_send, st_recv,
):
    rep, fs, tp = lax.axis_index("rep"), lax.axis_index("fs"), lax.axis_index("tp")
    x, c = tp // 2, tp % 2
    zl, y = fs // 4, fs % 4
    z8 = rep * 4 + zl

    def dev(dx, dy, dz, dc):
        return (dz // 4, (dz % 4) * 4 + dy, dx * 2 + dc)

    sib = dev(x, y, z8, 1 - c)
    xo = (x + 1 + 2 * ((x + c) % 2)) % 4
    xt = (x + 1 + 2 * ((x + c + 1) % 2)) % 4
    partner = dev(xo, y, z8, c)
    y_plus, y_minus = dev(x, (y + 1) % 4, z8, c), dev(x, (y + 3) % 4, z8, c)
    z_plus, z_minus = dev(x, y, (z8 + 1) % 8, c), dev(x, y, (z8 + 7) % 8, c)
    swap_to = dev((x + 2) % 4, y, z8, c)
    weights = (wgl, wd, wuv, wmd)
    relays = (rgl, rd, ruv, rmd)
    x_dirs = (dev((x + 1) % 4, y, z8, c), dev((x + 3) % 4, y, z8, c))

    barrier = pltpu.get_barrier_semaphore()
    greeted = (
        sib, partner, dev(xo, y, z8, 1 - c), dev(xt, y, z8, 0), dev(xt, y, z8, 1),
        y_plus, y_minus, z_plus, z_minus, swap_to,
    )
    for other in greeted:
        pl.semaphore_signal(barrier, inc=1, device_id=other, device_id_type=MESH)

    def remote(src, dst, ssem, rsem, to):
        return pltpu.make_async_remote_copy(
            src_ref=src, dst_ref=dst, send_sem=ssem, recv_sem=rsem, device_id=to, device_id_type=MESH
        )

    def start(copy):
        copy.start()

    loads = [
        pltpu.make_async_copy(src, dst, in_sem.at[i])
        for i, (src, dst) in enumerate(
            (
                (p_down, wd.at[0, zl, y]),
                (p_gate, gate_lift.at[0]),
                (p_lift, gate_lift.at[1]),
                (stream.at[pl.ds(0, CROWS)], res.at[0]),
                (stream.at[pl.ds(CROWS, CROWS)], res.at[1]),
                (h_gain_b, gain_b),
                (m_u, wuv.at[0, zl, y, :, pl.ds(0, 256)]),
                (m_v, wuv.at[0, zl, y, :, pl.ds(256, 256)]),
                (m_down, wmd.at[0, zl, y]),
                (l_gain, small.at[0]),
                (l_shift, small.at[1]),
                (s_shift, small.at[2]),
                (spat, sp2.at[0]),
                (h_gain_m, m_gain),
                (h_gain_a, gain_a),
            )
        )
    ]
    for load in loads:
        load.start()

    def region(w, s, part, phase, pos, sub):
        n = W_ROWS[w] // 2
        r0 = part * n
        if sub is not None:
            n //= 2
            r0 += sub * n
        rows = pl.ds(r0, n)
        ref = weights[w]
        if phase == 0:
            return ref.at[s, zl, pos, rows] if part == 0 else ref.at[s, pos, y, rows]
        return ref.at[s, pos, :, rows] if part == 0 else ref.at[s, :, pos, rows]

    def ring(part, phase):
        if part == phase:
            return y, y_plus, y_minus
        return zl, z_plus, z_minus

    def w_start(w, s, part, phase, i):
        me, plus, minus = ring(part, phase)
        pos = (me, me, (me + 3) % 4, (me + 1) % 4)[i]
        block = region(w, s, part, phase, pos, (None, None, 0, 1)[i])
        j = recv_index(w, s, part, phase, i)
        start(remote(block, block, w_send.at[w * 4 + s + phase], w_recv.at[j], (plus, minus, plus, minus)[i]))

    def w_wait(w, s, part, phase, i):
        me, plus, minus = ring(part, phase)
        pos = ((me + 3) % 4, (me + 1) % 4, (me + 2) % 4)[i]
        block = region(w, s, part, phase, pos, None)
        j = recv_index(w, s, part, phase, i)
        remote(block, block, w_send.at[w * 4 + s + phase], w_recv.at[j], plus).wait_recv()

    def p1(w):
        for part in (0, 1):
            for i in (0, 1):
                w_start(w, 0, part, 0, i)

    def forward(w, s, phase):
        for part in (0, 1):
            for i in (0, 1):
                w_wait(w, s, part, phase, i)
                w_start(w, s, part, phase, i + 2)

    def p2(w):
        forward(w, 0, 0)

    def x_copy(w, part, relayed):
        me = ring(part, 1)[0]
        block = region(w, 0, part, 1, me, None)
        if relayed:
            src, dst = relays[w].at[part], region(w, 1, part, 1, me, None)
        else:
            src, dst = block, relays[w].at[part]
        return remote(src, dst, w_send.at[w * 4 + 3], x_recv.at[w * 4 + relayed * 2 + part], x_dirs[part])

    def ready(w):
        for part in (0, 1):
            w_wait(w, 0, part, 0, 2)

    def x1(w):
        for part in (0, 1):
            start(x_copy(w, part, 0))

    def xr(w):
        for part in (0, 1):
            x_copy(w, part, 0).wait_recv()
            start(x_copy(w, part, 1))

    def p3(w, s):
        for part in (0, 1):
            if s == 1:
                x_copy(w, part, 1).wait_recv()
            for i in (0, 1):
                w_start(w, s, part, 1, i)

    def p4(w, s):
        forward(w, s, 1)

    def p5(w, s):
        for part in (0, 1):
            w_wait(w, s, part, 1, 2)

    def wait_sent():
        def drained(ref, sem):
            remote(ref, ref, sem, x_recv.at[0], sib).wait_send()

        for w in range(4):
            ref = weights[w]
            drained(ref.at[0, 0, 0:3], w_send.at[w * 4])
            drained(ref.at[0, 0:3], w_send.at[w * 4 + 1])
            drained(ref.at[1, 0:3], w_send.at[w * 4 + 2])
            drained(ref.at[0, 0:2], w_send.at[w * 4 + 3])
        for r in range(3):
            drained(xs.at[r, 0], ag_send.at[r * 2])
            drained(xs.at[r, 0, :, 0], ag_send.at[r * 2 + 1])
            drained(po.at[r], rs_send.at[r * 2])
            drained(pc.at[r], rs_send.at[r * 2 + 1])
        drained(sti, st_send.at[0])
        swap_prm.wait_send()
        swap_sp.wait_send()

    def ag_ici(r, ch):
        return remote(
            xs.at[r, L, ch, 0], xs.at[r, R, ch, 0], ag_send.at[r * 2], ag_recv.at[r * (2 * CH + 1) + ch], partner
        )

    def ag_d2d(r, ch):
        chunk = pl.ds(0, CH) if ch is None else ch
        return remote(
            xs.at[r, L, chunk, 0], xs.at[r, L, chunk, 1], ag_send.at[r * 2], ag_recv.at[r * (2 * CH + 1) + 2 * CH], sib
        )

    def ag_fwd(r, ch):
        return remote(
            xs.at[r, R, ch, 0], xs.at[r, R, ch, 1], ag_send.at[r * 2 + 1], ag_recv.at[r * (2 * CH + 1) + CH + ch], sib
        )

    def rs_d2d_right(r, ch):
        return remote(po.at[r, R, ch], ps.at[r, R, ch], rs_send.at[r * 2], rs_recv.at[r * (2 * CH + 1) + ch], sib)

    def rs_d2d_left(r):
        return remote(po.at[r, L], ps.at[r, L], rs_send.at[r * 2], rs_recv.at[r * (2 * CH + 1) + 2 * CH], sib)

    def rs_ici(r, ch):
        return remote(pc.at[r, ch], pr.at[r, ch], rs_send.at[r * 2 + 1], rs_recv.at[r * (2 * CH + 1) + CH + ch], partner)

    def normed(rows, gain):
        factor = lax.rsqrt(jnp.mean(rows * rows, axis=1, keepdims=True) + norm_epsilon)
        return (rows * factor * gain[...]).astype(BF16)

    def ag_send_chunk(r, ch):
        start(ag_ici(r, ch))
        start(ag_d2d(r, ch))

    def ag_wait_left(r):
        ag_d2d(r, None).wait_recv()

    def ag_relay(r, ch):
        ag_ici(r, ch).wait_recv()
        start(ag_fwd(r, ch))

    def ag_wait_right(r, ch):
        ag_fwd(r, ch).wait_recv()

    loads[0].wait()
    pl.semaphore_wait(barrier, len(greeted))
    p1(DN)
    loads[1].wait()
    loads[2].wait()
    wgl[0, zl, y] = jnp.concatenate(
        [gate_lift[half, j * 128 : (j + 1) * 128] for j in range(3) for half in (0, 1)]
        + [gate_lift[half, 384:448] for half in (0, 1)],
        axis=0,
    ).T
    p1(GL)
    for load in loads[3:]:
        load.wait()

    for ch in range(CH):

        @pl.loop(0, CROWS // STEP)
        def _(i):
            rows = pl.ds(i * STEP, STEP)
            xs[0, L, ch, 0, rows, :] = normed(res[ch, rows, :].astype(F32), gain_b)

    prm[0] = jnp.concatenate([small[0], small[1], small[2], jnp.zeros((2, 128), F32)], axis=0)
    swap_prm = remote(prm.at[0], prm.at[1], sw_send.at[0], sw_recv.at[0], swap_to)
    swap_sp = remote(sp2.at[0], sp2.at[1], sw_send.at[1], sw_recv.at[1], swap_to)
    for ch in range(CH):
        ag_send_chunk(0, ch)
    start(swap_prm)
    start(swap_sp)

    def pick(ref, b, ch):
        return ref[b].reshape(256, ref.shape[-1]) if ch is None else ref[b, ch]

    def put(ref, b, ch, cols, value):
        if ch is None:
            for k in range(CH):
                ref[b, k, :, cols] = value[k * 128 : (k + 1) * 128]
        else:
            ref[b, ch, :, cols] = value

    def batch_x(r, b, ch):
        return xs[r, b].reshape(256, 2048) if ch is None else xs[r, b, ch].reshape(128, 2048)

    def up_slot(r, b, s, ch=None):
        o = dot(batch_x(r, b, ch), wgl[s, :, :, :, 0:768].reshape(2048, 768))
        for j in range(3):
            to = pl.ds(pl.multiple_of(s * 384 + j * 128, 128), 128)
            h = silu(o[:, j * 256 : j * 256 + 128]) * o[:, j * 256 + 128 : j * 256 + 256]
            put(hid, b, ch, to, h.astype(BF16))

    def up_tail(r, b, ch=None):
        w = jnp.concatenate([wgl[s, :, :, :, 768:896].reshape(2048, 128) for s in (0, 1)], axis=1)
        o = dot(batch_x(r, b, ch), w)
        t0, t1 = o[:, :128], o[:, 128:]
        low = lax.broadcasted_iota(jnp.int32, t0.shape, 1) < 64
        gate = jnp.where(low, t0, pltpu.roll(t1, 64, axis=1))
        lift = jnp.where(low, pltpu.roll(t0, 64, axis=1), t1)
        put(hid, b, ch, pl.ds(768, 128), (silu(gate) * lift).astype(BF16))

    def up(r, b, ch=None):
        for s in (0, 1):
            up_slot(r, b, s, ch)
        up_tail(r, b, ch)

    def wd_cols(zz, yy):
        return jnp.concatenate(
            [wd[0, zz, yy, 0:384], wd[1, zz, yy, 0:384], wd[0, zz, yy, 384:448], wd[1, zz, yy, 384:448]], axis=0
        )

    def wmd_cols(zz, yy):
        return jnp.concatenate([wmd[0, zz, yy], wmd[1, zz, yy]], axis=0)

    def down(r, b, ch, half, lhs, columns_of):
        rhs = jnp.concatenate([columns_of(half * 2 + n // 4, n % 4) for n in range(8)], axis=1)
        o = dot(pick(lhs, b, ch), rhs)
        cols = pl.ds(half * 1024, 1024)
        for i, k in enumerate(range(CH) if ch is None else (ch,)):
            acc[b, k, :, cols] = o[i * 128 : i * 128 + 64]
            po[r, b, k, :, cols] = o[i * 128 + 64 : i * 128 + 128].astype(BF16)

    def down_right(r, ch, lhs, columns_of):
        for half in (0, 1):
            down(r, R, ch, half, lhs, columns_of)
        start(rs_d2d_right(r, ch))

    def rs_right(r, ch):
        rs_d2d_right(r, ch).wait_recv()

        @pl.loop(0, CROWS // STEP)
        def _(i):
            rows = pl.ds(i * STEP, STEP)
            pc[r, ch, rows, :] = (acc[R, ch, rows, :] + ps[r, R, ch, rows, :].astype(F32)).astype(BF16)

        start(rs_ici(r, ch))

    def down_rest(r, lhs, columns_of, first):
        first()
        down(r, L, None, 0, lhs, columns_of)
        rs_right(r, 1)
        down(r, L, None, 1, lhs, columns_of)
        start(rs_d2d_left(r))

    def rs_left(r, coefficient, gain, between=None):
        rs_d2d_left(r).wait_recv()
        for ch in range(CH):
            rs_ici(r, ch).wait_recv()

            @pl.loop(0, CROWS // STEP)
            def _(i):
                rows = pl.ds(i * STEP, STEP)
                delta = acc[L, ch, rows, :] + ps[r, L, ch, rows, :].astype(F32) + pr[r, ch, rows, :].astype(F32)
                new = (res[ch, rows, :].astype(F32) + coefficient * delta).astype(BF16)
                if gain is None:
                    out[pl.ds(ch * CROWS + i * STEP, STEP), :] = new
                else:
                    res[ch, rows, :] = new
                    xs[r + 1, L, ch, 0, rows, :] = normed(new.astype(F32), gain)

            if gain is not None:
                ag_send_chunk(r + 1, ch)
            if between is not None and ch == 0:
                between()

    def mixer_up(b, ch=None):
        for s in (0, 1):
            to = pl.ds(s * 256, 256)
            o = dot(batch_x(1, b, ch), wuv[s].reshape(2048, 512))
            put(gu, b, ch, to, gelu(o[:, :256]))
            put(lf, b, ch, to, gelu(o[:, 256:]))

    def tokens(ref, b, q, cols):
        return jnp.concatenate([ref[b, k, q * 64 : q * 64 + 64, cols] for k in range(CH)], axis=0)

    lane = lax.broadcasted_iota(jnp.int32, (128, 128), 1)

    def stat_send():
        table = jnp.zeros((128, 128), F32)
        for q in (0, 1):
            for b in (0, 1):
                v = tokens(lf, b, q, slice(None))
                mean = jnp.mean(v, axis=1, keepdims=True)
                dev2 = jnp.sum(jnp.square(v - mean), axis=1, keepdims=True)
                table = jnp.where(lane == q * 8 + b * 2, mean, table)
                table = jnp.where(lane == q * 8 + b * 2 + 1, dev2, table)
        flipped = table.T
        sto[0] = flipped[0:8]
        sto[1] = flipped[8:16]
        routes = (
            (0, 1, 0, sib),
            (1, 0, 0, sib),
            (0, 0, 1, partner),
            (0, 1, 2, dev(xo, y, z8, 1 - c)),
            (1, 0, 2, dev(xt, y, z8, 1 - c)),
            (1, 1, 1, dev(xt, y, z8, c)),
        )
        for q, dest, slot, to in routes:
            start(remote(sto.at[q], sti.at[dest, slot], st_send.at[0], st_recv.at[0], to))

    def stat_combine():
        remote(sti, sti, st_send.at[0], st_recv.at[0], sib).wait_recv()
        rows = []
        for q in (0, 1):
            for b in (0, 1):
                parts = [(sto, q, None, b), (sti, q, 0, b), (sti, q, 1, 1 - b), (sti, q, 2, 1 - b)]
                means, devs = [], []
                for ref, qq, slot, bb in parts:
                    block = ref[qq] if slot is None else ref[qq, slot]
                    means.append(block[bb * 2 : bb * 2 + 1])
                    devs.append(block[bb * 2 + 1 : bb * 2 + 2])
                centre = (means[0] + means[1] + means[2] + means[3]) * 0.25
                spread = devs[0] + devs[1] + devs[2] + devs[3]
                for m in means:
                    spread = spread + 512.0 * jnp.square(m - centre)
                rows.append(centre)
                rows.append(lax.rsqrt(spread * (1.0 / A) + layer_epsilon))
        for s in (0, 1):
            for g in (0, 1):
                rows.append(prm[s, 4 + g : 5 + g])
        rows.append(jnp.zeros((116, 128), F32))
        colm[...] = jnp.concatenate(rows, axis=0).T

    def mixer_mid(b):
        for q in (0, 1):
            k = (q * 2 + b) * 2
            centre, factor = colm[:, k : k + 1], colm[:, k + 1 : k + 2]
            for s in (0, 1):
                for g in (0, 1):
                    n = s * 2 + g
                    cols = pl.ds(n * 128, 128)
                    v = (tokens(lf, b, q, cols) - centre) * factor * prm[s, g : g + 1] + prm[s, 2 + g : 3 + g]
                    mixed = dot(msp[n], v.astype(BF16)) + colm[:, 8 + n : 9 + n]
                    gated = (tokens(gu, b, q, cols) * mixed).astype(BF16)
                    for k in range(CH):
                        hid2[b, k, q * 64 : q * 64 + 64, cols] = gated[k * 64 : k * 64 + 64]

    p1(MD)
    p2(DN)
    p1(UV)
    p2(GL)
    ready(DN)
    p3(DN, 0)
    ready(GL)
    x1(GL)
    p3(GL, 0)
    p2(UV)
    p4(DN, 0)
    xr(GL)
    x1(DN)
    p4(GL, 0)
    ready(UV)
    p2(MD)
    ag_relay(0, 0)
    ag_relay(0, 1)
    ag_wait_left(0)
    ag_wait_right(0, 0)
    ag_wait_right(0, 1)
    p3(GL, 1)
    p5(GL, 0)

    @pl.loop(0, 2)
    def _(b):
        up_slot(0, b, 0)

    xr(DN)
    x1(UV)
    ready(MD)
    p4(GL, 1)
    p3(DN, 1)
    xr(UV)
    x1(MD)
    p5(GL, 1)
    up_slot(0, L, 1)
    up_tail(0, L)
    p4(DN, 1)
    p3(UV, 0)
    up_slot(0, R, 1)
    up_tail(0, R)
    xr(MD)
    p5(DN, 0)
    p5(DN, 1)
    p3(UV, 1)
    down_right(0, 0, hid, wd_cols)
    down_right(0, 1, hid, wd_cols)
    down_rest(0, hid, wd_cols, lambda: rs_right(0, 0))
    p4(UV, 0)
    swap_prm.wait_recv()
    swap_sp.wait_recv()
    causal = lax.broadcasted_iota(jnp.int32, (128, 128), 0) >= lane
    for s in (0, 1):
        for g in (0, 1):
            msp[s * 2 + g] = jnp.where(causal, sp2[s, g].astype(F32), 0.0).astype(BF16)

    def weights_between():
        p4(UV, 1)
        p3(MD, 0)
        p3(MD, 1)

    rs_left(0, 0.5, m_gain, weights_between)
    p4(MD, 0)
    def between_right():
        rs_right(1, 0)
        mixer_mid(L)

    ag_relay(1, 0)
    p5(UV, 0)
    p5(UV, 1)
    ag_relay(1, 1)
    ag_wait_left(1)
    mixer_up(L)
    ag_wait_right(1, 0)
    mixer_up(R, 0)
    p4(MD, 1)
    ag_wait_right(1, 1)
    mixer_up(R, 1)
    stat_send()
    p5(MD, 0)
    p5(MD, 1)
    stat_combine()
    mixer_mid(R)
    down_right(1, 0, hid2, wmd_cols)
    down_right(1, 1, hid2, wmd_cols)
    down_rest(1, hid2, wmd_cols, between_right)
    rs_left(1, 1.0, gain_a)
    ag_wait_left(2)
    up_slot(2, L, 0)
    ag_relay(2, 0)
    up_slot(2, L, 1)
    up_tail(2, L)
    ag_wait_right(2, 0)
    up_slot(2, R, 0, 0)
    ag_relay(2, 1)
    up_slot(2, R, 1, 0)
    up_tail(2, R, 0)
    down_right(2, 0, hid, wd_cols)
    ag_wait_right(2, 1)
    up(2, R, 1)
    rs_right(2, 0)
    down_right(2, 1, hid, wd_cols)
    down_rest(2, hid, wd_cols, lambda: None)
    rs_left(2, 0.5, None)
    wait_sent()


def layer(stream, gain_b, gain_a, p_gate, p_lift, p_down, m_gain, m_u, m_v, l_gain, l_shift, spat, s_shift, m_down):
    dma = pltpu.SemaphoreType.DMA
    return pl.pallas_call(
        kernel,
        out_shape=pltpu.VMEM((128, 2048), BF16),
        in_specs=[pl.BlockSpec(memory_space=pl.ANY)] * 14,
        out_specs=pl.BlockSpec(memory_space=pltpu.VMEM),
        scratch_shapes=[
            pltpu.VMEM((2, 4, 4, 128, 896), BF16),
            pltpu.VMEM((2, 4, 4, 448, 128), BF16),
            pltpu.VMEM((2, 4, 4, 128, 512), BF16),
            pltpu.VMEM((2, 4, 4, 256, 128), BF16),
            pltpu.VMEM((2, 4, 64, 896), BF16),
            pltpu.VMEM((2, 4, 224, 128), BF16),
            pltpu.VMEM((2, 4, 64, 512), BF16),
            pltpu.VMEM((2, 4, 128, 128), BF16),
            pltpu.VMEM((2, 448, 128), BF16),
            pltpu.VMEM((1, 2048), F32),
            pltpu.VMEM((1, 2048), F32),
            pltpu.VMEM((1, 2048), F32),
            pltpu.VMEM((3, 2, 128), F32),
            pltpu.VMEM((4, 128, 128), BF16),
            pltpu.VMEM((2, 2, 128, 128), BF16),
            pltpu.VMEM((2, 8, 128), F32),
            pltpu.VMEM((3, 2, CH, 2, CROWS, 2048), BF16),
            pltpu.VMEM((3, 2, CH, CROWS, 2048), BF16),
            pltpu.VMEM((3, 2, CH, CROWS, 2048), BF16),
            pltpu.VMEM((3, CH, CROWS, 2048), BF16),
            pltpu.VMEM((3, CH, CROWS, 2048), BF16),
            pltpu.VMEM((2, CH, CROWS, 2048), F32),
            pltpu.VMEM((2, CH, 128, 896), BF16),
            pltpu.VMEM((2, CH, 128, 512), BF16),
            pltpu.VMEM((2, CH, 128, 512), F32),
            pltpu.VMEM((2, CH, 128, 512), F32),
            pltpu.VMEM((CH, CROWS, 2048), BF16),
            pltpu.VMEM((2, 8, 128), F32),
            pltpu.VMEM((2, 3, 8, 128), F32),
            pltpu.VMEM((128, 128), F32),
            dma((15,)),
            dma((16,)), dma((72,)), dma((16,)),
            dma((2,)), dma((2,)),
            dma((6,)), dma((3 * (2 * CH + 1),)),
            dma((6,)), dma((3 * (2 * CH + 1),)),
            dma((1,)), dma((1,)),
        ],
        compiler_params=pltpu.CompilerParams(
            collective_id=0, has_side_effects=True, vmem_limit_bytes=58 * 1024 * 1024
        ),
    )(
        stream, gain_b.reshape(1, -1), gain_a.reshape(1, -1), p_gate.T, p_lift.T, p_down, m_gain.reshape(1, -1),
        m_u, m_v, l_gain.reshape(2, 128), l_shift.reshape(2, 128), spat, s_shift, m_down,
    )


def solution(mesh):
    placed = (
        P(("rep", "fs", "tp"), None),
        P(),
        P(),
        P("fs", "tp"),
        P("fs", "tp"),
        P("tp", "fs"),
        P(),
        P("fs", "tp"),
        P("fs", "tp"),
        P("tp"),
        P("tp"),
        P("tp", None, None),
        P("tp", None),
        P("tp", "fs"),
    )
    return jax.shard_map(
        layer, mesh=mesh, in_specs=placed, out_specs=P(("rep", "fs", "tp"), None), check_vma=False
    )
```
